512 devices in a mesh: rep: 2 (over z_hi), fs: 32 (over z_lo, y), tp: 8 (over x, core).
Axes of the slice: x: 4, y: 8, z: 8 (z_hi: 2, z_lo: 4; z = z_hi * 4 + z_lo), core: 2. Of those that a mesh axis runs over, the one named last changes fastest.
Arguments:
- states: bfloat16 [24576, 2048], P(('rep', 'fs'), 'tp'), may hold values from -6 to 6
- mix_gain: float32 [2048], replicated, may hold values from 0.1 to 1.9
- w_value: bfloat16 [2048, 2048], P('fs', 'tp'), may hold values from -1 to 1
- w_gate: bfloat16 [2048, 2048], P('fs', 'tp'), may hold values from -0.125 to 0.125
- conv_kernel: float32 [31, 2048], replicated, may hold values from -1 to 1
- chan_gain: float32 [2048], replicated, may hold values from 0.1 to 1.9
- w_mix_out: bfloat16 [2048, 2048], P('fs', 'tp'), may hold values from -0.125 to 0.125
- mlp_gain: float32 [2048], replicated, may hold values from 0.1 to 1.9
- w_up: bfloat16 [2048, 6144], P('fs', 'tp'), may hold values from -0.125 to 0.125
- w_down_t: bfloat16 [2048, 6144], P('fs', 'tp'), may hold values from -0.078125 to 0.078125
Outputs:
- layer_out: bfloat16 [24576, 2048], P(('rep', 'fs'), 'tp')
The draws below stay inside these ranges and needn't reach their ends.
All inputs are finite; a program needn't handle non-finite values.
Results may differ from the reference program's by a relative error of at most 0.017.
Values may be sent and summed in bfloat16 or wider, within the bound.
No kernel may reach another device: no remote copies, remote signals or barrier semaphores. Data moves between devices by JAX's collectives and lax.ppermute only.
A program may use at most 64 MiB of HBM per device.

```python
import jax
import jax.numpy as jnp
from jax import lax

D = 2048
FF = 6144
KWIDTH = 31
LENGTH = 128
SEQS = 3
ROWS = 384
TOKENS = 24576
N_TP = 8


def draw_w_value(key, part):
    first_key, second_key = jax.random.split(jax.random.fold_in(key, 17))
    column = jnp.arange(D, dtype=jnp.float32)
    ramp = 10.0 ** (column / D)
    base = jnp.clip(jax.random.normal(first_key, (D, D), jnp.float32), -6.0, 6.0)
    jitter = jax.random.uniform(second_key, (D,), jnp.float32, 0.7, 1.3)
    scale = ramp * jitter / (3.0 * jnp.sqrt(jnp.float32(D)))
    return jnp.clip(base * scale[None, :], -1.0, 1.0).astype(jnp.bfloat16)


def shard_levels(own_key, shape, cuts, low, high):
    loudness, own = 1.0, jax.random.fold_in(own_key, 6)
    for position, blocks in cuts:
        heights = jnp.exp(jax.random.uniform(jax.random.fold_in(own, position), (blocks,), jnp.float32, low / len(cuts), high / len(cuts)))
        loudness = loudness * jnp.repeat(heights, shape[position] // blocks).reshape([-1 if axis == position else 1 for axis in range(len(shape))])
    return loudness


def normal_values(key, shape, deviation, most, cuts=(), kind=jnp.bfloat16):
    values = deviation * jax.random.normal(key, shape, jnp.float32)
    if cuts:
        values = values * shard_levels(key, shape, cuts, -0.22, 0.18)
    return jnp.clip(values, -most, most).astype(kind)


def setup_inputs(seed: int = 0) -> dict:
    arg_keys = jax.random.split(jax.random.key(seed), 11)
    return {
        "states": normal_values(arg_keys[0], (TOKENS, D), 1.0, 6.0, ((0, 64), (1, 8))),
        "mix_gain": jnp.clip(1.0 + 0.18 * jax.random.normal(arg_keys[1], (D,), jnp.float32), 0.1, 1.9),
        "w_value": draw_w_value(jax.random.fold_in(arg_keys[10], 71), 0),
        "w_gate": normal_values(arg_keys[3], (D, D), D ** -0.5, 0.125, ((0, 32), (1, 8))),
        "conv_kernel": normal_values(arg_keys[4], (KWIDTH, D), KWIDTH ** -0.5, 1.0, (), jnp.float32),
        "chan_gain": jnp.clip(1.0 + 0.18 * jax.random.normal(arg_keys[5], (D,), jnp.float32), 0.1, 1.9),
        "w_mix_out": normal_values(arg_keys[6], (D, D), D ** -0.5, 0.125, ((0, 32), (1, 8))),
        "mlp_gain": jnp.clip(1.0 + 0.18 * jax.random.normal(arg_keys[7], (D,), jnp.float32), 0.1, 1.9),
        "w_up": normal_values(arg_keys[8], (D, FF), D ** -0.5, 0.125, ((0, 32), (1, 8))),
        "w_down_t": normal_values(arg_keys[9], (D, FF), FF ** -0.5, 0.078125, ((0, 32), (1, 8))),
    }


EPS = 1e-06

def rms_norm(rows, gain):
    values = rows.astype(jnp.float32)
    scaled = values * lax.rsqrt(lax.optimization_barrier(jnp.mean(values * values, axis=-1, keepdims=True)) + EPS)
    return (scaled * gain).astype(jnp.bfloat16)

def causal_filter(gated, conv_kernel):
    width = gated.shape[1]
    blocks = gated.reshape(SEQS, LENGTH, width)
    padded = jnp.pad(blocks, ((0, 0), (KWIDTH - 1, 0), (0, 0)))
    total = jnp.zeros_like(blocks)
    for tap in range(KWIDTH):
        total = total + conv_kernel[tap][None, None, :] * padded[:, tap:tap + LENGTH, :]
    return total.reshape(SEQS * LENGTH, width)

def project_out(activated, weight_t):
    block = activated.shape[1] // N_TP
    total = jnp.zeros((activated.shape[0], weight_t.shape[0]), jnp.float32)
    for index in range(N_TP):
        piece = lax.dot_general(activated[:, index * block:(index + 1) * block], weight_t[:, index * block:(index + 1) * block], (((1,), (1,)), ((), ())), preferred_element_type=jnp.float32)
        total = total + piece.astype(jnp.bfloat16).astype(jnp.float32)
    return total

def one_group(rows, mix_gain, w_value, w_gate, conv_kernel, chan_gain, w_mix_out, mlp_gain, w_up, w_down_t):
    normed = rms_norm(rows, mix_gain)
    value = jnp.dot(normed, w_value, preferred_element_type=jnp.float32)
    gate = jnp.dot(normed, w_gate, preferred_element_type=jnp.float32)
    gated = value * jax.nn.sigmoid(gate)
    filtered = causal_filter(gated, conv_kernel)
    mean_rows = lax.optimization_barrier(jnp.mean(filtered, axis=-1, keepdims=True))
    variance = lax.optimization_barrier(jnp.mean(filtered * filtered, axis=-1, keepdims=True)) - mean_rows * mean_rows
    activated = jax.nn.silu((filtered - mean_rows) * lax.rsqrt(variance + EPS) * chan_gain).astype(jnp.bfloat16)
    middle = (rows.astype(jnp.float32) + project_out(activated, w_mix_out)).astype(jnp.bfloat16)
    normed_mid = rms_norm(middle, mlp_gain)
    upward = jnp.dot(normed_mid, w_up, preferred_element_type=jnp.float32)
    hidden = jnp.square(jnp.maximum(upward, 0.0)).astype(jnp.bfloat16)
    return (middle.astype(jnp.float32) + project_out(hidden, w_down_t)).astype(jnp.bfloat16)

def reference(states, mix_gain, w_value, w_gate, conv_kernel, chan_gain, w_mix_out, mlp_gain, w_up, w_down_t):
    groups = states.reshape(states.shape[0] // ROWS, ROWS, states.shape[1])

    def apply(rows):
        return one_group(rows, mix_gain, w_value, w_gate, conv_kernel, chan_gain, w_mix_out, mlp_gain, w_up, w_down_t)
    return lax.map(apply, groups).reshape(states.shape)
```

```python
import jax
import jax.numpy as jnp
from jax import lax
from jax.sharding import Mesh
from jax.sharding import PartitionSpec as P

D = 2048
KWIDTH = 31
LENGTH = 128
TP = ("tp_0", "tp_1")


EPS = 1e-06


def cut_rows(length, count):
    hop = length // count
    if hop >= 8:
        hop -= hop % 8
    return [hop * k for k in range(1, count)]


def gather_in_order(shard, axes, order):
    pieces = shard
    for k in order:
        pieces = lax.all_gather(pieces, axes[k])
    done = order[::-1]
    back = [done.index(k) for k in range(len(axes))]
    pieces = pieces.transpose(*back, *range(len(axes), pieces.ndim))
    return pieces.reshape(-1, *shard.shape)


def laid_out(pieces, dim):
    pieces = jnp.moveaxis(pieces, 0, dim)
    dims = pieces.shape
    return pieces.reshape(*dims[:dim], dims[dim] * dims[dim + 1], *dims[dim + 2 :])


def gather_at_once(shard, axes, dim):
    split_at = max(range(max(1, shard.ndim - 1)), key=lambda d: shard.shape[d])
    count, outs = (len(axes), [])
    for initial, slab in enumerate(
        jnp.split(shard, cut_rows(shard.shape[split_at], count), axis=split_at)
    ):
        if slab.size:
            order = [(initial - k) % count for k in range(count)]
            outs.append(gather_in_order(slab, axes, order))
    return laid_out(jnp.concatenate(outs, axis=split_at + 1), dim)


def half_of(weight):
    width = weight.shape[1] // 2
    return lax.dynamic_slice_in_dim(weight, lax.axis_index("rep") * width, width, 1)


def whole_halves(weights):
    mine = jnp.concatenate([half_of(w) for w in weights], axis=1)
    pieces = lax.all_gather(mine, ("rep", "fs"), axis=0, tiled=True)
    pieces = pieces.reshape(2, -1, mine.shape[1])
    ends, at = [], 0
    for w in weights[:-1]:
        at += w.shape[1] // 2
        ends.append(at)
    return [jnp.split(pieces[r], ends, axis=1) for r in range(2)]


def copy_for_each(shard, axis):
    copies = jnp.broadcast_to(shard, (lax.axis_size(axis), *shard.shape))
    return lax.all_to_all(copies, axis, split_axis=0, concat_axis=0, tiled=True)


def over_copies(shard, axis):
    everything = copy_for_each(shard, axis)
    return jnp.sum(everything, axis=0)


def in_one(arrays, axis):
    ends = [0]
    for a in arrays:
        ends.append(ends[-1] + a.size)
    so_far = over_copies(jnp.concatenate([a.ravel() for a in arrays]), axis)
    return tuple((so_far[b:e].reshape(a.shape) for a, b, e in zip(arrays, ends, ends[1:])))


def in_blocks(shard, dim, count):
    before, after = (shard.shape[:dim], shard.shape[dim + 1 :])
    return jnp.moveaxis(shard.reshape(*before, count, -1, *after), dim, 0)


def summed_on_arrival(shard, axis, dim):
    count = lax.axis_size(axis)
    pieces = lax.all_to_all(in_blocks(shard, dim, count), axis, 0, 0, tiled=True)
    return jnp.sum(pieces.astype(jnp.float32), axis=0)


def collect(shard, axis, dim):
    pieces = copy_for_each(shard, axis)
    return laid_out(pieces, dim)


def rms_norm(rows, gain):
    values = rows.astype(jnp.float32)
    scaled = values * lax.rsqrt(jnp.mean(values * values, axis=-1, keepdims=True) + EPS)
    return (scaled * gain).astype(jnp.bfloat16)


def times_transposed(left, right):
    return lax.dot_general(
        left, right, (((1,), (1,)), ((), ())), preferred_element_type=jnp.float32
    )


def body(
    states, mix_gain, w_value, w_gate, conv_kernel, chan_gain, w_mix_out, mlp_gain, w_up, w_down_t
):
    width = states.shape[1]
    offset = lax.axis_index(TP) * width
    token_rows = states.shape[0]
    whole_rows = gather_at_once(states, TP, 1)
    normed = rms_norm(whole_rows, mix_gain)
    mix = whole_halves((w_value, w_gate, w_mix_out))
    value = jnp.concatenate(
        [jnp.dot(normed, h[0], preferred_element_type=jnp.float32) for h in mix], axis=1
    )
    gate = jnp.concatenate(
        [jnp.dot(normed, h[1], preferred_element_type=jnp.float32) for h in mix], axis=1
    )
    gated = value * jax.nn.sigmoid(gate)
    own_kernel = lax.dynamic_slice_in_dim(conv_kernel, offset, width, 1)
    blocks = gated.reshape(token_rows // LENGTH, LENGTH, width)
    padded = jnp.pad(blocks, ((0, 0), (KWIDTH - 1, 0), (0, 0)))
    filtered = jnp.zeros_like(blocks)
    for tap in range(KWIDTH):
        filtered = filtered + own_kernel[tap][None, None, :] * padded[:, tap : tap + LENGTH, :]
    filtered = filtered.reshape(token_rows, width)
    sum_rows, square_rows = in_one(
        (jnp.sum(filtered, axis=-1), jnp.sum(filtered * filtered, axis=-1)), TP
    )
    mean_rows = (sum_rows / D)[:, None]
    variance = (square_rows / D)[:, None] - mean_rows * mean_rows
    own_gain = lax.dynamic_slice_in_dim(chan_gain, offset, width, 0)
    activated = jax.nn.silu((filtered - mean_rows) * lax.rsqrt(variance + EPS) * own_gain).astype(
        jnp.bfloat16
    )
    mixer_terms = times_transposed(activated, jnp.concatenate([h[2] for h in mix], axis=1))
    mixed = summed_on_arrival(mixer_terms.astype(jnp.bfloat16), TP, 1)
    middle = (states.astype(jnp.float32) + mixed).astype(jnp.bfloat16)
    middle_rows = collect(middle, TP, 1)
    normed_mid = rms_norm(middle_rows, mlp_gain)
    fed_terms = 0.0
    for up, down in whole_halves((w_up, w_down_t)):
        upward = jnp.dot(normed_mid, up, preferred_element_type=jnp.float32)
        hidden = jnp.square(jnp.maximum(upward, 0.0)).astype(jnp.bfloat16)
        fed_terms = fed_terms + times_transposed(hidden, down)
    fed = summed_on_arrival(fed_terms.astype(jnp.bfloat16), TP, 1)
    return (middle.astype(jnp.float32) + fed).astype(jnp.bfloat16)


def solution(mesh):
    split = Mesh(
        mesh.devices.reshape(mesh.shape["rep"], mesh.shape["fs"], 4, 2),
        ("rep", "fs", "tp_0", "tp_1"),
    )
    return jax.shard_map(
        body,
        mesh=split,
        in_specs=(
            P(("rep", "fs"), TP),
            P(),
            P("fs", TP),
            P("fs", TP),
            P(),
            P(),
            P("fs", TP),
            P(),
            P("fs", TP),
            P("fs", TP),
        ),
        out_specs=P(("rep", "fs"), TP),
        check_vma=False,
    )
```

```python
import jax
import jax.numpy as jnp
from jax import lax
from jax.experimental import pallas as pl
from jax.experimental.pallas import tpu as pltpu
from jax.sharding import Mesh
from jax.sharding import PartitionSpec as P

D = 2048
KWIDTH = 31
LENGTH = 128
EPS = 1e-06
LATE = 256
TP = ("x", "c")
SWAP = [(0, 1), (1, 0)]


MIB = 1 << 20


def pack_kernel(value_ref, gate_ref, out_ref, up_ref, down_ref, early_ref, late_ref):
    width, first = value_ref.shape[1], up_ref.shape[1] - LATE
    at = 0
    for ref, count in (
        (value_ref, width),
        (gate_ref, width),
        (out_ref, width),
        (up_ref, first),
        (down_ref, first),
    ):
        early_ref[:, at : at + count] = ref[:, :count]
        at += count
    for copy in range(late_ref.shape[0]):
        late_ref[copy, :, :LATE] = up_ref[:, first:]
        late_ref[copy, :, LATE:] = down_ref[:, first:]


def packed(w_value, w_gate, w_mix_out, w_up, w_down_t):
    rows, width = w_value.shape
    columns = 3 * width + 2 * (w_up.shape[1] - LATE)
    return pl.pallas_call(
        pack_kernel,
        out_shape=(
            jax.ShapeDtypeStruct((rows, columns), jnp.bfloat16),
            jax.ShapeDtypeStruct((lax.axis_size("y"), rows, 2 * LATE), jnp.bfloat16),
        ),
        compiler_params=pltpu.CompilerParams(vmem_limit_bytes=4 * MIB),
        cost_estimate=pl.CostEstimate(flops=0, bytes_accessed=MIB, transcendentals=0),
        name="pack",
    )(w_value, w_gate, w_mix_out, w_up, w_down_t)


def over_y(run):
    return lax.all_gather(run, "y", axis=1, tiled=True)


def over_z(slab):
    half = slab.shape[0] // 2

    def from_z(piece, step):
        return lax.ppermute(piece, ("rep", "zl"), [((i + step) % 8, i) for i in range(8)])

    return [slab, from_z(slab, 1), from_z(slab[:half], 2), from_z(slab[half:], -2), from_z(slab, -1)]


def in_one_sum(arrays):
    both = jnp.stack(arrays)
    copies = jnp.broadcast_to(both[None], (lax.axis_size(TP), *both.shape))
    return jnp.sum(lax.all_to_all(copies, TP, 0, 0, tiled=True), axis=0)


def norm_kernel(own_ref, other_ref, gain_ref, out_ref):
    core = lax.axis_index("c")
    count, rows, width = own_ref.shape
    pieces = [(r[i].astype(jnp.float32), i, s) for s, r in enumerate((own_ref, other_ref)) for i in range(count)]
    total = sum(jnp.sum(v * v, axis=-1, keepdims=True) for v, _, _ in pieces)
    scale = lax.rsqrt(total / D + EPS)
    for values, i, side in pieces:
        which = core if side == 0 else 1 - core
        at = pl.ds(pl.multiple_of((2 * i + which) * width, width), width)
        out_ref[:, at] = (values * scale * gain_ref[:, at]).astype(jnp.bfloat16)


def normed_channels(block, gain, beside=()):
    own = lax.all_gather(block, "x", axis=0)
    if beside:
        own, beside = lax.optimization_barrier((own, beside))
    other = lax.ppermute(own, "c", SWAP)
    count, rows, width = own.shape
    part = pl.BlockSpec((count, LENGTH, width), lambda i: (0, i, 0))
    return pl.pallas_call(
        norm_kernel,
        grid=(rows // LENGTH,),
        in_specs=[part, part, pl.BlockSpec((1, D), lambda i: (0, 0))],
        out_specs=pl.BlockSpec((LENGTH, D), lambda i: (i, 0)),
        out_shape=jax.ShapeDtypeStruct((rows, D), jnp.bfloat16),
        cost_estimate=pl.CostEstimate(
            flops=6 * rows * D, bytes_accessed=4 * rows * D, transcendentals=rows
        ),
        compiler_params=pltpu.CompilerParams(vmem_limit_bytes=12 * MIB),
        name="norm",
    )(own, other, gain[None]), beside


def times_transposed(left, right):
    return lax.dot_general(
        left, right, (((1,), (1,)), ((), ())), preferred_element_type=jnp.float32
    )


def over_group(mine, theirs):
    got = lax.ppermute(theirs, "c", SWAP)
    pair = (mine + got.astype(jnp.float32)).astype(jnp.bfloat16)
    return jnp.sum(lax.all_to_all(pair, "x", 0, 0, tiled=True).astype(jnp.float32), axis=0)


def own_sum(left, weight):
    width = weight.shape[1] // 2
    core = lax.axis_index("c")

    def half(which):
        part = lax.dynamic_slice_in_dim(weight, which * width, width, 1)
        total = times_transposed(left, part.reshape(-1, part.shape[2]))
        return total.reshape(total.shape[0], -1, width).transpose(1, 0, 2)

    return over_group(half(core), half(1 - core).astype(jnp.bfloat16))


def squared_relu(upward):
    return jnp.square(jnp.maximum(upward, 0.0)).astype(jnp.bfloat16)


def feed_forward_kernel(x_ref, up_ref, down_ref, *refs):
    *slab_refs, theirs_ref, mine_ref, total_ref = refs
    core, here = lax.axis_index("c"), lax.axis_index("zl")
    step, last = pl.program_id(0), pl.num_programs(0) - 1
    count, depth, _ = up_ref.shape

    def times_t(left, right):
        return lax.dot_general(
            left, right, (((1,), (1,)), ((), ())), preferred_element_type=jnp.float32
        )

    @pl.when(step == 0)
    def _():
        half = depth // 2
        places = []
        for ref, turn, low in zip(slab_refs, (0, 1, 2, 2, 3), (0, 0, 0, half, 0)):
            places.append((ref, lax.rem(here + turn, count), low, ref.shape[0]))
        upward = 0.0
        for ref, z, low, rows in places:
            at = pl.ds(pl.multiple_of(z * depth + low, half), rows)
            upward += jnp.dot(x_ref[:, at], ref[:, :LATE], preferred_element_type=jnp.float32)
        hidden = squared_relu(upward)
        for ref, z, low, rows in places:
            total_ref[z, :, low : low + rows] = times_t(hidden, ref[:, LATE:])

    @pl.when(step > 0)
    def _():
        upward = 0.0
        for z in range(count):
            x = x_ref[:, z * depth : (z + 1) * depth]
            upward += jnp.dot(x, up_ref[z], preferred_element_type=jnp.float32)
        hidden = squared_relu(upward)
        for z in range(count):
            total_ref[z] += times_t(hidden, down_ref[z])

    @pl.when(step == last)
    def _():
        width = depth // 2
        for z in range(count):
            for ref, which in ((theirs_ref, 1 - core), (mine_ref, core)):
                at = pl.ds(pl.multiple_of(which * width, width), width)
                ref[z] = total_ref[z, :, at].astype(ref.dtype)


def feed_forward(x, first, late):
    rows = x.shape[0]
    count, depth, columns = first.shape
    block = 256
    blocks = columns // (2 * block)
    whole = lambda shape: pl.BlockSpec(shape, lambda i: (0,) * len(shape))
    weight = lambda at: pl.BlockSpec(
        (count, depth, block), lambda i: (0, 0, at + jnp.maximum(i - 1, 0))
    )
    out = (count, rows, depth // 2)
    hidden = columns // 2 + LATE
    return pl.pallas_call(
        feed_forward_kernel,
        grid=(blocks + 1,),
        in_specs=[whole(x.shape), weight(0), weight(blocks), *(whole(s.shape) for s in late)],
        out_specs=(whole(out), whole(out)),
        out_shape=(
            jax.ShapeDtypeStruct(out, jnp.bfloat16),
            jax.ShapeDtypeStruct(out, jnp.float32),
        ),
        scratch_shapes=[pltpu.VMEM((count, rows, depth), jnp.float32)],
        compiler_params=pltpu.CompilerParams(vmem_limit_bytes=36 * MIB),
        cost_estimate=pl.CostEstimate(
            flops=4 * rows * D * hidden, bytes_accessed=4 * D * hidden, transcendentals=0
        ),
        name="feed_forward",
    )(x, first, first, *late)


def body(
    states, mix_gain, w_value, w_gate, conv_kernel, chan_gain, w_mix_out, mlp_gain, w_up, w_down_t
):
    width = states.shape[1]
    offset = lax.axis_index(TP) * width
    token_rows = states.shape[0]
    early, late = packed(w_value, w_gate, w_mix_out, w_up, w_down_t)
    run = lax.all_gather(early, "zl", axis=0)
    mix = over_y(run[:, :, : 3 * width])
    normed, _ = normed_channels(states, mix_gain)
    slab = lax.all_to_all(late, "y", 0, 0, tiled=True).reshape(-1, late.shape[2])
    normed, slab = lax.optimization_barrier((normed, slab))
    ffn_late = over_z(slab)
    ffn_first = over_y(run[:, :, 3 * width :])
    rows = mix.reshape(-1, mix.shape[2])
    value = jnp.dot(normed, rows[:, :width], preferred_element_type=jnp.float32)
    gate = jnp.dot(normed, rows[:, width : 2 * width], preferred_element_type=jnp.float32)
    gated = value * jax.nn.sigmoid(gate)
    own_kernel = lax.dynamic_slice_in_dim(conv_kernel, offset, width, 1)
    blocks = gated.reshape(token_rows // LENGTH, LENGTH, width)
    padded = jnp.pad(blocks, ((0, 0), (KWIDTH - 1, 0), (0, 0)))
    filtered = jnp.zeros_like(blocks)
    for tap in range(KWIDTH):
        filtered = filtered + own_kernel[tap][None, None, :] * padded[:, tap : tap + LENGTH, :]
    filtered = filtered.reshape(token_rows, width)
    sums = in_one_sum((jnp.sum(filtered, axis=-1), jnp.sum(filtered * filtered, axis=-1)))
    mean_rows = (sums[0] / D)[:, None]
    variance = (sums[1] / D)[:, None] - mean_rows * mean_rows
    own_gain = lax.dynamic_slice_in_dim(chan_gain, offset, width, 0)
    activated = jax.nn.silu((filtered - mean_rows) * lax.rsqrt(variance + EPS) * own_gain).astype(
        jnp.bfloat16
    )
    mixed = own_sum(activated, mix[:, :, 2 * width :])
    middle = (states.astype(jnp.float32) + mixed).astype(jnp.bfloat16)
    normed_mid, ffn_late = normed_channels(middle, mlp_gain, ffn_late)
    theirs, mine = feed_forward(normed_mid, ffn_first, ffn_late)
    fed = over_group(mine, theirs)
    return (middle.astype(jnp.float32) + fed).astype(jnp.bfloat16)


def solution(mesh):
    split = Mesh(mesh.devices.reshape(2, 4, 8, 4, 2), ("rep", "zl", "y", "x", "c"))
    fs = ("zl", "y")
    return jax.shard_map(
        body,
        mesh=split,
        in_specs=(
            P(("rep", *fs), TP),
            P(),
            P(fs, TP),
            P(fs, TP),
            P(),
            P(),
            P(fs, TP),
            P(),
            P(fs, TP),
            P(fs, TP),
        ),
        out_specs=P(("rep", *fs), TP),
        check_vma=False,
    )
```

```python
import jax
import jax.numpy as jnp
from jax import lax
from jax.experimental import pallas as pl
from jax.experimental.pallas import tpu as pltpu
from jax.sharding import Mesh
from jax.sharding import PartitionSpec as P

D = 2048
KWIDTH = 31
LENGTH = 128
EPS = 1e-06
LATE = 256
TP = ("x", "c")
SWAP = [(0, 1), (1, 0)]


MIB = 1 << 20
FFN_VMEM = 40 * MIB
FULL = 60 * MIB


def pack_kernel(value_ref, gate_ref, out_ref, up_ref, down_ref, mix_ref, first_ref, late_ref):
    width, first = value_ref.shape[1], up_ref.shape[1] - LATE
    for i, ref in enumerate((value_ref, gate_ref, out_ref)):
        mix_ref[:, i * width : (i + 1) * width] = ref[...]
    first_ref[:, :first] = up_ref[:, :first]
    first_ref[:, first:] = down_ref[:, :first]
    for copy in range(late_ref.shape[0]):
        late_ref[copy, :, :LATE] = up_ref[:, first:]
        late_ref[copy, :, LATE:] = down_ref[:, first:]


def packed(w_value, w_gate, w_mix_out, w_up, w_down_t):
    rows, width = w_value.shape
    first = w_up.shape[1] - LATE
    return pl.pallas_call(
        pack_kernel,
        out_shape=(
            jax.ShapeDtypeStruct((rows, 3 * width), jnp.bfloat16),
            jax.ShapeDtypeStruct((rows, 2 * first), jnp.bfloat16),
            jax.ShapeDtypeStruct((lax.axis_size("y"), rows, 2 * LATE), jnp.bfloat16),
        ),
        compiler_params=pltpu.CompilerParams(vmem_limit_bytes=FULL),
        cost_estimate=pl.CostEstimate(flops=0, bytes_accessed=MIB, transcendentals=0),
        name="pack",
    )(w_value, w_gate, w_mix_out, w_up, w_down_t)


def over_y(run):
    return lax.all_gather(run, "y", axis=1, tiled=True)


def over_z(slab):
    def from_z(step):
        return lax.ppermute(slab, ("rep", "zl"), [((i + step) % 8, i) for i in range(8)])

    return [slab, from_z(1), from_z(2), from_z(-1)]


def in_one_sum(arrays):
    both = jnp.stack(arrays)
    copies = jnp.broadcast_to(both[None], (lax.axis_size(TP), *both.shape))
    return jnp.sum(lax.all_to_all(copies, TP, 0, 0, tiled=True), axis=0)


def norm_kernel(own_ref, other_ref, gain_ref, out_ref):
    core = lax.axis_index("c")
    count, rows, width = own_ref.shape
    pieces = [(r[i].astype(jnp.float32), i, s) for s, r in enumerate((own_ref, other_ref)) for i in range(count)]
    total = sum(jnp.sum(v * v, axis=-1, keepdims=True) for v, _, _ in pieces)
    scale = lax.rsqrt(total / D + EPS)
    for values, i, side in pieces:
        which = core if side == 0 else 1 - core
        at = pl.ds(pl.multiple_of((2 * i + which) * width, width), width)
        out_ref[:, at] = (values * scale * gain_ref[:, at]).astype(jnp.bfloat16)


def normed_channels(block, gain, beside=()):
    own = lax.all_gather(block, "x", axis=0)
    if beside:
        own, beside = lax.optimization_barrier((own, beside))
    other = lax.ppermute(own, "c", SWAP)
    count, rows, width = own.shape
    part = pl.BlockSpec((count, LENGTH, width), lambda i: (0, i, 0))
    return pl.pallas_call(
        norm_kernel,
        grid=(rows // LENGTH,),
        in_specs=[part, part, pl.BlockSpec((1, D), lambda i: (0, 0))],
        out_specs=pl.BlockSpec((LENGTH, D), lambda i: (i, 0)),
        out_shape=jax.ShapeDtypeStruct((rows, D), jnp.bfloat16),
        cost_estimate=pl.CostEstimate(
            flops=6 * rows * D, bytes_accessed=4 * rows * D, transcendentals=rows
        ),
        compiler_params=pltpu.CompilerParams(vmem_limit_bytes=12 * MIB),
        name="norm",
    )(own, other, gain[None]), beside


def times_transposed(left, right):
    return lax.dot_general(
        left, right, (((1,), (1,)), ((), ())), preferred_element_type=jnp.float32
    )


def over_group(mine, theirs):
    got = lax.ppermute(theirs, "c", SWAP)
    pair = (mine + got.astype(jnp.float32)).astype(jnp.bfloat16)
    return jnp.sum(lax.all_to_all(pair, "x", 0, 0, tiled=True).astype(jnp.float32), axis=0)


def own_sum(left, weight):
    width = weight.shape[1] // 2
    core = lax.axis_index("c")

    def half(which):
        part = lax.dynamic_slice_in_dim(weight, which * width, width, 1)
        total = times_transposed(left, part.reshape(-1, part.shape[2]))
        return total.reshape(total.shape[0], -1, width).transpose(1, 0, 2)

    return over_group(half(core), half(1 - core).astype(jnp.bfloat16))


def squared_relu(upward):
    return jnp.square(jnp.maximum(upward, 0.0)).astype(jnp.bfloat16)


def times_t(left, right):
    return lax.dot_general(
        left, right, (((1,), (1,)), ((), ())), preferred_element_type=jnp.float32
    )


def feed_forward_kernel(x_ref, first_ref, *refs):
    *slab_refs, theirs_ref, mine_ref, up_ref, down_ref, hidden_ref, sems = refs
    core, here = lax.axis_index("c"), lax.axis_index("zl")
    count, depth, columns = up_ref.shape
    width = depth // 2
    copies = []
    for i, ref in enumerate((up_ref, down_ref)):
        part = first_ref.at[:, :, i * columns : (i + 1) * columns]
        copies.append(pltpu.make_async_copy(part, ref, sems.at[i]))
        copies[i].start()
    upward = 0.0
    for turn, ref in enumerate(slab_refs):
        at = pl.ds(pl.multiple_of(lax.rem(here + turn, count) * depth, depth), depth)
        upward += jnp.dot(x_ref[:, at], ref[:, :LATE], preferred_element_type=jnp.float32)
    hidden_ref[:, columns:] = squared_relu(upward)
    copies[0].wait()
    for low in range(0, columns, 256):
        upward = 0.0
        for z in range(count):
            x = x_ref[:, z * depth : (z + 1) * depth]
            upward += jnp.dot(
                x, up_ref[z, :, low : low + 256], preferred_element_type=jnp.float32
            )
        hidden_ref[:, low : low + 256] = squared_relu(upward)
    copies[1].wait()
    for turn, ref in enumerate(slab_refs):
        z = lax.rem(here + turn, count)
        for out_ref, which in ((theirs_ref, 1 - core), (mine_ref, core)):
            rows = pl.ds(pl.multiple_of(which * width, width), width)
            part = times_t(hidden_ref[:, :columns], down_ref[z, rows, :])
            part += times_t(hidden_ref[:, columns:], ref[rows, LATE:])
            out_ref[z] = part.astype(out_ref.dtype)


def feed_forward(x, first, late):
    rows = x.shape[0]
    count, depth, columns = first.shape
    out = (count, rows, depth // 2)
    hidden = columns // 2 + LATE
    vmem = pl.BlockSpec(memory_space=pltpu.VMEM)
    weights = pltpu.VMEM((count, depth, columns // 2), jnp.bfloat16)
    return pl.pallas_call(
        feed_forward_kernel,
        in_specs=[vmem, pl.BlockSpec(memory_space=pltpu.HBM), *(vmem for _ in late)],
        out_specs=(vmem, vmem),
        out_shape=(
            jax.ShapeDtypeStruct(out, jnp.bfloat16),
            jax.ShapeDtypeStruct(out, jnp.float32),
        ),
        scratch_shapes=[
            weights,
            weights,
            pltpu.VMEM((rows, hidden), jnp.bfloat16),
            pltpu.SemaphoreType.DMA((2,)),
        ],
        compiler_params=pltpu.CompilerParams(vmem_limit_bytes=FFN_VMEM),
        cost_estimate=pl.CostEstimate(
            flops=4 * rows * D * hidden, bytes_accessed=4 * D * hidden, transcendentals=0
        ),
        name="feed_forward",
    )(x, first, *late)


def body(
    states, mix_gain, w_value, w_gate, conv_kernel, chan_gain, w_mix_out, mlp_gain, w_up, w_down_t
):
    width = states.shape[1]
    offset = lax.axis_index(TP) * width
    token_rows = states.shape[0]
    early, first, late = packed(w_value, w_gate, w_mix_out, w_up, w_down_t)
    mix = over_y(lax.all_gather(early, "zl", axis=0))
    normed, _ = normed_channels(states, mix_gain)
    ffn_first = over_y(lax.all_gather(first, "zl", axis=0))
    slab = lax.all_to_all(late, "y", 0, 0, tiled=True).reshape(-1, late.shape[2])
    normed, slab = lax.optimization_barrier((normed, slab))
    ffn_late = over_z(slab)
    rows = mix.reshape(-1, mix.shape[2])
    value = jnp.dot(normed, rows[:, :width], preferred_element_type=jnp.float32)
    gate = jnp.dot(normed, rows[:, width : 2 * width], preferred_element_type=jnp.float32)
    gated = value * jax.nn.sigmoid(gate)
    own_kernel = lax.dynamic_slice_in_dim(conv_kernel, offset, width, 1)
    blocks = gated.reshape(token_rows // LENGTH, LENGTH, width)
    padded = jnp.pad(blocks, ((0, 0), (KWIDTH - 1, 0), (0, 0)))
    filtered = jnp.zeros_like(blocks)
    for tap in range(KWIDTH):
        filtered = filtered + own_kernel[tap][None, None, :] * padded[:, tap : tap + LENGTH, :]
    filtered = filtered.reshape(token_rows, width)
    sums = in_one_sum((jnp.sum(filtered, axis=-1), jnp.sum(filtered * filtered, axis=-1)))
    mean_rows = (sums[0] / D)[:, None]
    variance = (sums[1] / D)[:, None] - mean_rows * mean_rows
    own_gain = lax.dynamic_slice_in_dim(chan_gain, offset, width, 0)
    activated = jax.nn.silu((filtered - mean_rows) * lax.rsqrt(variance + EPS) * own_gain).astype(
        jnp.bfloat16
    )
    mixed = own_sum(activated, mix[:, :, 2 * width :])
    middle = (states.astype(jnp.float32) + mixed).astype(jnp.bfloat16)
    normed_mid, ffn_late = normed_channels(middle, mlp_gain, ffn_late)
    theirs, mine = feed_forward(normed_mid, ffn_first, ffn_late)
    fed = over_group(mine, theirs)
    return (middle.astype(jnp.float32) + fed).astype(jnp.bfloat16)


def solution(mesh):
    split = Mesh(mesh.devices.reshape(2, 4, 8, 4, 2), ("rep", "zl", "y", "x", "c"))
    fs = ("zl", "y")
    return jax.shard_map(
        body,
        mesh=split,
        in_specs=(
            P(("rep", *fs), TP),
            P(),
            P(fs, TP),
            P(fs, TP),
            P(),
            P(),
            P(fs, TP),
            P(),
            P(fs, TP),
            P(fs, TP),
        ),
        out_specs=P(("rep", *fs), TP),
        check_vma=False,
    )
```

```python
import jax
import jax.numpy as jnp
from jax import lax
from jax.experimental import pallas as pl
from jax.experimental.pallas import tpu as pltpu
from jax.sharding import Mesh
from jax.sharding import PartitionSpec as P

D = 2048
KWIDTH = 31
LENGTH = 128
EPS = 1e-06
TP = ("x", "c")
SWAP = [(0, 1), (1, 0)]


MIB = 1 << 20
LANES = 128


def times_t(left, right):
    return lax.dot_general(
        left, right, (((1,), (1,)), ((), ())), preferred_element_type=jnp.float32
    )


def copies_kernel(*refs):
    *in_refs, out_ref = refs
    for copy in range(out_ref.shape[0]):
        at = 0
        for ref in in_refs:
            out_ref[copy, :, at : at + ref.shape[1]] = ref[...]
            at += ref.shape[1]


def over_y(*shards):
    rows, columns = shards[0].shape[0], sum(s.shape[1] for s in shards)
    copies = pl.pallas_call(
        copies_kernel,
        out_shape=jax.ShapeDtypeStruct((lax.axis_size("y"), rows, columns), jnp.bfloat16),
        compiler_params=pltpu.CompilerParams(vmem_limit_bytes=60 * MIB),
        cost_estimate=pl.CostEstimate(flops=0, bytes_accessed=MIB, transcendentals=0),
        name="copies",
    )(*shards)
    return lax.all_to_all(copies, "y", 0, 0, tiled=True).reshape(-1, columns)


def over_z(slab):
    half = slab.shape[0] // 2

    def from_z(piece, step):
        return lax.ppermute(piece, ("rep", "zl"), [((i + step) % 8, i) for i in range(8)])

    return [slab, from_z(slab, 1), from_z(slab[:half], 2), from_z(slab[half:], -2), from_z(slab, -1)]


def gate_kernel(x_ref, taps_ref, *refs):
    *slab_refs, filtered_ref, sums_ref, padded_ref = refs
    here, count = lax.axis_index("zl"), lax.axis_size("zl")
    depth, width = slab_refs[0].shape[0], slab_refs[0].shape[1] // 2
    value, gate = 0.0, 0.0
    for ref, turn, low in zip(slab_refs, (0, 1, 2, 2, 3), (0, 0, 0, depth // 2, 0)):
        start = lax.rem(here + turn, count) * depth + low
        x = x_ref[:, pl.ds(pl.multiple_of(start, depth // 2), ref.shape[0])]
        value += jnp.dot(x, ref[:, :width], preferred_element_type=jnp.float32)
        gate += jnp.dot(x, ref[:, width:], preferred_element_type=jnp.float32)
    gated = value * jax.nn.sigmoid(gate)
    pad = padded_ref.shape[1] - LENGTH
    sequences = padded_ref.shape[0]
    for s in range(sequences):
        padded_ref[s, :pad] = jnp.zeros((pad, width), jnp.float32)
        padded_ref[s, pad:] = gated[s * LENGTH : (s + 1) * LENGTH]
    first = lax.axis_index(TP) * width
    for lane in range(0, width, LANES):
        taps = taps_ref[:, pl.ds(pl.multiple_of(first + lane, LANES), LANES)]
        for s in range(sequences):
            total = jnp.zeros((LENGTH, LANES), jnp.float32)
            for shift in range(8):
                offsets = [o for o in range(pad - KWIDTH + 1, pad + 1) if o % 8 == shift]
                span = offsets[-1] - shift + LENGTH
                rows = padded_ref[s, shift : shift + span, lane : lane + LANES]
                for o in offsets:
                    tap = o - (pad - KWIDTH + 1)
                    total += taps[tap : tap + 1] * rows[o - shift : o - shift + LENGTH]
            filtered_ref[s * LENGTH : (s + 1) * LENGTH, lane : lane + LANES] = total
    filtered = filtered_ref[...]
    ones = jnp.ones((8, width), jnp.float32)
    rows = x_ref.shape[0]
    for i, terms in enumerate((filtered, filtered * filtered)):
        sums = lax.dot_general(
            ones,
            terms,
            (((1,), (1,)), ((), ())),
            precision=lax.Precision.HIGHEST,
            preferred_element_type=jnp.float32,
        )
        for copy in range(sums_ref.shape[0]):
            sums_ref[copy, :, i * rows : (i + 1) * rows] = sums[:1]


def gated_filter(x, taps, slabs):
    rows, width = x.shape[0], slabs[0].shape[1] // 2
    vmem = pl.BlockSpec(memory_space=pltpu.VMEM)
    return pl.pallas_call(
        gate_kernel,
        in_specs=[vmem] * (2 + len(slabs)),
        out_specs=(vmem, vmem),
        out_shape=(
            jax.ShapeDtypeStruct((rows, width), jnp.float32),
            jax.ShapeDtypeStruct((lax.axis_size(TP), 1, 2 * rows), jnp.float32),
        ),
        scratch_shapes=[pltpu.VMEM((rows // LENGTH, LENGTH + 32, width), jnp.float32)],
        compiler_params=pltpu.CompilerParams(vmem_limit_bytes=24 * MIB),
        cost_estimate=pl.CostEstimate(
            flops=4 * rows * D * width, bytes_accessed=4 * D * width, transcendentals=rows * width
        ),
        name="gated_filter",
    )(x, taps, *slabs)


def mixer_kernel(filtered_ref, sums_ref, gain_ref, *refs):
    *slab_refs, theirs_ref, mine_ref = refs
    core, here, count = lax.axis_index("c"), lax.axis_index("zl"), lax.axis_size("zl")
    rows, width = filtered_ref.shape
    sums = sum(sums_ref[d] for d in range(sums_ref.shape[0])) / D
    mean = sums[:, :rows]
    scale = lax.rsqrt(sums[:, rows:] - mean * mean + EPS)

    def down_rows(row):
        column = jnp.broadcast_to(row, (LANES, rows)).T
        return jnp.concatenate([column] * (width // LANES), axis=1)

    gain = gain_ref[:, pl.ds(pl.multiple_of(lax.axis_index(TP) * width, width), width)]
    values = (filtered_ref[...] - down_rows(mean)) * down_rows(scale) * gain
    activated = (values / (1.0 + jnp.exp(-values))).astype(jnp.bfloat16)
    near, one, low, high, three = slab_refs
    for turn, ref in ((0, near), (1, one), (2, None), (3, three)):
        z = lax.rem(here + turn, count)
        for out_ref, which in ((theirs_ref, 1 - core), (mine_ref, core)):
            if ref is None:
                weight = jnp.where(which == 0, low[...], high[...])
            else:
                weight = ref[pl.ds(pl.multiple_of(which * width, width), width)]
            out_ref[z] = times_t(activated, weight).astype(out_ref.dtype)


def mixer(filtered, sums, gain, slabs):
    rows, width = filtered.shape
    vmem = pl.BlockSpec(memory_space=pltpu.VMEM)
    out = (lax.axis_size("zl"), rows, width)
    return pl.pallas_call(
        mixer_kernel,
        in_specs=[vmem] * (3 + len(slabs)),
        out_specs=(vmem, vmem),
        out_shape=(
            jax.ShapeDtypeStruct(out, jnp.bfloat16),
            jax.ShapeDtypeStruct(out, jnp.float32),
        ),
        compiler_params=pltpu.CompilerParams(vmem_limit_bytes=24 * MIB),
        cost_estimate=pl.CostEstimate(
            flops=2 * rows * D * width, bytes_accessed=2 * D * width, transcendentals=rows * width
        ),
        name="mixer",
    )(filtered, sums, gain[None], *slabs)


def norm_kernel(own_ref, other_ref, gain_ref, out_ref):
    core = lax.axis_index("c")
    count, rows, width = own_ref.shape
    pieces = [(r[i].astype(jnp.float32), i, s) for s, r in enumerate((own_ref, other_ref)) for i in range(count)]
    total = sum(jnp.sum(v * v, axis=-1, keepdims=True) for v, _, _ in pieces)
    scale = lax.rsqrt(total / D + EPS)
    for values, i, side in pieces:
        which = core if side == 0 else 1 - core
        at = pl.ds(pl.multiple_of((2 * i + which) * width, width), width)
        out_ref[:, at] = (values * scale * gain_ref[:, at]).astype(jnp.bfloat16)


def normed_channels(block, gain):
    own = lax.all_gather(block, "x", axis=0)
    other = lax.ppermute(own, "c", SWAP)
    count, rows, width = own.shape
    part = pl.BlockSpec((count, LENGTH, width), lambda i: (0, i, 0))
    return pl.pallas_call(
        norm_kernel,
        grid=(rows // LENGTH,),
        in_specs=[part, part, pl.BlockSpec((1, D), lambda i: (0, 0))],
        out_specs=pl.BlockSpec((LENGTH, D), lambda i: (i, 0)),
        out_shape=jax.ShapeDtypeStruct((rows, D), jnp.bfloat16),
        cost_estimate=pl.CostEstimate(
            flops=6 * rows * D, bytes_accessed=4 * rows * D, transcendentals=rows
        ),
        compiler_params=pltpu.CompilerParams(vmem_limit_bytes=12 * MIB),
        name="norm",
    )(own, other, gain[None])


def over_group(mine, theirs):
    got = lax.ppermute(theirs, "c", SWAP)
    pair = (mine + got.astype(jnp.float32)).astype(jnp.bfloat16)
    return jnp.sum(lax.all_to_all(pair, "x", 0, 0, tiled=True).astype(jnp.float32), axis=0)


def feed_forward_kernel(x_ref, weight_ref, theirs_ref, mine_ref, up_ref, down_ref, hidden_ref, sems):
    core = lax.axis_index("c")
    count, _, width = mine_ref.shape
    copies = []
    for i, ref in enumerate((up_ref, down_ref)):
        copies.append(pltpu.make_async_copy(weight_ref.at[i], ref, sems.at[i]))
        copies[i].start()
    copies[0].wait()
    for low in range(0, up_ref.shape[1], width):
        upward = jnp.dot(
            x_ref[...], up_ref[:, low : low + width], preferred_element_type=jnp.float32
        )
        hidden = jnp.square(jnp.maximum(upward, 0.0))
        hidden_ref[:, low : low + width] = hidden.astype(jnp.bfloat16)
    copies[1].wait()
    for out_ref, which in ((theirs_ref, 1 - core), (mine_ref, core)):
        for i in range(count):
            at = pl.ds(pl.multiple_of((2 * i + which) * width, width), width)
            out_ref[i] = times_t(hidden_ref[...], down_ref[at]).astype(out_ref.dtype)


def feed_forward(x, weights):
    rows = x.shape[0]
    hidden = weights.shape[2]
    out = (4, rows, D // 8)
    vmem = pl.BlockSpec(memory_space=pltpu.VMEM)
    return pl.pallas_call(
        feed_forward_kernel,
        in_specs=[vmem, pl.BlockSpec(memory_space=pl.ANY)],
        out_specs=(vmem, vmem),
        out_shape=(
            jax.ShapeDtypeStruct(out, jnp.bfloat16),
            jax.ShapeDtypeStruct(out, jnp.float32),
        ),
        scratch_shapes=[
            pltpu.VMEM((D, hidden), jnp.bfloat16),
            pltpu.VMEM((D, hidden), jnp.bfloat16),
            pltpu.VMEM((rows, hidden), jnp.bfloat16),
            pltpu.SemaphoreType.DMA((2,)),
        ],
        compiler_params=pltpu.CompilerParams(vmem_limit_bytes=56 * MIB),
        cost_estimate=pl.CostEstimate(
            flops=4 * rows * D * hidden, bytes_accessed=4 * D * hidden, transcendentals=0
        ),
        name="feed_forward",
    )(x, weights)


def body(
    states, mix_gain, w_value, w_gate, conv_kernel, chan_gain, w_mix_out, mlp_gain, w_up, w_down_t
):
    sent = jnp.where(lax.axis_index("rep") == 0, w_up, w_down_t)
    ffn = lax.all_gather(sent, ("rep", "zl", "y"), axis=0).reshape(2, -1, sent.shape[1])
    slab = over_y(w_value, w_gate)
    gate_slabs = over_z(slab)
    normed = normed_channels(states, mix_gain)
    slab, w_mix_out = lax.optimization_barrier((slab, w_mix_out))
    out_slabs = over_z(over_y(w_mix_out))
    filtered, sums = gated_filter(normed, conv_kernel, gate_slabs)
    sums = lax.all_to_all(sums, TP, 0, 0, tiled=True)
    theirs, mine = mixer(filtered, sums, chan_gain, out_slabs)
    mixed = over_group(mine, theirs)
    middle = (states.astype(jnp.float32) + mixed).astype(jnp.bfloat16)
    normed_mid = normed_channels(middle, mlp_gain)
    theirs, mine = feed_forward(normed_mid, ffn)
    fed = over_group(mine, theirs)
    return (middle.astype(jnp.float32) + fed).astype(jnp.bfloat16)


def solution(mesh):
    split = Mesh(mesh.devices.reshape(2, 4, 8, 4, 2), ("rep", "zl", "y", "x", "c"))
    fs = ("zl", "y")
    return jax.shard_map(
        body,
        mesh=split,
        in_specs=(
            P(("rep", *fs), TP),
            P(),
            P(fs, TP),
            P(fs, TP),
            P(),
            P(),
            P(fs, TP),
            P(),
            P(fs, TP),
            P(fs, TP),
        ),
        out_specs=P(("rep", *fs), TP),
        check_vma=False,
    )
```

```python
import jax
import jax.numpy as jnp
from jax import lax
from jax.experimental import pallas as pl
from jax.experimental.pallas import tpu as pltpu
from jax.sharding import Mesh
from jax.sharding import PartitionSpec as P

D = 2048
KWIDTH = 31
LENGTH = 128
EPS = 1e-06
TP = ("x", "c")
SWAP = [(0, 1), (1, 0)]


MIB = 1 << 20
LANES = 128


def times_t(left, right):
    return lax.dot_general(
        left, right, (((1,), (1,)), ((), ())), preferred_element_type=jnp.float32
    )


def copies_kernel(*refs):
    *in_refs, out_ref = refs
    for copy in range(out_ref.shape[0]):
        at = 0
        for ref in in_refs:
            out_ref[copy, :, at : at + ref.shape[1]] = ref[...]
            at += ref.shape[1]


def over_y(*shards):
    rows, columns = shards[0].shape[0], sum(s.shape[1] for s in shards)
    copies = pl.pallas_call(
        copies_kernel,
        out_shape=jax.ShapeDtypeStruct((lax.axis_size("y"), rows, columns), jnp.bfloat16),
        compiler_params=pltpu.CompilerParams(vmem_limit_bytes=60 * MIB),
        cost_estimate=pl.CostEstimate(flops=0, bytes_accessed=MIB, transcendentals=0),
        name="copies",
    )(*shards)
    return lax.all_to_all(copies, "y", 0, 0, tiled=True).reshape(-1, columns)


def over_z(slab):
    half = slab.shape[0] // 2

    def from_z(piece, step):
        return lax.ppermute(piece, ("rep", "zl"), [((i + step) % 8, i) for i in range(8)])

    return [slab, from_z(slab, 1), from_z(slab[:half], 2), from_z(slab[half:], -2), from_z(slab, -1)]


def gate_kernel(x_ref, taps_ref, *refs):
    *slab_refs, filtered_ref, sums_ref, padded_ref = refs
    here, count = lax.axis_index("zl"), lax.axis_size("zl")
    depth, width = slab_refs[0].shape[0], slab_refs[0].shape[1] // 3
    value, gate = 0.0, 0.0
    for ref, turn, low in zip(slab_refs, (0, 1, 2, 2, 3), (0, 0, 0, depth // 2, 0)):
        start = lax.rem(here + turn, count) * depth + low
        x = x_ref[:, pl.ds(pl.multiple_of(start, depth // 2), ref.shape[0])]
        value += jnp.dot(x, ref[:, :width], preferred_element_type=jnp.float32)
        gate += jnp.dot(x, ref[:, width : 2 * width], preferred_element_type=jnp.float32)
    gated = value * jax.nn.sigmoid(gate)
    pad = padded_ref.shape[1] - LENGTH
    sequences = padded_ref.shape[0]
    for s in range(sequences):
        padded_ref[s, :pad] = jnp.zeros((pad, width), jnp.float32)
        padded_ref[s, pad:] = gated[s * LENGTH : (s + 1) * LENGTH]
    first = lax.axis_index(TP) * width
    for lane in range(0, width, LANES):
        taps = taps_ref[:, pl.ds(pl.multiple_of(first + lane, LANES), LANES)]
        for s in range(sequences):
            total = jnp.zeros((LENGTH, LANES), jnp.float32)
            for shift in range(8):
                offsets = [o for o in range(pad - KWIDTH + 1, pad + 1) if o % 8 == shift]
                span = offsets[-1] - shift + LENGTH
                rows = padded_ref[s, shift : shift + span, lane : lane + LANES]
                for o in offsets:
                    tap = o - (pad - KWIDTH + 1)
                    total += taps[tap : tap + 1] * rows[o - shift : o - shift + LENGTH]
            filtered_ref[s * LENGTH : (s + 1) * LENGTH, lane : lane + LANES] = total
    filtered = filtered_ref[...]
    ones = jnp.ones((8, width), jnp.float32)
    rows = x_ref.shape[0]
    for i, terms in enumerate((filtered, filtered * filtered)):
        sums = lax.dot_general(
            ones,
            terms,
            (((1,), (1,)), ((), ())),
            precision=lax.Precision.HIGHEST,
            preferred_element_type=jnp.float32,
        )
        for copy in range(sums_ref.shape[0]):
            sums_ref[copy, :, i * rows : (i + 1) * rows] = sums[:1]


def gated_filter(x, taps, slabs):
    rows, width = x.shape[0], slabs[0].shape[1] // 3
    vmem = pl.BlockSpec(memory_space=pltpu.VMEM)
    return pl.pallas_call(
        gate_kernel,
        in_specs=[vmem] * (2 + len(slabs)),
        out_specs=(vmem, vmem),
        out_shape=(
            jax.ShapeDtypeStruct((rows, width), jnp.float32),
            jax.ShapeDtypeStruct((lax.axis_size(TP), 1, 2 * rows), jnp.float32),
        ),
        scratch_shapes=[pltpu.VMEM((rows // LENGTH, LENGTH + 32, width), jnp.float32)],
        compiler_params=pltpu.CompilerParams(vmem_limit_bytes=24 * MIB),
        cost_estimate=pl.CostEstimate(
            flops=4 * rows * D * width, bytes_accessed=4 * D * width, transcendentals=rows * width
        ),
        name="gated_filter",
    )(x, taps, *slabs)


def mixer_kernel(filtered_ref, sums_ref, gain_ref, *refs):
    *slab_refs, theirs_ref, mine_ref = refs
    core, here, count = lax.axis_index("c"), lax.axis_index("zl"), lax.axis_size("zl")
    rows, width = filtered_ref.shape
    sums = sum(sums_ref[d] for d in range(sums_ref.shape[0])) / D
    mean = sums[:, :rows]
    scale = lax.rsqrt(sums[:, rows:] - mean * mean + EPS)

    def down_rows(row):
        column = jnp.broadcast_to(row, (LANES, rows)).T
        return jnp.concatenate([column] * (width // LANES), axis=1)

    gain = gain_ref[:, pl.ds(pl.multiple_of(lax.axis_index(TP) * width, width), width)]
    values = (filtered_ref[...] - down_rows(mean)) * down_rows(scale) * gain
    activated = (values / (1.0 + jnp.exp(-values))).astype(jnp.bfloat16)
    near, one, low, high, three = slab_refs
    for turn, ref in ((0, near), (1, one), (2, None), (3, three)):
        z = lax.rem(here + turn, count)
        for out_ref, which in ((theirs_ref, 1 - core), (mine_ref, core)):
            if ref is None:
                weight = jnp.where(which == 0, low[:, 2 * width :], high[:, 2 * width :])
            else:
                weight = ref[pl.ds(pl.multiple_of(which * width, width), width), 2 * width :]
            out_ref[z] = times_t(activated, weight).astype(out_ref.dtype)


def mixer(filtered, sums, gain, slabs):
    rows, width = filtered.shape
    vmem = pl.BlockSpec(memory_space=pltpu.VMEM)
    out = (lax.axis_size("zl"), rows, width)
    return pl.pallas_call(
        mixer_kernel,
        in_specs=[vmem] * (3 + len(slabs)),
        out_specs=(vmem, vmem),
        out_shape=(
            jax.ShapeDtypeStruct(out, jnp.bfloat16),
            jax.ShapeDtypeStruct(out, jnp.float32),
        ),
        compiler_params=pltpu.CompilerParams(vmem_limit_bytes=24 * MIB),
        cost_estimate=pl.CostEstimate(
            flops=2 * rows * D * width, bytes_accessed=2 * D * width, transcendentals=rows * width
        ),
        name="mixer",
    )(filtered, sums, gain[None], *slabs)


def norm_kernel(own_ref, other_ref, gain_ref, out_ref):
    core = lax.axis_index("c")
    count, rows, width = own_ref.shape
    pieces = [(r[i].astype(jnp.float32), i, s) for s, r in enumerate((own_ref, other_ref)) for i in range(count)]
    total = sum(jnp.sum(v * v, axis=-1, keepdims=True) for v, _, _ in pieces)
    scale = lax.rsqrt(total / D + EPS)
    for values, i, side in pieces:
        which = core if side == 0 else 1 - core
        at = pl.ds(pl.multiple_of((2 * i + which) * width, width), width)
        out_ref[:, at] = (values * scale * gain_ref[:, at]).astype(jnp.bfloat16)


def normed_channels(block, gain):
    own = lax.all_gather(block, "x", axis=0)
    other = lax.ppermute(own, "c", SWAP)
    count, rows, width = own.shape
    part = pl.BlockSpec((count, LENGTH, width), lambda i: (0, i, 0))
    return pl.pallas_call(
        norm_kernel,
        grid=(rows // LENGTH,),
        in_specs=[part, part, pl.BlockSpec((1, D), lambda i: (0, 0))],
        out_specs=pl.BlockSpec((LENGTH, D), lambda i: (i, 0)),
        out_shape=jax.ShapeDtypeStruct((rows, D), jnp.bfloat16),
        cost_estimate=pl.CostEstimate(
            flops=6 * rows * D, bytes_accessed=4 * rows * D, transcendentals=rows
        ),
        compiler_params=pltpu.CompilerParams(vmem_limit_bytes=12 * MIB),
        name="norm",
    )(own, other, gain[None])


def over_group(mine, theirs):
    got = lax.ppermute(theirs, "c", SWAP)
    pair = (mine + got.astype(jnp.float32)).astype(jnp.bfloat16)
    return jnp.sum(lax.all_to_all(pair, "x", 0, 0, tiled=True).astype(jnp.float32), axis=0)


def feed_forward_kernel(x_ref, weight_ref, theirs_ref, mine_ref, up_ref, down_ref, hidden_ref, sems):
    core = lax.axis_index("c")
    count, _, width = mine_ref.shape
    steps = [slice(low, low + width) for low in range(0, up_ref.shape[1], width)]
    copies = [
        pltpu.make_async_copy(weight_ref.at[0, :, at], up_ref.at[:, at], sems.at[i])
        for i, at in enumerate(steps)
    ]
    copies.append(pltpu.make_async_copy(weight_ref.at[1], down_ref, sems.at[len(steps)]))
    for copy in copies:
        copy.start()
    for copy, at in zip(copies, steps):
        copy.wait()
        upward = jnp.dot(x_ref[...], up_ref[:, at], preferred_element_type=jnp.float32)
        hidden_ref[:, at] = jnp.square(jnp.maximum(upward, 0.0)).astype(jnp.bfloat16)
    copies[-1].wait()
    for out_ref, which in ((theirs_ref, 1 - core), (mine_ref, core)):
        for i in range(count):
            at = pl.ds(pl.multiple_of((2 * i + which) * width, width), width)
            out_ref[i] = times_t(hidden_ref[...], down_ref[at]).astype(out_ref.dtype)


def feed_forward(x, weights):
    rows = x.shape[0]
    hidden = weights.shape[2]
    width = D // 8
    out = (4, rows, width)
    vmem = pl.BlockSpec(memory_space=pltpu.VMEM)
    return pl.pallas_call(
        feed_forward_kernel,
        in_specs=[vmem, pl.BlockSpec(memory_space=pl.ANY)],
        out_specs=(vmem, vmem),
        out_shape=(
            jax.ShapeDtypeStruct(out, jnp.bfloat16),
            jax.ShapeDtypeStruct(out, jnp.float32),
        ),
        scratch_shapes=[
            pltpu.VMEM((D, hidden), jnp.bfloat16),
            pltpu.VMEM((D, hidden), jnp.bfloat16),
            pltpu.VMEM((rows, hidden), jnp.bfloat16),
            pltpu.SemaphoreType.DMA((hidden // width + 1,)),
        ],
        compiler_params=pltpu.CompilerParams(vmem_limit_bytes=50 * MIB),
        cost_estimate=pl.CostEstimate(
            flops=4 * rows * D * hidden, bytes_accessed=4 * D * hidden, transcendentals=0
        ),
        name="feed_forward",
    )(x, weights)


def body(
    states, mix_gain, w_value, w_gate, conv_kernel, chan_gain, w_mix_out, mlp_gain, w_up, w_down_t
):
    sent = jnp.where(lax.axis_index("rep") == 0, w_up, w_down_t)
    ffn = lax.all_gather(sent, ("rep", "zl", "y"), axis=0).reshape(2, -1, sent.shape[1])
    slabs = over_z(over_y(w_value, w_gate, w_mix_out))
    normed = normed_channels(states, mix_gain)
    filtered, sums = gated_filter(normed, conv_kernel, slabs)
    sums = lax.all_to_all(sums, TP, 0, 0, tiled=True)
    theirs, mine = mixer(filtered, sums, chan_gain, slabs)
    mixed = over_group(mine, theirs)
    middle = (states.astype(jnp.float32) + mixed).astype(jnp.bfloat16)
    normed_mid = normed_channels(middle, mlp_gain)
    theirs, mine = feed_forward(normed_mid, ffn)
    fed = over_group(mine, theirs)
    return (middle.astype(jnp.float32) + fed).astype(jnp.bfloat16)


def solution(mesh):
    split = Mesh(mesh.devices.reshape(2, 4, 8, 4, 2), ("rep", "zl", "y", "x", "c"))
    fs = ("zl", "y")
    return jax.shard_map(
        body,
        mesh=split,
        in_specs=(
            P(("rep", *fs), TP),
            P(),
            P(fs, TP),
            P(fs, TP),
            P(),
            P(),
            P(fs, TP),
            P(),
            P(fs, TP),
            P(fs, TP),
        ),
        out_specs=P(("rep", *fs), TP),
        check_vma=False,
    )
```

```python
import jax
import jax.numpy as jnp
from jax import lax
from jax.experimental import pallas as pl
from jax.experimental.pallas import tpu as pltpu
from jax.sharding import Mesh
from jax.sharding import PartitionSpec as P

D = 2048
KWIDTH = 31
LENGTH = 128
EPS = 1e-06
TP = ("x", "c")
SWAP = [(0, 1), (1, 0)]


MIB = 1 << 20
LANES = 128
LATE = 256


def times_t(left, right):
    return lax.dot_general(
        left, right, (((1,), (1,)), ((), ())), preferred_element_type=jnp.float32
    )


def pack_kernel(value_ref, gate_ref, out_ref, up_ref, down_ref, mix_ref, first_ref, late_ref):
    width, first = value_ref.shape[1], up_ref.shape[1] - LATE
    for i, ref in enumerate((value_ref, gate_ref, out_ref)):
        mix_ref[:, i * width : (i + 1) * width] = ref[...]
    first_ref[:, :first] = up_ref[:, :first]
    first_ref[:, first:] = down_ref[:, :first]
    parts = late_ref.shape[0] // 2
    for i in range(parts):
        at = first + i * LANES
        late_ref[i] = up_ref[:, at : at + LANES]
        late_ref[parts + i] = down_ref[:, at : at + LANES]


def packed(w_value, w_gate, w_mix_out, w_up, w_down_t):
    rows, width = w_value.shape
    first = w_up.shape[1] - LATE
    return pl.pallas_call(
        pack_kernel,
        out_shape=(
            jax.ShapeDtypeStruct((rows, 3 * width), jnp.bfloat16),
            jax.ShapeDtypeStruct((rows, 2 * first), jnp.bfloat16),
            jax.ShapeDtypeStruct((2 * LATE // LANES, rows, LANES), jnp.bfloat16),
        ),
        compiler_params=pltpu.CompilerParams(vmem_limit_bytes=60 * MIB),
        cost_estimate=pl.CostEstimate(flops=0, bytes_accessed=MIB, transcendentals=0),
        name="pack",
    )(w_value, w_gate, w_mix_out, w_up, w_down_t)


def over_y(run):
    return lax.all_gather(run, "y", axis=1, tiled=True)


def over_z(slab):
    half = slab.shape[1] // 2

    def from_z(piece, step):
        return lax.ppermute(piece, ("rep", "zl"), [((i + step) % 8, i) for i in range(8)])

    far = [from_z(slab[:, :half], 2), from_z(slab[:, half:], -2)]
    return [slab, from_z(slab, 1), *far, from_z(slab, -1)]


def gate_kernel(x_ref, taps_ref, weight_ref, filtered_ref, sums_ref, padded_ref, held_ref, sems):
    count, depth, width = held_ref.shape[0], held_ref.shape[1], held_ref.shape[2] // 2
    copies = [
        pltpu.make_async_copy(weight_ref.at[z, :, : 2 * width], held_ref.at[z], sems.at[z])
        for z in range(count)
    ]
    for copy in copies:
        copy.start()
    value, gate = 0.0, 0.0
    for z, copy in enumerate(copies):
        copy.wait()
        x = x_ref[:, z * depth : (z + 1) * depth]
        value += jnp.dot(x, held_ref[z, :, :width], preferred_element_type=jnp.float32)
        gate += jnp.dot(x, held_ref[z, :, width:], preferred_element_type=jnp.float32)
    gated = value * jax.nn.sigmoid(gate)
    pad = padded_ref.shape[1] - LENGTH
    sequences = padded_ref.shape[0]
    for s in range(sequences):
        padded_ref[s, :pad] = jnp.zeros((pad, width), jnp.float32)
        padded_ref[s, pad:] = gated[s * LENGTH : (s + 1) * LENGTH]
    first = lax.axis_index(TP) * width
    for lane in range(0, width, LANES):
        taps = taps_ref[:, pl.ds(pl.multiple_of(first + lane, LANES), LANES)]
        for s in range(sequences):
            total = jnp.zeros((LENGTH, LANES), jnp.float32)
            for shift in range(8):
                offsets = [o for o in range(pad - KWIDTH + 1, pad + 1) if o % 8 == shift]
                span = offsets[-1] - shift + LENGTH
                rows = padded_ref[s, shift : shift + span, lane : lane + LANES]
                for o in offsets:
                    tap = o - (pad - KWIDTH + 1)
                    total += taps[tap : tap + 1] * rows[o - shift : o - shift + LENGTH]
            filtered_ref[s * LENGTH : (s + 1) * LENGTH, lane : lane + LANES] = total
    filtered = filtered_ref[...]
    ones = jnp.ones((8, width), jnp.float32)
    rows = x_ref.shape[0]
    for i, terms in enumerate((filtered, filtered * filtered)):
        sums = lax.dot_general(
            ones,
            terms,
            (((1,), (1,)), ((), ())),
            precision=lax.Precision.HIGHEST,
            preferred_element_type=jnp.float32,
        )
        for copy in range(sums_ref.shape[0]):
            sums_ref[copy, :, i * rows : (i + 1) * rows] = sums[:1]


def gated_filter(x, taps, weights, width):
    rows = x.shape[0]
    count, depth, _ = weights.shape
    vmem = pl.BlockSpec(memory_space=pltpu.VMEM)
    return pl.pallas_call(
        gate_kernel,
        in_specs=[vmem, vmem, pl.BlockSpec(memory_space=pl.ANY)],
        out_specs=(vmem, vmem),
        out_shape=(
            jax.ShapeDtypeStruct((rows, width), jnp.float32),
            jax.ShapeDtypeStruct((lax.axis_size(TP), 1, 2 * rows), jnp.float32),
        ),
        scratch_shapes=[
            pltpu.VMEM((rows // LENGTH, LENGTH + 32, width), jnp.float32),
            pltpu.VMEM((count, depth, 2 * width), jnp.bfloat16),
            pltpu.SemaphoreType.DMA((count,)),
        ],
        compiler_params=pltpu.CompilerParams(vmem_limit_bytes=51 * MIB),
        cost_estimate=pl.CostEstimate(
            flops=4 * rows * D * width, bytes_accessed=4 * D * width, transcendentals=rows * width
        ),
        name="gated_filter",
    )(x, taps, weights)


def mixer_kernel(filtered_ref, sums_ref, gain_ref, weight_ref, theirs_ref, mine_ref, held_ref, sem):
    core = lax.axis_index("c")
    rows, width = filtered_ref.shape
    copy = pltpu.make_async_copy(weight_ref.at[:, :, 2 * width : 3 * width], held_ref, sem)
    copy.start()
    sums = sum(sums_ref[d] for d in range(sums_ref.shape[0])) / D
    mean = sums[:, :rows]
    scale = lax.rsqrt(sums[:, rows:] - mean * mean + EPS)

    def down_rows(row):
        column = jnp.broadcast_to(row, (LANES, rows)).T
        return jnp.concatenate([column] * (width // LANES), axis=1)

    gain = gain_ref[:, pl.ds(pl.multiple_of(lax.axis_index(TP) * width, width), width)]
    values = (filtered_ref[...] - down_rows(mean)) * down_rows(scale) * gain
    activated = (values / (1.0 + jnp.exp(-values))).astype(jnp.bfloat16)
    copy.wait()
    for out_ref, which in ((theirs_ref, 1 - core), (mine_ref, core)):
        at = pl.ds(pl.multiple_of(which * width, width), width)
        for z in range(held_ref.shape[0]):
            out_ref[z] = times_t(activated, held_ref[z, at]).astype(out_ref.dtype)


def mixer(filtered, sums, gain, weights):
    rows, width = filtered.shape
    count, depth, _ = weights.shape
    vmem = pl.BlockSpec(memory_space=pltpu.VMEM)
    out = (count, rows, width)
    return pl.pallas_call(
        mixer_kernel,
        in_specs=[vmem, vmem, vmem, pl.BlockSpec(memory_space=pl.ANY)],
        out_specs=(vmem, vmem),
        out_shape=(
            jax.ShapeDtypeStruct(out, jnp.bfloat16),
            jax.ShapeDtypeStruct(out, jnp.float32),
        ),
        scratch_shapes=[
            pltpu.VMEM((count, depth, width), jnp.bfloat16),
            pltpu.SemaphoreType.DMA,
        ],
        compiler_params=pltpu.CompilerParams(vmem_limit_bytes=51 * MIB),
        cost_estimate=pl.CostEstimate(
            flops=2 * rows * D * width, bytes_accessed=2 * D * width, transcendentals=rows * width
        ),
        name="mixer",
    )(filtered, sums, gain[None], weights)


def norm_kernel(own_ref, other_ref, gain_ref, out_ref):
    core = lax.axis_index("c")
    count, rows, width = own_ref.shape
    pieces = [(r[i].astype(jnp.float32), i, s) for s, r in enumerate((own_ref, other_ref)) for i in range(count)]
    total = sum(jnp.sum(v * v, axis=-1, keepdims=True) for v, _, _ in pieces)
    scale = lax.rsqrt(total / D + EPS)
    for values, i, side in pieces:
        which = core if side == 0 else 1 - core
        at = pl.ds(pl.multiple_of((2 * i + which) * width, width), width)
        out_ref[:, at] = (values * scale * gain_ref[:, at]).astype(jnp.bfloat16)


def normed_channels(block, gain, beside=()):
    own = lax.all_gather(block, "x", axis=0)
    if beside:
        own, beside = lax.optimization_barrier((own, beside))
    other = lax.ppermute(own, "c", SWAP)
    count, rows, width = own.shape
    part = pl.BlockSpec((count, LENGTH, width), lambda i: (0, i, 0))
    return pl.pallas_call(
        norm_kernel,
        grid=(rows // LENGTH,),
        in_specs=[part, part, pl.BlockSpec((1, D), lambda i: (0, 0))],
        out_specs=pl.BlockSpec((LENGTH, D), lambda i: (i, 0)),
        out_shape=jax.ShapeDtypeStruct((rows, D), jnp.bfloat16),
        cost_estimate=pl.CostEstimate(
            flops=6 * rows * D, bytes_accessed=4 * rows * D, transcendentals=rows
        ),
        compiler_params=pltpu.CompilerParams(vmem_limit_bytes=12 * MIB),
        name="norm",
    )(own, other, gain[None]), beside


def over_group(mine, theirs):
    got = lax.ppermute(theirs, "c", SWAP)
    pair = (mine + got.astype(jnp.float32)).astype(jnp.bfloat16)
    return jnp.sum(lax.all_to_all(pair, "x", 0, 0, tiled=True).astype(jnp.float32), axis=0)


def feed_forward_kernel(x_ref, first_ref, *refs):
    *slab_refs, theirs_ref, mine_ref, up_ref, down_ref, hidden_ref, sems = refs
    core, here = lax.axis_index("c"), lax.axis_index("zl")
    count, depth, columns = up_ref.shape
    width, parts = depth // 2, LATE // LANES
    steps = [slice(low, low + width) for low in range(0, columns, width)]
    copies = [
        pltpu.make_async_copy(first_ref.at[:, :, at], up_ref.at[:, :, at], sems.at[i])
        for i, at in enumerate(steps)
    ]
    down = first_ref.at[:, :, columns:]
    copies.append(pltpu.make_async_copy(down, down_ref, sems.at[len(steps)]))
    for copy in copies:
        copy.start()

    def squared_relu(upward):
        return jnp.square(jnp.maximum(upward, 0.0)).astype(jnp.bfloat16)

    def joined(ref, first, rows=slice(None)):
        return jnp.concatenate([ref[first + i, rows] for i in range(parts)], axis=1)

    upward = 0.0
    for ref, turn, low in zip(slab_refs, (0, 1, 2, 2, 3), (0, 0, 0, width, 0)):
        start = lax.rem(here + turn, count) * depth + low
        x = x_ref[:, pl.ds(pl.multiple_of(start, width), ref.shape[1])]
        upward += jnp.dot(x, joined(ref, 0), preferred_element_type=jnp.float32)
    hidden_ref[:, columns:] = squared_relu(upward)
    for copy, at in zip(copies, steps):
        copy.wait()
        upward = 0.0
        for z in range(count):
            x = x_ref[:, z * depth : (z + 1) * depth]
            upward += jnp.dot(x, up_ref[z, :, at], preferred_element_type=jnp.float32)
        hidden_ref[:, at] = squared_relu(upward)
    copies[-1].wait()
    near, one, low, high, three = slab_refs
    for out_ref, which in ((theirs_ref, 1 - core), (mine_ref, core)):
        rows = pl.ds(pl.multiple_of(which * width, width), width)
        for turn, ref in ((0, near), (1, one), (2, None), (3, three)):
            z = lax.rem(here + turn, count)
            if ref is None:
                late = jnp.where(which == 0, joined(low, parts), joined(high, parts))
            else:
                late = joined(ref, parts, rows)
            part = times_t(hidden_ref[:, :columns], down_ref[z, rows])
            out_ref[z] = (part + times_t(hidden_ref[:, columns:], late)).astype(out_ref.dtype)


def feed_forward(x, first, late):
    rows = x.shape[0]
    count, depth, columns = first.shape
    columns //= 2
    width = depth // 2
    out = (count, rows, width)
    vmem = pl.BlockSpec(memory_space=pltpu.VMEM)
    weights = pltpu.VMEM((count, depth, columns), jnp.bfloat16)
    hidden = columns + LATE
    return pl.pallas_call(
        feed_forward_kernel,
        in_specs=[vmem, pl.BlockSpec(memory_space=pl.ANY), *(vmem for _ in late)],
        out_specs=(vmem, vmem),
        out_shape=(
            jax.ShapeDtypeStruct(out, jnp.bfloat16),
            jax.ShapeDtypeStruct(out, jnp.float32),
        ),
        scratch_shapes=[
            weights,
            weights,
            pltpu.VMEM((rows, hidden), jnp.bfloat16),
            pltpu.SemaphoreType.DMA((columns // width + 1,)),
        ],
        compiler_params=pltpu.CompilerParams(vmem_limit_bytes=46 * MIB),
        cost_estimate=pl.CostEstimate(
            flops=4 * rows * D * hidden, bytes_accessed=4 * D * hidden, transcendentals=0
        ),
        name="feed_forward",
    )(x, first, *late)


def body(
    states, mix_gain, w_value, w_gate, conv_kernel, chan_gain, w_mix_out, mlp_gain, w_up, w_down_t
):
    width = states.shape[1]
    early, first, late = packed(w_value, w_gate, w_mix_out, w_up, w_down_t)
    run = lax.all_gather(early, "zl", axis=0)
    mix = over_y(jnp.concatenate([run, late], axis=2))
    normed, _ = normed_channels(states, mix_gain)
    ffn_first = over_y(lax.all_gather(first, "zl", axis=0))
    ffn_late = over_z(mix[:, :, 3 * width :])
    filtered, sums = gated_filter(normed, conv_kernel, mix, width)
    sums = lax.all_to_all(sums, TP, 0, 0, tiled=True)
    theirs, mine = mixer(filtered, sums, chan_gain, mix)
    mixed = over_group(mine, theirs)
    middle = (states.astype(jnp.float32) + mixed).astype(jnp.bfloat16)
    normed_mid, ffn_late = normed_channels(middle, mlp_gain, ffn_late)
    theirs, mine = feed_forward(normed_mid, ffn_first, ffn_late)
    fed = over_group(mine, theirs)
    return (middle.astype(jnp.float32) + fed).astype(jnp.bfloat16)


def solution(mesh):
    split = Mesh(mesh.devices.reshape(2, 4, 8, 4, 2), ("rep", "zl", "y", "x", "c"))
    fs = ("zl", "y")
    return jax.shard_map(
        body,
        mesh=split,
        in_specs=(
            P(("rep", *fs), TP),
            P(),
            P(fs, TP),
            P(fs, TP),
            P(),
            P(),
            P(fs, TP),
            P(),
            P(fs, TP),
            P(fs, TP),
        ),
        out_specs=P(("rep", *fs), TP),
        check_vma=False,
    )
```

```python
import jax
import jax.numpy as jnp
from jax import lax
from jax.experimental import pallas as pl
from jax.experimental.pallas import tpu as pltpu
from jax.sharding import Mesh
from jax.sharding import PartitionSpec as P

D = 2048
KWIDTH = 31
LENGTH = 128
EPS = 1e-06
TP = ("x", "c")
SWAP = [(0, 1), (1, 0)]


MIB = 1 << 20
LANES = 128
LATE = 256


def times_t(left, right):
    return lax.dot_general(
        left, right, (((1,), (1,)), ((), ())), preferred_element_type=jnp.float32
    )


def pack_kernel(value_ref, gate_ref, out_ref, up_ref, down_ref, mix_ref, first_ref, late_ref):
    width, first = value_ref.shape[1], up_ref.shape[1] - LATE
    for i, ref in enumerate((value_ref, gate_ref, out_ref)):
        mix_ref[:, i * width : (i + 1) * width] = ref[...]
    first_ref[:, :first] = up_ref[:, :first]
    first_ref[:, first:] = down_ref[:, :first]
    parts = late_ref.shape[0] // 2
    for i in range(parts):
        at = first + i * LANES
        late_ref[i] = up_ref[:, at : at + LANES]
        late_ref[parts + i] = down_ref[:, at : at + LANES]


def packed(w_value, w_gate, w_mix_out, w_up, w_down_t):
    rows, width = w_value.shape
    first = w_up.shape[1] - LATE
    return pl.pallas_call(
        pack_kernel,
        out_shape=(
            jax.ShapeDtypeStruct((rows, 3 * width), jnp.bfloat16),
            jax.ShapeDtypeStruct((rows, 2 * first), jnp.bfloat16),
            jax.ShapeDtypeStruct((2 * LATE // LANES, rows, LANES), jnp.bfloat16),
        ),
        compiler_params=pltpu.CompilerParams(vmem_limit_bytes=60 * MIB),
        cost_estimate=pl.CostEstimate(flops=0, bytes_accessed=MIB, transcendentals=0),
        name="pack",
    )(w_value, w_gate, w_mix_out, w_up, w_down_t)


def over_y(run):
    return lax.all_gather(run, "y", axis=1, tiled=True)


def from_z(piece, step):
    return lax.ppermute(piece, ("rep", "zl"), [((i + step) % 8, i) for i in range(8)])


def gate_kernel(
    x_ref, taps_ref, weight_ref, filtered_ref, sums_ref, out_ref, *refs
):
    *late_refs, padded_ref, held_ref, sems = refs
    count, depth, width = held_ref.shape[0], held_ref.shape[1], held_ref.shape[2] // 2
    copies = [
        pltpu.make_async_copy(weight_ref.at[z, :, : 2 * width], held_ref.at[z], sems.at[z])
        for z in range(count)
    ]
    late = weight_ref.at[:, :, 3 * width :]
    parts = [late, late.at[:, : depth // 2], late.at[:, depth // 2 :]]
    parts.append(weight_ref.at[:, :, 2 * width : 3 * width])
    for i, (part, ref) in enumerate(zip(parts, (*late_refs, out_ref))):
        copies.append(pltpu.make_async_copy(part, ref, sems.at[count + i]))
    for copy in copies:
        copy.start()
    value, gate = 0.0, 0.0
    for z, copy in enumerate(copies[:count]):
        copy.wait()
        x = x_ref[:, z * depth : (z + 1) * depth]
        value += jnp.dot(x, held_ref[z, :, :width], preferred_element_type=jnp.float32)
        gate += jnp.dot(x, held_ref[z, :, width:], preferred_element_type=jnp.float32)
    gated = value * jax.nn.sigmoid(gate)
    pad = padded_ref.shape[1] - LENGTH
    sequences = padded_ref.shape[0]
    for s in range(sequences):
        padded_ref[s, :pad] = jnp.zeros((pad, width), jnp.float32)
        padded_ref[s, pad:] = gated[s * LENGTH : (s + 1) * LENGTH]
    first = lax.axis_index(TP) * width
    for lane in range(0, width, LANES):
        taps = taps_ref[:, pl.ds(pl.multiple_of(first + lane, LANES), LANES)]
        for s in range(sequences):
            total = jnp.zeros((LENGTH, LANES), jnp.float32)
            for shift in range(8):
                offsets = [o for o in range(pad - KWIDTH + 1, pad + 1) if o % 8 == shift]
                span = offsets[-1] - shift + LENGTH
                rows = padded_ref[s, shift : shift + span, lane : lane + LANES]
                for o in offsets:
                    tap = o - (pad - KWIDTH + 1)
                    total += taps[tap : tap + 1] * rows[o - shift : o - shift + LENGTH]
            filtered_ref[s * LENGTH : (s + 1) * LENGTH, lane : lane + LANES] = total
    filtered = filtered_ref[...]
    ones = jnp.ones((8, width), jnp.float32)
    rows = x_ref.shape[0]
    for i, terms in enumerate((filtered, filtered * filtered)):
        sums = lax.dot_general(
            ones,
            terms,
            (((1,), (1,)), ((), ())),
            precision=lax.Precision.HIGHEST,
            preferred_element_type=jnp.float32,
        )
        for d in range(sums_ref.shape[0]):
            sums_ref[d, :, i * rows : (i + 1) * rows] = sums[:1]
    for copy in copies[count:]:
        copy.wait()


def gated_filter(x, taps, weights, width):
    rows = x.shape[0]
    count, depth, columns = weights.shape
    late = columns - 3 * width
    vmem = pl.BlockSpec(memory_space=pltpu.VMEM)
    return pl.pallas_call(
        gate_kernel,
        in_specs=[vmem, vmem, pl.BlockSpec(memory_space=pl.ANY)],
        out_specs=(vmem,) * 6,
        out_shape=(
            jax.ShapeDtypeStruct((rows, width), jnp.float32),
            jax.ShapeDtypeStruct((lax.axis_size(TP), 1, 2 * rows), jnp.float32),
            jax.ShapeDtypeStruct((count, depth, width), jnp.bfloat16),
            jax.ShapeDtypeStruct((count, depth, late), jnp.bfloat16),
            jax.ShapeDtypeStruct((count, depth // 2, late), jnp.bfloat16),
            jax.ShapeDtypeStruct((count, depth // 2, late), jnp.bfloat16),
        ),
        scratch_shapes=[
            pltpu.VMEM((rows // LENGTH, LENGTH + 32, width), jnp.float32),
            pltpu.VMEM((count, depth, 2 * width), jnp.bfloat16),
            pltpu.SemaphoreType.DMA((count + 4,)),
        ],
        compiler_params=pltpu.CompilerParams(vmem_limit_bytes=51 * MIB),
        cost_estimate=pl.CostEstimate(
            flops=4 * rows * D * width, bytes_accessed=4 * D * width, transcendentals=rows * width
        ),
        name="gated_filter",
    )(x, taps, weights)


def mixer_kernel(filtered_ref, sums_ref, gain_ref, weight_ref, theirs_ref, mine_ref):
    core = lax.axis_index("c")
    rows, width = filtered_ref.shape
    sums = sum(sums_ref[d] for d in range(sums_ref.shape[0])) / D
    mean = sums[:, :rows]
    scale = lax.rsqrt(sums[:, rows:] - mean * mean + EPS)

    def down_rows(row):
        column = jnp.broadcast_to(row, (LANES, rows)).T
        return jnp.concatenate([column] * (width // LANES), axis=1)

    gain = gain_ref[:, pl.ds(pl.multiple_of(lax.axis_index(TP) * width, width), width)]
    values = (filtered_ref[...] - down_rows(mean)) * down_rows(scale) * gain
    activated = (values / (1.0 + jnp.exp(-values))).astype(jnp.bfloat16)
    for out_ref, which in ((theirs_ref, 1 - core), (mine_ref, core)):
        at = pl.ds(pl.multiple_of(which * width, width), width)
        for z in range(weight_ref.shape[0]):
            out_ref[z] = times_t(activated, weight_ref[z, at]).astype(out_ref.dtype)


def mixer(filtered, sums, gain, weights):
    rows, width = filtered.shape
    vmem = pl.BlockSpec(memory_space=pltpu.VMEM)
    out = (weights.shape[0], rows, width)
    return pl.pallas_call(
        mixer_kernel,
        in_specs=[vmem] * 4,
        out_specs=(vmem, vmem),
        out_shape=(
            jax.ShapeDtypeStruct(out, jnp.bfloat16),
            jax.ShapeDtypeStruct(out, jnp.float32),
        ),
        compiler_params=pltpu.CompilerParams(vmem_limit_bytes=24 * MIB),
        cost_estimate=pl.CostEstimate(
            flops=2 * rows * D * width, bytes_accessed=2 * D * width, transcendentals=rows * width
        ),
        name="mixer",
    )(filtered, sums, gain[None], weights)


def norm_kernel(own_ref, other_ref, gain_ref, out_ref):
    core = lax.axis_index("c")
    count, _, width = own_ref.shape
    pieces = [(r[i].astype(jnp.float32), i, s) for s, r in enumerate((own_ref, other_ref)) for i in range(count)]
    total = sum(jnp.sum(v * v, axis=-1, keepdims=True) for v, _, _ in pieces)
    scale = lax.rsqrt(total / D + EPS)
    for values, i, side in pieces:
        which = core if side == 0 else 1 - core
        at = pl.ds(pl.multiple_of((2 * i + which) * width, width), width)
        out_ref[:, at] = (values * scale * gain_ref[:, at]).astype(jnp.bfloat16)


def normed_channels(block, gain, beside=()):
    own = lax.all_gather(block, "x", axis=0)
    if beside:
        own, beside = lax.optimization_barrier((own, beside))
    other = lax.ppermute(own, "c", SWAP)
    count, rows, width = own.shape
    part = pl.BlockSpec((count, LENGTH, width), lambda i: (0, i, 0))
    return pl.pallas_call(
        norm_kernel,
        grid=(rows // LENGTH,),
        in_specs=[part, part, pl.BlockSpec((1, D), lambda i: (0, 0))],
        out_specs=pl.BlockSpec((LENGTH, D), lambda i: (i, 0)),
        out_shape=jax.ShapeDtypeStruct((rows, D), jnp.bfloat16),
        cost_estimate=pl.CostEstimate(
            flops=6 * rows * D, bytes_accessed=4 * rows * D, transcendentals=rows
        ),
        compiler_params=pltpu.CompilerParams(vmem_limit_bytes=12 * MIB),
        name="norm",
    )(own, other, gain[None]), beside


def over_group(mine, theirs):
    got = lax.ppermute(theirs, "c", SWAP)
    pair = (mine + got.astype(jnp.float32)).astype(jnp.bfloat16)
    return jnp.sum(lax.all_to_all(pair, "x", 0, 0, tiled=True).astype(jnp.float32), axis=0)


def feed_forward_kernel(x_ref, first_ref, *refs):
    *slab_refs, theirs_ref, mine_ref, up_ref, down_ref, hidden_ref, sems = refs
    core, here = lax.axis_index("c"), lax.axis_index("zl")
    count, depth, columns = up_ref.shape
    width, parts = depth // 2, LATE // LANES
    steps = [slice(low, low + width) for low in range(0, columns, width)]
    copies = [
        pltpu.make_async_copy(first_ref.at[:, :, at], up_ref.at[:, :, at], sems.at[i])
        for i, at in enumerate(steps)
    ]
    down = first_ref.at[:, :, columns:]
    copies.append(pltpu.make_async_copy(down, down_ref, sems.at[len(steps)]))
    for copy in copies:
        copy.start()

    def squared_relu(upward):
        return jnp.square(jnp.maximum(upward, 0.0)).astype(jnp.bfloat16)

    def joined(ref, first, rows=slice(None)):
        return jnp.concatenate([ref[first + i, rows] for i in range(parts)], axis=1)

    upward = 0.0
    for ref, turn, low in zip(slab_refs, (0, 1, 2, 2, 3), (0, 0, 0, width, 0)):
        start = lax.rem(here + turn, count) * depth + low
        x = x_ref[:, pl.ds(pl.multiple_of(start, width), ref.shape[1])]
        upward += jnp.dot(x, joined(ref, 0), preferred_element_type=jnp.float32)
    hidden_ref[:, columns:] = squared_relu(upward)
    for copy, at in zip(copies, steps):
        copy.wait()
        upward = 0.0
        for z in range(count):
            x = x_ref[:, z * depth : (z + 1) * depth]
            upward += jnp.dot(x, up_ref[z, :, at], preferred_element_type=jnp.float32)
        hidden_ref[:, at] = squared_relu(upward)
    copies[-1].wait()
    near, one, low, high, three = slab_refs
    for out_ref, which in ((theirs_ref, 1 - core), (mine_ref, core)):
        rows = pl.ds(pl.multiple_of(which * width, width), width)
        for turn, ref in ((0, near), (1, one), (2, None), (3, three)):
            z = lax.rem(here + turn, count)
            if ref is None:
                late = jnp.where(which == 0, joined(low, parts), joined(high, parts))
            else:
                late = joined(ref, parts, rows)
            part = times_t(hidden_ref[:, :columns], down_ref[z, rows])
            out_ref[z] = (part + times_t(hidden_ref[:, columns:], late)).astype(out_ref.dtype)


def feed_forward(x, first, late):
    rows = x.shape[0]
    count, depth, columns = first.shape
    columns //= 2
    width = depth // 2
    out = (count, rows, width)
    vmem = pl.BlockSpec(memory_space=pltpu.VMEM)
    weights = pltpu.VMEM((count, depth, columns), jnp.bfloat16)
    hidden = columns + LATE
    return pl.pallas_call(
        feed_forward_kernel,
        in_specs=[vmem, pl.BlockSpec(memory_space=pl.ANY), *(vmem for _ in late)],
        out_specs=(vmem, vmem),
        out_shape=(
            jax.ShapeDtypeStruct(out, jnp.bfloat16),
            jax.ShapeDtypeStruct(out, jnp.float32),
        ),
        scratch_shapes=[
            weights,
            weights,
            pltpu.VMEM((rows, hidden), jnp.bfloat16),
            pltpu.SemaphoreType.DMA((columns // width + 1,)),
        ],
        compiler_params=pltpu.CompilerParams(vmem_limit_bytes=46 * MIB),
        cost_estimate=pl.CostEstimate(
            flops=4 * rows * D * hidden, bytes_accessed=4 * D * hidden, transcendentals=0
        ),
        name="feed_forward",
    )(x, first, *late)


def body(
    states, mix_gain, w_value, w_gate, conv_kernel, chan_gain, w_mix_out, mlp_gain, w_up, w_down_t
):
    width = states.shape[1]
    early, first, late = packed(w_value, w_gate, w_mix_out, w_up, w_down_t)
    run = lax.all_gather(early, "zl", axis=0)
    mix = over_y(jnp.concatenate([run, late], axis=2))
    normed, _ = normed_channels(states, mix_gain)
    ffn_first = over_y(lax.all_gather(first, "zl", axis=0))
    filtered, sums, w_out, near, low, high = gated_filter(normed, conv_kernel, mix, width)
    sums = lax.all_to_all(sums, TP, 0, 0, tiled=True)
    low = from_z(low, 2)
    high = from_z(high, -2)
    sums, low, high = lax.optimization_barrier((sums, low, high))
    ffn_late = (near, from_z(near, 1), low, high, from_z(near, -1))
    theirs, mine = mixer(filtered, sums, chan_gain, w_out)
    mixed = over_group(mine, theirs)
    middle = (states.astype(jnp.float32) + mixed).astype(jnp.bfloat16)
    normed_mid, ffn_late = normed_channels(middle, mlp_gain, ffn_late)
    theirs, mine = feed_forward(normed_mid, ffn_first, ffn_late)
    fed = over_group(mine, theirs)
    return (middle.astype(jnp.float32) + fed).astype(jnp.bfloat16)


def solution(mesh):
    split = Mesh(mesh.devices.reshape(2, 4, 8, 4, 2), ("rep", "zl", "y", "x", "c"))
    fs = ("zl", "y")
    return jax.shard_map(
        body,
        mesh=split,
        in_specs=(
            P(("rep", *fs), TP),
            P(),
            P(fs, TP),
            P(fs, TP),
            P(),
            P(),
            P(fs, TP),
            P(),
            P(fs, TP),
            P(fs, TP),
        ),
        out_specs=P(("rep", *fs), TP),
        check_vma=False,
    )
```

```python
import jax
import jax.numpy as jnp
from jax import lax
from jax.experimental import pallas as pl
from jax.experimental.pallas import tpu as pltpu
from jax.sharding import Mesh
from jax.sharding import PartitionSpec as P

D = 2048
KWIDTH = 31
LENGTH = 128
EPS = 1e-06
TP = ("x", "c")
SWAP = [(0, 1), (1, 0)]


MIB = 1 << 20
LANES = 128
LATE = 256


def times_t(left, right):
    return lax.dot_general(
        left, right, (((1,), (1,)), ((), ())), preferred_element_type=jnp.float32
    )


def pack_kernel(value_ref, gate_ref, out_ref, up_ref, down_ref, early_ref, late_ref):
    width, first = value_ref.shape[1], up_ref.shape[1] - LATE
    at = 0
    for ref, count in ((value_ref, width), (gate_ref, width), (up_ref, first), (down_ref, first)):
        early_ref[:, at : at + count] = ref[:, :count]
        at += count
    for copy in range(late_ref.shape[0]):
        late_ref[copy, :, :width] = out_ref[...]
        late_ref[copy, :, width : width + LATE] = up_ref[:, first:]
        late_ref[copy, :, width + LATE :] = down_ref[:, first:]


def packed(w_value, w_gate, w_mix_out, w_up, w_down_t):
    rows, width = w_value.shape
    first = w_up.shape[1] - LATE
    return pl.pallas_call(
        pack_kernel,
        out_shape=(
            jax.ShapeDtypeStruct((rows, 2 * (width + first)), jnp.bfloat16),
            jax.ShapeDtypeStruct((lax.axis_size("y"), rows, width + 2 * LATE), jnp.bfloat16),
        ),
        compiler_params=pltpu.CompilerParams(vmem_limit_bytes=60 * MIB),
        cost_estimate=pl.CostEstimate(flops=0, bytes_accessed=MIB, transcendentals=0),
        name="pack",
    )(w_value, w_gate, w_mix_out, w_up, w_down_t)


def over_y(run):
    return lax.all_gather(run, "y", axis=1, tiled=True)


def over_z(slab):
    half = slab.shape[0] // 2

    def from_z(piece, step):
        return lax.ppermute(piece, ("rep", "zl"), [((i + step) % 8, i) for i in range(8)])

    return [slab, from_z(slab, 1), from_z(slab[:half], 2), from_z(slab[half:], -2), from_z(slab, -1)]


def gate_kernel(x_ref, taps_ref, weight_ref, filtered_ref, sums_ref, padded_ref, held_ref, sems):
    count, depth, width = held_ref.shape[0], held_ref.shape[1], held_ref.shape[2] // 2
    copies = [
        pltpu.make_async_copy(weight_ref.at[z, :, : 2 * width], held_ref.at[z], sems.at[z])
        for z in range(count)
    ]
    for copy in copies:
        copy.start()
    value, gate = 0.0, 0.0
    for z, copy in enumerate(copies):
        copy.wait()
        x = x_ref[:, z * depth : (z + 1) * depth]
        value += jnp.dot(x, held_ref[z, :, :width], preferred_element_type=jnp.float32)
        gate += jnp.dot(x, held_ref[z, :, width:], preferred_element_type=jnp.float32)
    gated = value * jax.nn.sigmoid(gate)
    pad = padded_ref.shape[1] - LENGTH
    sequences = padded_ref.shape[0]
    for s in range(sequences):
        padded_ref[s, :pad] = jnp.zeros((pad, width), jnp.float32)
        padded_ref[s, pad:] = gated[s * LENGTH : (s + 1) * LENGTH]
    first = lax.axis_index(TP) * width
    for lane in range(0, width, LANES):
        taps = taps_ref[:, pl.ds(pl.multiple_of(first + lane, LANES), LANES)]
        for s in range(sequences):
            total = jnp.zeros((LENGTH, LANES), jnp.float32)
            for shift in range(8):
                offsets = [o for o in range(pad - KWIDTH + 1, pad + 1) if o % 8 == shift]
                span = offsets[-1] - shift + LENGTH
                rows = padded_ref[s, shift : shift + span, lane : lane + LANES]
                for o in offsets:
                    tap = o - (pad - KWIDTH + 1)
                    total += taps[tap : tap + 1] * rows[o - shift : o - shift + LENGTH]
            filtered_ref[s * LENGTH : (s + 1) * LENGTH, lane : lane + LANES] = total
    filtered = filtered_ref[...]
    ones = jnp.ones((8, width), jnp.float32)
    rows = x_ref.shape[0]
    for i, terms in enumerate((filtered, filtered * filtered)):
        sums = lax.dot_general(
            ones,
            terms,
            (((1,), (1,)), ((), ())),
            precision=lax.Precision.HIGHEST,
            preferred_element_type=jnp.float32,
        )
        for copy in range(sums_ref.shape[0]):
            sums_ref[copy, :, i * rows : (i + 1) * rows] = sums[:1]


def gated_filter(x, taps, weights, width):
    rows = x.shape[0]
    count, depth, _ = weights.shape
    vmem = pl.BlockSpec(memory_space=pltpu.VMEM)
    return pl.pallas_call(
        gate_kernel,
        in_specs=[vmem, vmem, pl.BlockSpec(memory_space=pl.ANY)],
        out_specs=(vmem, vmem),
        out_shape=(
            jax.ShapeDtypeStruct((rows, width), jnp.float32),
            jax.ShapeDtypeStruct((lax.axis_size(TP), 1, 2 * rows), jnp.float32),
        ),
        scratch_shapes=[
            pltpu.VMEM((rows // LENGTH, LENGTH + 32, width), jnp.float32),
            pltpu.VMEM((count, depth, 2 * width), jnp.bfloat16),
            pltpu.SemaphoreType.DMA((count,)),
        ],
        compiler_params=pltpu.CompilerParams(vmem_limit_bytes=51 * MIB),
        cost_estimate=pl.CostEstimate(
            flops=4 * rows * D * width, bytes_accessed=4 * D * width, transcendentals=rows * width
        ),
        name="gated_filter",
    )(x, taps, weights)


def mixer_kernel(filtered_ref, sums_ref, gain_ref, *refs):
    *slab_refs, theirs_ref, mine_ref = refs
    core, here, count = lax.axis_index("c"), lax.axis_index("zl"), lax.axis_size("zl")
    rows, width = filtered_ref.shape
    sums = sum(sums_ref[d] for d in range(sums_ref.shape[0])) / D
    mean = sums[:, :rows]
    scale = lax.rsqrt(sums[:, rows:] - mean * mean + EPS)

    def down_rows(row):
        column = jnp.broadcast_to(row, (LANES, rows)).T
        return jnp.concatenate([column] * (width // LANES), axis=1)

    gain = gain_ref[:, pl.ds(pl.multiple_of(lax.axis_index(TP) * width, width), width)]
    values = (filtered_ref[...] - down_rows(mean)) * down_rows(scale) * gain
    activated = (values / (1.0 + jnp.exp(-values))).astype(jnp.bfloat16)
    near, one, low, high, three = slab_refs
    for turn, ref in ((0, near), (1, one), (2, None), (3, three)):
        z = lax.rem(here + turn, count)
        for out_ref, which in ((theirs_ref, 1 - core), (mine_ref, core)):
            if ref is None:
                weight = jnp.where(which == 0, low[:, :width], high[:, :width])
            else:
                weight = ref[pl.ds(pl.multiple_of(which * width, width), width), :width]
            out_ref[z] = times_t(activated, weight).astype(out_ref.dtype)


def mixer(filtered, sums, gain, slabs):
    rows, width = filtered.shape
    vmem = pl.BlockSpec(memory_space=pltpu.VMEM)
    out = (lax.axis_size("zl"), rows, width)
    return pl.pallas_call(
        mixer_kernel,
        in_specs=[vmem] * (3 + len(slabs)),
        out_specs=(vmem, vmem),
        out_shape=(
            jax.ShapeDtypeStruct(out, jnp.bfloat16),
            jax.ShapeDtypeStruct(out, jnp.float32),
        ),
        compiler_params=pltpu.CompilerParams(vmem_limit_bytes=24 * MIB),
        cost_estimate=pl.CostEstimate(
            flops=2 * rows * D * width, bytes_accessed=2 * D * width, transcendentals=rows * width
        ),
        name="mixer",
    )(filtered, sums, gain[None], *slabs)


def norm_kernel(own_ref, other_ref, gain_ref, out_ref):
    core = lax.axis_index("c")
    count, _, width = own_ref.shape
    pieces = [(r[i].astype(jnp.float32), i, s) for s, r in enumerate((own_ref, other_ref)) for i in range(count)]
    total = sum(jnp.sum(v * v, axis=-1, keepdims=True) for v, _, _ in pieces)
    scale = lax.rsqrt(total / D + EPS)
    for values, i, side in pieces:
        which = core if side == 0 else 1 - core
        at = pl.ds(pl.multiple_of((2 * i + which) * width, width), width)
        out_ref[:, at] = (values * scale * gain_ref[:, at]).astype(jnp.bfloat16)


def normed_channels(block, gain):
    own = lax.all_gather(block, "x", axis=0)
    other = lax.ppermute(own, "c", SWAP)
    count, rows, width = own.shape
    part = pl.BlockSpec((count, LENGTH, width), lambda i: (0, i, 0))
    return pl.pallas_call(
        norm_kernel,
        grid=(rows // LENGTH,),
        in_specs=[part, part, pl.BlockSpec((1, D), lambda i: (0, 0))],
        out_specs=pl.BlockSpec((LENGTH, D), lambda i: (i, 0)),
        out_shape=jax.ShapeDtypeStruct((rows, D), jnp.bfloat16),
        cost_estimate=pl.CostEstimate(
            flops=6 * rows * D, bytes_accessed=4 * rows * D, transcendentals=rows
        ),
        compiler_params=pltpu.CompilerParams(vmem_limit_bytes=12 * MIB),
        name="norm",
    )(own, other, gain[None])


def over_group(mine, theirs):
    got = lax.ppermute(theirs, "c", SWAP)
    pair = (mine + got.astype(jnp.float32)).astype(jnp.bfloat16)
    return jnp.sum(lax.all_to_all(pair, "x", 0, 0, tiled=True).astype(jnp.float32), axis=0)


def feed_forward_kernel(x_ref, first_ref, *refs):
    *slab_refs, theirs_ref, mine_ref, up_ref, down_ref, hidden_ref, sems = refs
    core, here = lax.axis_index("c"), lax.axis_index("zl")
    count, depth, columns = up_ref.shape
    width = depth // 2
    up_at, down_at = slice(width, width + LATE), slice(width + LATE, width + 2 * LATE)
    steps = [slice(low, low + width) for low in range(0, columns, width)]
    copies = [
        pltpu.make_async_copy(first_ref.at[:, :, at], up_ref.at[:, :, at], sems.at[i])
        for i, at in enumerate(steps)
    ]
    down = first_ref.at[:, :, columns:]
    copies.append(pltpu.make_async_copy(down, down_ref, sems.at[len(steps)]))
    for copy in copies:
        copy.start()

    def squared_relu(upward):
        return jnp.square(jnp.maximum(upward, 0.0)).astype(jnp.bfloat16)

    upward = 0.0
    for ref, turn, low in zip(slab_refs, (0, 1, 2, 2, 3), (0, 0, 0, width, 0)):
        start = lax.rem(here + turn, count) * depth + low
        x = x_ref[:, pl.ds(pl.multiple_of(start, width), ref.shape[0])]
        upward += jnp.dot(x, ref[:, up_at], preferred_element_type=jnp.float32)
    hidden_ref[:, columns:] = squared_relu(upward)
    for copy, at in zip(copies, steps):
        copy.wait()
        upward = 0.0
        for z in range(count):
            x = x_ref[:, z * depth : (z + 1) * depth]
            upward += jnp.dot(x, up_ref[z, :, at], preferred_element_type=jnp.float32)
        hidden_ref[:, at] = squared_relu(upward)
    copies[-1].wait()
    near, one, low, high, three = slab_refs
    for out_ref, which in ((theirs_ref, 1 - core), (mine_ref, core)):
        rows = pl.ds(pl.multiple_of(which * width, width), width)
        for turn, ref in ((0, near), (1, one), (2, None), (3, three)):
            z = lax.rem(here + turn, count)
            if ref is None:
                late = jnp.where(which == 0, low[:, down_at], high[:, down_at])
            else:
                late = ref[rows, down_at]
            part = times_t(hidden_ref[:, :columns], down_ref[z, rows])
            out_ref[z] = (part + times_t(hidden_ref[:, columns:], late)).astype(out_ref.dtype)


def feed_forward(x, first, late):
    rows = x.shape[0]
    count, depth, columns = first.shape
    columns //= 2
    width = depth // 2
    out = (count, rows, width)
    vmem = pl.BlockSpec(memory_space=pltpu.VMEM)
    weights = pltpu.VMEM((count, depth, columns), jnp.bfloat16)
    hidden = columns + LATE
    return pl.pallas_call(
        feed_forward_kernel,
        in_specs=[vmem, pl.BlockSpec(memory_space=pl.ANY), *(vmem for _ in late)],
        out_specs=(vmem, vmem),
        out_shape=(
            jax.ShapeDtypeStruct(out, jnp.bfloat16),
            jax.ShapeDtypeStruct(out, jnp.float32),
        ),
        scratch_shapes=[
            weights,
            weights,
            pltpu.VMEM((rows, hidden), jnp.bfloat16),
            pltpu.SemaphoreType.DMA((columns // width + 1,)),
        ],
        compiler_params=pltpu.CompilerParams(vmem_limit_bytes=46 * MIB),
        cost_estimate=pl.CostEstimate(
            flops=4 * rows * D * hidden, bytes_accessed=4 * D * hidden, transcendentals=0
        ),
        name="feed_forward",
    )(x, first, *late)


def body(
    states, mix_gain, w_value, w_gate, conv_kernel, chan_gain, w_mix_out, mlp_gain, w_up, w_down_t
):
    width = states.shape[1]
    early, late = packed(w_value, w_gate, w_mix_out, w_up, w_down_t)
    slab = lax.all_to_all(late, "y", 0, 0, tiled=True).reshape(-1, late.shape[2])
    run = lax.all_gather(early, "zl", axis=0)
    gates = over_y(run[:, :, : 2 * width])
    normed = normed_channels(states, mix_gain)
    ffn_first = over_y(run[:, :, 2 * width :])
    slabs = over_z(slab)
    filtered, sums = gated_filter(normed, conv_kernel, gates, width)
    sums = lax.all_to_all(sums, TP, 0, 0, tiled=True)
    theirs, mine = mixer(filtered, sums, chan_gain, slabs)
    mixed = over_group(mine, theirs)
    middle = (states.astype(jnp.float32) + mixed).astype(jnp.bfloat16)
    normed_mid = normed_channels(middle, mlp_gain)
    theirs, mine = feed_forward(normed_mid, ffn_first, slabs)
    fed = over_group(mine, theirs)
    return (middle.astype(jnp.float32) + fed).astype(jnp.bfloat16)


def solution(mesh):
    split = Mesh(mesh.devices.reshape(2, 4, 8, 4, 2), ("rep", "zl", "y", "x", "c"))
    fs = ("zl", "y")
    return jax.shard_map(
        body,
        mesh=split,
        in_specs=(
            P(("rep", *fs), TP),
            P(),
            P(fs, TP),
            P(fs, TP),
            P(),
            P(),
            P(fs, TP),
            P(),
            P(fs, TP),
            P(fs, TP),
        ),
        out_specs=P(("rep", *fs), TP),
        check_vma=False,
    )
```

```python
import jax
import jax.numpy as jnp
from jax import lax
from jax.experimental import pallas as pl
from jax.experimental.pallas import tpu as pltpu
from jax.sharding import Mesh
from jax.sharding import PartitionSpec as P

D = 2048
KWIDTH = 31
LENGTH = 128
EPS = 1e-06
TP = ("x", "c")
SWAP = [(0, 1), (1, 0)]


MIB = 1 << 20
LANES = 128
ANY = pl.BlockSpec(memory_space=pl.ANY)
LATE = 256


def times_t(left, right):
    return lax.dot_general(
        left, right, (((1,), (1,)), ((), ())), preferred_element_type=jnp.float32
    )


def pack_kernel(value_ref, gate_ref, out_ref, up_ref, down_ref, gates_ref, first_ref, late_ref):
    width, first = value_ref.shape[1], up_ref.shape[1] - LATE
    gates_ref[:, :width] = value_ref[...]
    gates_ref[:, width:] = gate_ref[...]
    first_ref[:, :first] = up_ref[:, :first]
    first_ref[:, first:] = down_ref[:, :first]
    for copy in range(late_ref.shape[0]):
        late_ref[copy, :, :width] = out_ref[...]
        late_ref[copy, :, width : width + LATE] = up_ref[:, first:]
        late_ref[copy, :, width + LATE :] = down_ref[:, first:]


def packed(w_value, w_gate, w_mix_out, w_up, w_down_t):
    rows, width = w_value.shape
    first = w_up.shape[1] - LATE
    return pl.pallas_call(
        pack_kernel,
        out_shape=(
            jax.ShapeDtypeStruct((rows, 2 * width), jnp.bfloat16),
            jax.ShapeDtypeStruct((rows, 2 * first), jnp.bfloat16),
            jax.ShapeDtypeStruct((lax.axis_size("y"), rows, width + 2 * LATE), jnp.bfloat16),
        ),
        compiler_params=pltpu.CompilerParams(vmem_limit_bytes=60 * MIB),
        cost_estimate=pl.CostEstimate(flops=0, bytes_accessed=MIB, transcendentals=0),
        name="pack",
    )(w_value, w_gate, w_mix_out, w_up, w_down_t)


def over_y(run):
    return lax.all_gather(run, "y", axis=1, tiled=True)


def over_z(slab):
    half = slab.shape[0] // 2

    def from_z(piece, step):
        return lax.ppermute(piece, ("rep", "zl"), [((i + step) % 8, i) for i in range(8)])

    return [slab, from_z(slab, 1), from_z(slab[:half], 2), from_z(slab[half:], -2), from_z(slab, -1)]


def gate_kernel(x_ref, taps_ref, weight_ref, filtered_ref, sums_ref, padded_ref, held_ref, sems):
    count, depth, width = held_ref.shape[0], held_ref.shape[1], held_ref.shape[2] // 2
    copies = [
        pltpu.make_async_copy(weight_ref.at[z, :, : 2 * width], held_ref.at[z], sems.at[z])
        for z in range(count)
    ]
    for copy in copies:
        copy.start()
    value, gate = 0.0, 0.0
    for z, copy in enumerate(copies):
        copy.wait()
        x = x_ref[:, z * depth : (z + 1) * depth]
        value += jnp.dot(x, held_ref[z, :, :width], preferred_element_type=jnp.float32)
        gate += jnp.dot(x, held_ref[z, :, width:], preferred_element_type=jnp.float32)
    gated = value * jax.nn.sigmoid(gate)
    pad = padded_ref.shape[1] - LENGTH
    sequences = padded_ref.shape[0]
    for s in range(sequences):
        padded_ref[s, :pad] = jnp.zeros((pad, width), jnp.float32)
        padded_ref[s, pad:] = gated[s * LENGTH : (s + 1) * LENGTH]
    for lane in range(0, width, LANES):
        taps = taps_ref[:, lane : lane + LANES]
        for s in range(sequences):
            total = jnp.zeros((LENGTH, LANES), jnp.float32)
            for shift in range(8):
                offsets = [o for o in range(pad - KWIDTH + 1, pad + 1) if o % 8 == shift]
                span = offsets[-1] - shift + LENGTH
                rows = padded_ref[s, shift : shift + span, lane : lane + LANES]
                for o in offsets:
                    tap = o - (pad - KWIDTH + 1)
                    total += taps[tap : tap + 1] * rows[o - shift : o - shift + LENGTH]
            filtered_ref[s * LENGTH : (s + 1) * LENGTH, lane : lane + LANES] = total
    filtered = filtered_ref[...]
    ones = jnp.ones((8, width), jnp.float32)
    rows = x_ref.shape[0]
    for i, terms in enumerate((filtered, filtered * filtered)):
        sums = lax.dot_general(
            ones,
            terms,
            (((1,), (1,)), ((), ())),
            precision=lax.Precision.HIGHEST,
            preferred_element_type=jnp.float32,
        )
        for copy in range(sums_ref.shape[0]):
            sums_ref[copy, :, i * rows : (i + 1) * rows] = sums[:1]


def gated_filter(x, taps, weights, width):
    rows = x.shape[0]
    count, depth, _ = weights.shape
    vmem = pl.BlockSpec(memory_space=pltpu.VMEM)
    return pl.pallas_call(
        gate_kernel,
        in_specs=[vmem, vmem, ANY],
        out_specs=(vmem, vmem),
        out_shape=(
            jax.ShapeDtypeStruct((rows, width), jnp.float32),
            jax.ShapeDtypeStruct((lax.axis_size(TP), 1, 2 * rows), jnp.float32),
        ),
        scratch_shapes=[
            pltpu.VMEM((rows // LENGTH, LENGTH + 32, width), jnp.float32),
            pltpu.VMEM((count, depth, 2 * width), jnp.bfloat16),
            pltpu.SemaphoreType.DMA((count,)),
        ],
        compiler_params=pltpu.CompilerParams(vmem_limit_bytes=51 * MIB),
        cost_estimate=pl.CostEstimate(
            flops=4 * rows * D * width, bytes_accessed=4 * D * width, transcendentals=rows * width
        ),
        name="gated_filter",
    )(x, taps, weights)


def fetched(slab_refs, held_ref, columns, sems):
    here, count = lax.axis_index("zl"), lax.axis_size("zl")
    copies = []
    for i, (ref, turn) in enumerate(zip(slab_refs, (0, 1, 2, 2, 3))):
        low = ref.shape[0] if i == 3 else 0
        to = held_ref.at[lax.rem(here + turn, count), low : low + ref.shape[0]]
        copies.append(pltpu.make_async_copy(ref.at[:, columns], to, sems.at[i]))
        copies[i].start()
    return copies


def mixer_kernel(filtered_ref, sums_ref, gain_ref, *refs):
    *slab_refs, theirs_ref, mine_ref, held_ref, sems = refs
    core = lax.axis_index("c")
    rows, width = filtered_ref.shape
    copies = fetched(slab_refs, held_ref, slice(0, width), sems)
    sums = sum(sums_ref[d] for d in range(sums_ref.shape[0])) / D
    mean = sums[:, :rows]
    scale = lax.rsqrt(sums[:, rows:] - mean * mean + EPS)

    def down_rows(row):
        column = jnp.broadcast_to(row, (LANES, rows)).T
        return jnp.concatenate([column] * (width // LANES), axis=1)

    gain = gain_ref[:, pl.ds(pl.multiple_of(lax.axis_index(TP) * width, width), width)]
    values = (filtered_ref[...] - down_rows(mean)) * down_rows(scale) * gain
    activated = (values / (1.0 + jnp.exp(-values))).astype(jnp.bfloat16)
    for copy in copies:
        copy.wait()
    for out_ref, which in ((theirs_ref, 1 - core), (mine_ref, core)):
        at = pl.ds(pl.multiple_of(which * width, width), width)
        for z in range(held_ref.shape[0]):
            out_ref[z] = times_t(activated, held_ref[z, at]).astype(out_ref.dtype)


def mixer(filtered, sums, gain, slabs):
    rows, width = filtered.shape
    vmem = pl.BlockSpec(memory_space=pltpu.VMEM)
    out = (lax.axis_size("zl"), rows, width)
    return pl.pallas_call(
        mixer_kernel,
        in_specs=[vmem, vmem, vmem, *(ANY for _ in slabs)],
        out_specs=(vmem, vmem),
        out_shape=(
            jax.ShapeDtypeStruct(out, jnp.bfloat16),
            jax.ShapeDtypeStruct(out, jnp.float32),
        ),
        scratch_shapes=[
            pltpu.VMEM((out[0], 2 * width, width), jnp.bfloat16),
            pltpu.SemaphoreType.DMA((len(slabs),)),
        ],
        compiler_params=pltpu.CompilerParams(vmem_limit_bytes=24 * MIB),
        cost_estimate=pl.CostEstimate(
            flops=2 * rows * D * width, bytes_accessed=2 * D * width, transcendentals=rows * width
        ),
        name="mixer",
    )(filtered, sums, gain[None], *slabs)


def norm_kernel(own_ref, other_ref, gain_ref, out_ref):
    core = lax.axis_index("c")
    count, _, width = own_ref.shape
    pieces = [(r[i].astype(jnp.float32), i, s) for s, r in enumerate((own_ref, other_ref)) for i in range(count)]
    total = sum(jnp.sum(v * v, axis=-1, keepdims=True) for v, _, _ in pieces)
    scale = lax.rsqrt(total / D + EPS)
    for values, i, side in pieces:
        which = core if side == 0 else 1 - core
        at = pl.ds(pl.multiple_of((2 * i + which) * width, width), width)
        out_ref[:, at] = (values * scale * gain_ref[:, at]).astype(jnp.bfloat16)


def normed_channels(own, gain):
    other = lax.ppermute(own, "c", SWAP)
    count, rows, width = own.shape
    part = pl.BlockSpec((count, LENGTH, width), lambda i: (0, i, 0))
    return pl.pallas_call(
        norm_kernel,
        grid=(rows // LENGTH,),
        in_specs=[part, part, pl.BlockSpec((1, D), lambda i: (0, 0))],
        out_specs=pl.BlockSpec((LENGTH, D), lambda i: (i, 0)),
        out_shape=jax.ShapeDtypeStruct((rows, D), jnp.bfloat16),
        cost_estimate=pl.CostEstimate(
            flops=6 * rows * D, bytes_accessed=4 * rows * D, transcendentals=rows
        ),
        compiler_params=pltpu.CompilerParams(vmem_limit_bytes=12 * MIB),
        name="norm",
    )(own, other, gain[None])


def over_group(mine, theirs):
    got = lax.ppermute(theirs, "c", SWAP)
    pair = (mine + got.astype(jnp.float32)).astype(jnp.bfloat16)
    return jnp.sum(lax.all_to_all(pair, "x", 0, 0, tiled=True).astype(jnp.float32), axis=0)


def feed_forward_kernel(x_ref, first_ref, *refs):
    *slab_refs, theirs_ref, mine_ref, up_ref, down_ref, late_ref, hidden_ref, sems = refs
    core = lax.axis_index("c")
    count, depth, columns = up_ref.shape
    width = depth // 2
    steps = [slice(low, low + width) for low in range(0, columns, width)]
    copies = [
        pltpu.make_async_copy(first_ref.at[:, :, at], up_ref.at[:, :, at], sems.at[i])
        for i, at in enumerate(steps)
    ]
    for copy in copies:
        copy.start()
    past = len(steps) + 1
    late_copies = fetched(slab_refs, late_ref, slice(width, width + 2 * LATE), sems.at[past:])
    down = pltpu.make_async_copy(first_ref.at[:, :, columns:], down_ref, sems.at[len(steps)])
    down.start()

    def hidden_of(weight_ref, at):
        upward = 0.0
        for z in range(count):
            x = x_ref[:, z * depth : (z + 1) * depth]
            upward += jnp.dot(x, weight_ref[z, :, at], preferred_element_type=jnp.float32)
        return jnp.square(jnp.maximum(upward, 0.0)).astype(jnp.bfloat16)

    for copy, at in zip(copies, steps):
        copy.wait()
        hidden_ref[:, at] = hidden_of(up_ref, at)
    for copy in late_copies:
        copy.wait()
    hidden_ref[:, columns:] = hidden_of(late_ref, slice(0, LATE))
    down.wait()
    for out_ref, which in ((theirs_ref, 1 - core), (mine_ref, core)):
        rows = pl.ds(pl.multiple_of(which * width, width), width)
        for z in range(count):
            part = times_t(hidden_ref[:, :columns], down_ref[z, rows])
            part += times_t(hidden_ref[:, columns:], late_ref[z, rows, LATE:])
            out_ref[z] = part.astype(out_ref.dtype)


def feed_forward(x, first, late):
    rows = x.shape[0]
    count, depth, columns = first.shape
    columns //= 2
    width = depth // 2
    out = (count, rows, width)
    vmem = pl.BlockSpec(memory_space=pltpu.VMEM)
    weights = pltpu.VMEM((count, depth, columns), jnp.bfloat16)
    hidden = columns + LATE
    return pl.pallas_call(
        feed_forward_kernel,
        in_specs=[vmem, ANY, *(ANY for _ in late)],
        out_specs=(vmem, vmem),
        out_shape=(
            jax.ShapeDtypeStruct(out, jnp.bfloat16),
            jax.ShapeDtypeStruct(out, jnp.float32),
        ),
        scratch_shapes=[
            weights,
            weights,
            pltpu.VMEM((count, depth, 2 * LATE), jnp.bfloat16),
            pltpu.VMEM((rows, hidden), jnp.bfloat16),
            pltpu.SemaphoreType.DMA((columns // width + 1 + len(late),)),
        ],
        compiler_params=pltpu.CompilerParams(vmem_limit_bytes=46 * MIB),
        cost_estimate=pl.CostEstimate(
            flops=4 * rows * D * hidden, bytes_accessed=4 * D * hidden, transcendentals=0
        ),
        name="feed_forward",
    )(x, first, *late)


def body(
    states, mix_gain, w_value, w_gate, conv_kernel, chan_gain, w_mix_out, mlp_gain, w_up, w_down_t
):
    width = states.shape[1]
    gates, first, late = packed(w_value, w_gate, w_mix_out, w_up, w_down_t)
    slab = lax.all_to_all(late, "y", 0, 0, tiled=True).reshape(-1, late.shape[2])
    gates = lax.all_gather(gates, "zl", axis=0)
    first = lax.all_gather(first, "zl", axis=0)
    slabs = over_z(slab)
    own = lax.all_gather(states, "x", axis=0)
    taps = lax.dynamic_slice_in_dim(conv_kernel, lax.axis_index(TP) * width, width, 1)
    own, taps = lax.optimization_barrier((own, taps))
    gates, first = over_y(gates), over_y(first)
    normed = normed_channels(own, mix_gain)
    filtered, sums = gated_filter(normed, taps, gates, width)
    sums = lax.all_to_all(sums, TP, 0, 0, tiled=True)
    theirs, mine = mixer(filtered, sums, chan_gain, slabs)
    mixed = over_group(mine, theirs)
    middle = (states.astype(jnp.float32) + mixed).astype(jnp.bfloat16)
    normed_mid = normed_channels(lax.all_gather(middle, "x", axis=0), mlp_gain)
    theirs, mine = feed_forward(normed_mid, first, slabs)
    fed = over_group(mine, theirs)
    return (middle.astype(jnp.float32) + fed).astype(jnp.bfloat16)


def solution(mesh):
    split = Mesh(mesh.devices.reshape(2, 4, 8, 4, 2), ("rep", "zl", "y", "x", "c"))
    fs = ("zl", "y")
    return jax.shard_map(
        body,
        mesh=split,
        in_specs=(
            P(("rep", *fs), TP),
            P(),
            P(fs, TP),
            P(fs, TP),
            P(),
            P(),
            P(fs, TP),
            P(),
            P(fs, TP),
            P(fs, TP),
        ),
        out_specs=P(("rep", *fs), TP),
        check_vma=False,
    )
```

```python
import jax
import jax.numpy as jnp
from jax import lax
from jax.experimental import pallas as pl
from jax.experimental.pallas import tpu as pltpu
from jax.sharding import Mesh
from jax.sharding import PartitionSpec as P

D = 2048
KWIDTH = 31
LENGTH = 128
EPS = 1e-06
TP = ("x", "c")
SWAP = [(0, 1), (1, 0)]


MIB = 1 << 20
LANES = 128
ANY = pl.BlockSpec(memory_space=pl.ANY)
LATE = 256


def times_t(left, right):
    return lax.dot_general(
        left, right, (((1,), (1,)), ((), ())), preferred_element_type=jnp.float32
    )


def pack_kernel(value_ref, gate_ref, out_ref, up_ref, down_ref, gates_ref, first_ref, late_ref):
    width, first = value_ref.shape[1], up_ref.shape[1] - LATE
    gates_ref[:, :width] = value_ref[...]
    gates_ref[:, width:] = gate_ref[...]
    first_ref[:, :first] = up_ref[:, :first]
    first_ref[:, first:] = down_ref[:, :first]
    for copy in range(late_ref.shape[0]):
        late_ref[copy, :, :width] = out_ref[...]
        late_ref[copy, :, width : width + LATE] = up_ref[:, first:]
        late_ref[copy, :, width + LATE :] = down_ref[:, first:]


def packed(w_value, w_gate, w_mix_out, w_up, w_down_t):
    rows, width = w_value.shape
    first = w_up.shape[1] - LATE
    return pl.pallas_call(
        pack_kernel,
        out_shape=(
            jax.ShapeDtypeStruct((rows, 2 * width), jnp.bfloat16),
            jax.ShapeDtypeStruct((rows, 2 * first), jnp.bfloat16),
            jax.ShapeDtypeStruct((lax.axis_size("y"), rows, width + 2 * LATE), jnp.bfloat16),
        ),
        compiler_params=pltpu.CompilerParams(vmem_limit_bytes=60 * MIB),
        cost_estimate=pl.CostEstimate(flops=0, bytes_accessed=MIB, transcendentals=0),
        name="pack",
    )(w_value, w_gate, w_mix_out, w_up, w_down_t)


def over_y(run):
    return lax.all_gather(run, "y", axis=1, tiled=True)


def over_z(slab):
    def from_z(step):
        pairs = [((i + step(i)) % 8, i) for i in range(8)]
        return lax.ppermute(slab, ("rep", "zl"), pairs)

    two = from_z(lambda i: 2 if i % 2 == 0 else -2)
    return [slab, from_z(lambda i: 1), two, from_z(lambda i: -1)]


def gate_kernel(x_ref, taps_ref, weight_ref, filtered_ref, sums_ref, padded_ref, held_ref, sems):
    count, depth, width = held_ref.shape[0], held_ref.shape[1], held_ref.shape[2] // 2
    copies = [
        pltpu.make_async_copy(weight_ref.at[z, :, : 2 * width], held_ref.at[z], sems.at[z])
        for z in range(count)
    ]
    for copy in copies:
        copy.start()
    value, gate = 0.0, 0.0
    for z, copy in enumerate(copies):
        copy.wait()
        x = x_ref[:, z * depth : (z + 1) * depth]
        value += jnp.dot(x, held_ref[z, :, :width], preferred_element_type=jnp.float32)
        gate += jnp.dot(x, held_ref[z, :, width:], preferred_element_type=jnp.float32)
    gated = value * jax.nn.sigmoid(gate)
    pad = padded_ref.shape[1] - LENGTH
    sequences = padded_ref.shape[0]
    for s in range(sequences):
        padded_ref[s, :pad] = jnp.zeros((pad, width), jnp.float32)
        padded_ref[s, pad:] = gated[s * LENGTH : (s + 1) * LENGTH]
    for lane in range(0, width, LANES):
        taps = taps_ref[:, lane : lane + LANES]
        for s in range(sequences):
            total = jnp.zeros((LENGTH, LANES), jnp.float32)
            for shift in range(8):
                offsets = [o for o in range(pad - KWIDTH + 1, pad + 1) if o % 8 == shift]
                span = offsets[-1] - shift + LENGTH
                rows = padded_ref[s, shift : shift + span, lane : lane + LANES]
                for o in offsets:
                    tap = o - (pad - KWIDTH + 1)
                    total += taps[tap : tap + 1] * rows[o - shift : o - shift + LENGTH]
            filtered_ref[s * LENGTH : (s + 1) * LENGTH, lane : lane + LANES] = total
    filtered = filtered_ref[...]
    ones = jnp.ones((8, width), jnp.float32)
    rows = x_ref.shape[0]
    for i, terms in enumerate((filtered, filtered * filtered)):
        sums = lax.dot_general(
            ones,
            terms,
            (((1,), (1,)), ((), ())),
            precision=lax.Precision.HIGHEST,
            preferred_element_type=jnp.float32,
        )
        for copy in range(sums_ref.shape[0]):
            sums_ref[copy, :, i * rows : (i + 1) * rows] = sums[:1]


def gated_filter(x, taps, weights, width):
    rows = x.shape[0]
    count, depth, _ = weights.shape
    vmem = pl.BlockSpec(memory_space=pltpu.VMEM)
    return pl.pallas_call(
        gate_kernel,
        in_specs=[vmem, vmem, ANY],
        out_specs=(vmem, vmem),
        out_shape=(
            jax.ShapeDtypeStruct((rows, width), jnp.float32),
            jax.ShapeDtypeStruct((lax.axis_size(TP), 1, 2 * rows), jnp.float32),
        ),
        scratch_shapes=[
            pltpu.VMEM((rows // LENGTH, LENGTH + 32, width), jnp.float32),
            pltpu.VMEM((count, depth, 2 * width), jnp.bfloat16),
            pltpu.SemaphoreType.DMA((count,)),
        ],
        compiler_params=pltpu.CompilerParams(vmem_limit_bytes=52 * MIB),
        cost_estimate=pl.CostEstimate(
            flops=4 * rows * D * width, bytes_accessed=4 * D * width, transcendentals=rows * width
        ),
        name="gated_filter",
    )(x, taps, weights)


def fetched(slab_refs, held_ref, columns, sems):
    here, count = lax.axis_index("zl"), lax.axis_size("zl")
    copies = []
    for turn, ref in enumerate(slab_refs):
        to = held_ref.at[lax.rem(here + turn, count)]
        copies.append(pltpu.make_async_copy(ref.at[:, columns], to, sems.at[turn]))
        copies[turn].start()
    return copies


def mixer_kernel(filtered_ref, sums_ref, gain_ref, *refs):
    *slab_refs, theirs_ref, mine_ref, held_ref, sems = refs
    core = lax.axis_index("c")
    rows, width = filtered_ref.shape
    copies = fetched(slab_refs, held_ref, slice(0, width), sems)
    sums = sum(sums_ref[d] for d in range(sums_ref.shape[0])) / D
    mean = sums[:, :rows]
    scale = lax.rsqrt(sums[:, rows:] - mean * mean + EPS)

    def down_rows(row):
        column = jnp.broadcast_to(row, (LANES, rows)).T
        return jnp.concatenate([column] * (width // LANES), axis=1)

    gain = gain_ref[:, pl.ds(pl.multiple_of(lax.axis_index(TP) * width, width), width)]
    values = (filtered_ref[...] - down_rows(mean)) * down_rows(scale) * gain
    activated = (values / (1.0 + jnp.exp(-values))).astype(jnp.bfloat16)
    for copy in copies:
        copy.wait()
    for out_ref, which in ((theirs_ref, 1 - core), (mine_ref, core)):
        at = pl.ds(pl.multiple_of(which * width, width), width)
        for z in range(held_ref.shape[0]):
            out_ref[z] = times_t(activated, held_ref[z, at]).astype(out_ref.dtype)


def mixer(filtered, sums, gain, slabs):
    rows, width = filtered.shape
    vmem = pl.BlockSpec(memory_space=pltpu.VMEM)
    out = (lax.axis_size("zl"), rows, width)
    return pl.pallas_call(
        mixer_kernel,
        in_specs=[vmem, vmem, vmem, *(ANY for _ in slabs)],
        out_specs=(vmem, vmem),
        out_shape=(
            jax.ShapeDtypeStruct(out, jnp.bfloat16),
            jax.ShapeDtypeStruct(out, jnp.bfloat16),
        ),
        scratch_shapes=[
            pltpu.VMEM((out[0], 2 * width, width), jnp.bfloat16),
            pltpu.SemaphoreType.DMA((len(slabs),)),
        ],
        compiler_params=pltpu.CompilerParams(vmem_limit_bytes=52 * MIB),
        cost_estimate=pl.CostEstimate(
            flops=2 * rows * D * width, bytes_accessed=2 * D * width, transcendentals=rows * width
        ),
        name="mixer",
    )(filtered, sums, gain[None], *slabs)


def norm_kernel(own_ref, other_ref, gain_ref, out_ref):
    core = lax.axis_index("c")
    count, _, width = own_ref.shape
    pieces = [(r[i].astype(jnp.float32), i, s) for s, r in enumerate((own_ref, other_ref)) for i in range(count)]
    total = sum(jnp.sum(v * v, axis=-1, keepdims=True) for v, _, _ in pieces)
    scale = lax.rsqrt(total / D + EPS)
    for values, i, side in pieces:
        which = core if side == 0 else 1 - core
        at = pl.ds(pl.multiple_of((2 * i + which) * width, width), width)
        out_ref[:, at] = (values * scale * gain_ref[:, at]).astype(jnp.bfloat16)


def normed_channels(own, gain):
    other = lax.ppermute(own, "c", SWAP)
    count, rows, width = own.shape
    part = pl.BlockSpec((count, LENGTH, width), lambda i: (0, i, 0))
    return pl.pallas_call(
        norm_kernel,
        grid=(rows // LENGTH,),
        in_specs=[part, part, pl.BlockSpec((1, D), lambda i: (0, 0))],
        out_specs=pl.BlockSpec((LENGTH, D), lambda i: (i, 0)),
        out_shape=jax.ShapeDtypeStruct((rows, D), jnp.bfloat16),
        cost_estimate=pl.CostEstimate(
            flops=6 * rows * D, bytes_accessed=4 * rows * D, transcendentals=rows
        ),
        compiler_params=pltpu.CompilerParams(vmem_limit_bytes=12 * MIB),
        name="norm",
    )(own, other, gain[None])


def over_group(mine, theirs):
    got = lax.ppermute(theirs, "c", SWAP)
    pair = (mine.astype(jnp.float32) + got.astype(jnp.float32)).astype(jnp.bfloat16)
    return jnp.sum(lax.all_to_all(pair, "x", 0, 0, tiled=True).astype(jnp.float32), axis=0)


def feed_forward_kernel(x_ref, first_ref, *refs):
    *slab_refs, theirs_ref, mine_ref, up_ref, down_ref, late_ref, hidden_ref, sems = refs
    core = lax.axis_index("c")
    count, depth, columns = up_ref.shape
    width = depth // 2
    steps = [slice(low, low + width) for low in range(0, columns, width)]
    copies = [
        pltpu.make_async_copy(first_ref.at[:, :, at], up_ref.at[:, :, at], sems.at[i])
        for i, at in enumerate(steps)
    ]
    for copy in copies:
        copy.start()
    past = len(steps) + 1
    late_copies = fetched(slab_refs, late_ref, slice(width, width + 2 * LATE), sems.at[past:])
    down = pltpu.make_async_copy(first_ref.at[:, :, columns:], down_ref, sems.at[len(steps)])
    down.start()

    def hidden_of(weight_ref, at):
        upward = 0.0
        for z in range(count):
            x = x_ref[:, z * depth : (z + 1) * depth]
            upward += jnp.dot(x, weight_ref[z, :, at], preferred_element_type=jnp.float32)
        return jnp.square(jnp.maximum(upward, 0.0)).astype(jnp.bfloat16)

    for copy, at in zip(copies, steps):
        copy.wait()
        hidden_ref[:, at] = hidden_of(up_ref, at)
    for copy in late_copies:
        copy.wait()
    hidden_ref[:, columns:] = hidden_of(late_ref, slice(0, LATE))
    down.wait()
    for out_ref, which in ((theirs_ref, 1 - core), (mine_ref, core)):
        rows = pl.ds(pl.multiple_of(which * width, width), width)
        for z in range(count):
            part = times_t(hidden_ref[:, :columns], down_ref[z, rows])
            part += times_t(hidden_ref[:, columns:], late_ref[z, rows, LATE:])
            out_ref[z] = part.astype(out_ref.dtype)


def feed_forward(x, first, late):
    rows = x.shape[0]
    count, depth, columns = first.shape
    columns //= 2
    width = depth // 2
    out = (count, rows, width)
    vmem = pl.BlockSpec(memory_space=pltpu.VMEM)
    weights = pltpu.VMEM((count, depth, columns), jnp.bfloat16)
    hidden = columns + LATE
    return pl.pallas_call(
        feed_forward_kernel,
        in_specs=[vmem, ANY, *(ANY for _ in late)],
        out_specs=(vmem, vmem),
        out_shape=(
            jax.ShapeDtypeStruct(out, jnp.bfloat16),
            jax.ShapeDtypeStruct(out, jnp.bfloat16),
        ),
        scratch_shapes=[
            weights,
            weights,
            pltpu.VMEM((count, depth, 2 * LATE), jnp.bfloat16),
            pltpu.VMEM((rows, hidden), jnp.bfloat16),
            pltpu.SemaphoreType.DMA((columns // width + 1 + len(late),)),
        ],
        compiler_params=pltpu.CompilerParams(vmem_limit_bytes=52 * MIB),
        cost_estimate=pl.CostEstimate(
            flops=4 * rows * D * hidden, bytes_accessed=4 * D * hidden, transcendentals=0
        ),
        name="feed_forward",
    )(x, first, *late)


def body(
    states, mix_gain, w_value, w_gate, conv_kernel, chan_gain, w_mix_out, mlp_gain, w_up, w_down_t
):
    width = states.shape[1]
    gates, first, late = packed(w_value, w_gate, w_mix_out, w_up, w_down_t)
    slab = lax.all_to_all(late, "y", 0, 0, tiled=True).reshape(-1, late.shape[2])
    gates = lax.all_gather(gates, "zl", axis=0)
    first = lax.all_gather(first, "zl", axis=0)
    slabs = over_z(slab)
    own = lax.all_gather(states, "x", axis=0)
    taps = lax.dynamic_slice_in_dim(conv_kernel, lax.axis_index(TP) * width, width, 1)
    own, taps = lax.optimization_barrier((own, taps))
    gates, first = over_y(gates), over_y(first)
    normed = normed_channels(own, mix_gain)
    filtered, sums = gated_filter(normed, taps, gates, width)
    sums = lax.all_to_all(sums, TP, 0, 0, tiled=True)
    theirs, mine = mixer(filtered, sums, chan_gain, slabs)
    mixed = over_group(mine, theirs)
    middle = (states.astype(jnp.float32) + mixed).astype(jnp.bfloat16)
    normed_mid = normed_channels(lax.all_gather(middle, "x", axis=0), mlp_gain)
    theirs, mine = feed_forward(normed_mid, first, slabs)
    fed = over_group(mine, theirs)
    return (middle.astype(jnp.float32) + fed).astype(jnp.bfloat16)


def solution(mesh):
    split = Mesh(mesh.devices.reshape(2, 4, 8, 4, 2), ("rep", "zl", "y", "x", "c"))
    fs = ("zl", "y")
    return jax.shard_map(
        body,
        mesh=split,
        in_specs=(
            P(("rep", *fs), TP),
            P(),
            P(fs, TP),
            P(fs, TP),
            P(),
            P(),
            P(fs, TP),
            P(),
            P(fs, TP),
            P(fs, TP),
        ),
        out_specs=P(("rep", *fs), TP),
        check_vma=False,
    )
```

```python
import jax
import jax.numpy as jnp
from jax import lax
from jax.experimental import pallas as pl
from jax.experimental.pallas import tpu as pltpu
from jax.sharding import Mesh
from jax.sharding import PartitionSpec as P

D = 2048
KWIDTH = 31
LENGTH = 128
EPS = 1e-06
TP = ("x", "c")
SWAP = [(0, 1), (1, 0)]


MIB = 1 << 20
LANES = 128
ANY = pl.BlockSpec(memory_space=pl.ANY)
LATE = 256


def times_t(left, right):
    return lax.dot_general(
        left, right, (((1,), (1,)), ((), ())), preferred_element_type=jnp.float32
    )


def pack_kernel(value_ref, gate_ref, out_ref, up_ref, down_ref, gates_ref, first_ref, late_ref):
    width, first = value_ref.shape[1], up_ref.shape[1] - LATE
    gates_ref[:, :width] = value_ref[...]
    gates_ref[:, width:] = gate_ref[...]
    first_ref[:, :first] = up_ref[:, :first]
    first_ref[:, first:] = down_ref[:, :first]
    for copy in range(late_ref.shape[0]):
        late_ref[copy, :, :width] = out_ref[...]
        late_ref[copy, :, width : width + LATE] = up_ref[:, first:]
        late_ref[copy, :, width + LATE :] = down_ref[:, first:]


def packed(w_value, w_gate, w_mix_out, w_up, w_down_t):
    rows, width = w_value.shape
    first = w_up.shape[1] - LATE
    return pl.pallas_call(
        pack_kernel,
        out_shape=(
            jax.ShapeDtypeStruct((rows, 2 * width), jnp.bfloat16),
            jax.ShapeDtypeStruct((rows, 2 * first), jnp.bfloat16),
            jax.ShapeDtypeStruct((lax.axis_size("y"), rows, width + 2 * LATE), jnp.bfloat16),
        ),
        compiler_params=pltpu.CompilerParams(vmem_limit_bytes=60 * MIB),
        cost_estimate=pl.CostEstimate(flops=0, bytes_accessed=MIB, transcendentals=0),
        name="pack",
    )(w_value, w_gate, w_mix_out, w_up, w_down_t)


def over_y(run):
    return lax.all_gather(run, "y", axis=1, tiled=True)


def over_z(slab):
    def from_z(step):
        pairs = [((i + step(i)) % 8, i) for i in range(8)]
        return lax.ppermute(slab, ("rep", "zl"), pairs)

    one, three = from_z(lambda i: 1), from_z(lambda i: -1)
    two = from_z(lambda i: 2 if i % 2 == 0 else -2)
    return [slab, one, two, three]


def gate_kernel(x_ref, taps_ref, weight_ref, filtered_ref, sums_ref, padded_ref, held_ref, sems):
    count, depth, columns = weight_ref.shape
    width = columns // 2
    copies = [
        pltpu.make_async_copy(
            weight_ref.at[z], held_ref.at[z * depth : (z + 1) * depth], sems.at[z]
        )
        for z in range(count)
    ]
    for copy in copies:
        copy.start()
    both = 0.0
    for half in range(2):
        for copy in copies[half * count // 2 : (half + 1) * count // 2]:
            copy.wait()
        at = slice(half * D // 2, (half + 1) * D // 2)
        both += jnp.dot(x_ref[:, at], held_ref[at], preferred_element_type=jnp.float32)
    value, gate = both[:, :width], both[:, width:]
    gated = value * jax.nn.sigmoid(gate)
    pad = padded_ref.shape[1] - LENGTH
    sequences = padded_ref.shape[0]
    for s in range(sequences):
        padded_ref[s, :pad] = jnp.zeros((pad, width), jnp.float32)
        padded_ref[s, pad:] = gated[s * LENGTH : (s + 1) * LENGTH]
    for lane in range(0, width, LANES):
        taps = taps_ref[:, lane : lane + LANES]
        for s in range(sequences):
            total = jnp.zeros((LENGTH, LANES), jnp.float32)
            for shift in range(8):
                offsets = [o for o in range(pad - KWIDTH + 1, pad + 1) if o % 8 == shift]
                span = offsets[-1] - shift + LENGTH
                rows = padded_ref[s, shift : shift + span, lane : lane + LANES]
                for o in offsets:
                    tap = o - (pad - KWIDTH + 1)
                    total += taps[tap : tap + 1] * rows[o - shift : o - shift + LENGTH]
            filtered_ref[s * LENGTH : (s + 1) * LENGTH, lane : lane + LANES] = total
    filtered = filtered_ref[...]
    ones = jnp.ones((8, width), jnp.float32)
    rows = x_ref.shape[0]
    for i, terms in enumerate((filtered, filtered * filtered)):
        sums = lax.dot_general(
            ones,
            terms,
            (((1,), (1,)), ((), ())),
            precision=lax.Precision.HIGHEST,
            preferred_element_type=jnp.float32,
        )
        for copy in range(sums_ref.shape[0]):
            sums_ref[copy, :, i * rows : (i + 1) * rows] = sums[:1]


def gated_filter(x, taps, weights, width):
    rows = x.shape[0]
    count, _, _ = weights.shape
    vmem = pl.BlockSpec(memory_space=pltpu.VMEM)
    return pl.pallas_call(
        gate_kernel,
        in_specs=[vmem, vmem, ANY],
        out_specs=(vmem, vmem),
        out_shape=(
            jax.ShapeDtypeStruct((rows, width), jnp.float32),
            jax.ShapeDtypeStruct((lax.axis_size(TP), 1, 2 * rows), jnp.float32),
        ),
        scratch_shapes=[
            pltpu.VMEM((rows // LENGTH, LENGTH + 32, width), jnp.float32),
            pltpu.VMEM((D, 2 * width), jnp.bfloat16),
            pltpu.SemaphoreType.DMA((count,)),
        ],
        compiler_params=pltpu.CompilerParams(vmem_limit_bytes=52 * MIB),
        cost_estimate=pl.CostEstimate(
            flops=4 * rows * D * width, bytes_accessed=4 * D * width, transcendentals=rows * width
        ),
        name="gated_filter",
    )(x, taps, weights)


def fetched(slab_refs, held_ref, columns, at, sems):
    here, count = lax.axis_index("zl"), lax.axis_size("zl")
    copies = []
    for turn, ref in enumerate(slab_refs):
        depth = ref.shape[0]
        start = pl.multiple_of(lax.rem(here + turn, count) * depth, depth)
        to = held_ref.at[pl.ds(start, depth), at]
        copies.append(pltpu.make_async_copy(ref.at[:, columns], to, sems.at[turn]))
        copies[turn].start()
    return copies


def mixer_kernel(filtered_ref, sums_ref, gain_ref, *refs):
    *slab_refs, theirs_ref, mine_ref, held_ref, sems = refs
    core = lax.axis_index("c")
    rows, width = filtered_ref.shape
    own = slice(0, width)
    copies = fetched(slab_refs, held_ref, own, own, sems)
    sums = sum(sums_ref[d] for d in range(sums_ref.shape[0])) / D
    mean = sums[:, :rows]
    scale = lax.rsqrt(sums[:, rows:] - mean * mean + EPS)

    def down_rows(row):
        column = jnp.broadcast_to(row, (LANES, rows)).T
        return jnp.concatenate([column] * (width // LANES), axis=1)

    gain = gain_ref[:, pl.ds(pl.multiple_of(lax.axis_index(TP) * width, width), width)]
    values = (filtered_ref[...] - down_rows(mean)) * down_rows(scale) * gain
    activated = (values / (1.0 + jnp.exp(-values))).astype(jnp.bfloat16)
    for copy in copies:
        copy.wait()
    for out_ref, which in ((theirs_ref, 1 - core), (mine_ref, core)):
        for x in range(out_ref.shape[0]):
            at = pl.ds(pl.multiple_of((2 * x + which) * width, width), width)
            out_ref[x] = times_t(activated, held_ref[at]).astype(out_ref.dtype)


def mixer(filtered, sums, gain, slabs):
    rows, width = filtered.shape
    vmem = pl.BlockSpec(memory_space=pltpu.VMEM)
    out = (lax.axis_size("zl"), rows, width)
    return pl.pallas_call(
        mixer_kernel,
        in_specs=[vmem, vmem, vmem, *(ANY for _ in slabs)],
        out_specs=(vmem, vmem),
        out_shape=(
            jax.ShapeDtypeStruct(out, jnp.bfloat16),
            jax.ShapeDtypeStruct(out, jnp.bfloat16),
        ),
        scratch_shapes=[
            pltpu.VMEM((D, width), jnp.bfloat16),
            pltpu.SemaphoreType.DMA((len(slabs),)),
        ],
        compiler_params=pltpu.CompilerParams(vmem_limit_bytes=52 * MIB),
        cost_estimate=pl.CostEstimate(
            flops=2 * rows * D * width, bytes_accessed=2 * D * width, transcendentals=rows * width
        ),
        name="mixer",
    )(filtered, sums, gain[None], *slabs)


def norm_kernel(own_ref, other_ref, gain_ref, out_ref):
    core = lax.axis_index("c")
    count, _, width = own_ref.shape
    pieces = [(r[i].astype(jnp.float32), i, s) for s, r in enumerate((own_ref, other_ref)) for i in range(count)]
    total = sum(jnp.sum(v * v, axis=-1, keepdims=True) for v, _, _ in pieces)
    scale = lax.rsqrt(total / D + EPS)
    for values, i, side in pieces:
        which = core if side == 0 else 1 - core
        at = pl.ds(pl.multiple_of((2 * i + which) * width, width), width)
        out_ref[:, at] = (values * scale * gain_ref[:, at]).astype(jnp.bfloat16)


def normed_channels(own, gain):
    other = lax.ppermute(own, "c", SWAP)
    count, rows, width = own.shape
    part = pl.BlockSpec((count, LENGTH, width), lambda i: (0, i, 0))
    return pl.pallas_call(
        norm_kernel,
        grid=(rows // LENGTH,),
        in_specs=[part, part, pl.BlockSpec((1, D), lambda i: (0, 0))],
        out_specs=pl.BlockSpec((LENGTH, D), lambda i: (i, 0)),
        out_shape=jax.ShapeDtypeStruct((rows, D), jnp.bfloat16),
        cost_estimate=pl.CostEstimate(
            flops=6 * rows * D, bytes_accessed=4 * rows * D, transcendentals=rows
        ),
        compiler_params=pltpu.CompilerParams(vmem_limit_bytes=12 * MIB),
        name="norm",
    )(own, other, gain[None])


def over_group(mine, theirs):
    got = lax.ppermute(theirs, "c", SWAP)
    pair = (mine.astype(jnp.float32) + got.astype(jnp.float32)).astype(jnp.bfloat16)
    return jnp.sum(lax.all_to_all(pair, "x", 0, 0, tiled=True).astype(jnp.float32), axis=0)


def feed_forward_kernel(x_ref, first_ref, *refs):
    *slab_refs, theirs_ref, mine_ref, up_ref, down_ref, hidden_ref, sems = refs
    core = lax.axis_index("c")
    count, depth, columns = first_ref.shape
    columns //= 2
    width = depth // 2
    steps = [slice(low, low + width) for low in range(0, columns, width)]
    late = slice(columns, columns + LATE)

    def fetch(low, ref, at, sem):
        copies = [
            pltpu.make_async_copy(
                first_ref.at[z, :, low : low + at.stop - at.start],
                ref.at[z * depth : (z + 1) * depth, at],
                sem.at[z],
            )
            for z in range(count)
        ]
        for copy in copies:
            copy.start()
        return copies

    def wait(copies):
        for copy in copies:
            copy.wait()

    def hidden_of(at):
        upward = jnp.dot(x_ref[...], up_ref[:, at], preferred_element_type=jnp.float32)
        hidden_ref[:, at] = jnp.square(jnp.maximum(upward, 0.0)).astype(jnp.bfloat16)

    early = [fetch(at.start, up_ref, at, sems.at[i]) for i, at in enumerate(steps)]
    past = len(steps)
    late_up = fetched(slab_refs, up_ref, slice(width, width + LATE), late, sems.at[past])
    down = fetch(columns, down_ref, slice(0, columns), sems.at[past + 1])
    down += fetched(
        slab_refs, down_ref, slice(width + LATE, width + 2 * LATE), late, sems.at[past + 2]
    )
    for copies, at in zip(early, steps):
        wait(copies)
        hidden_of(at)
    wait(late_up)
    hidden_of(late)
    wait(down)
    for out_ref, which in ((theirs_ref, 1 - core), (mine_ref, core)):
        for x in range(count):
            rows = pl.ds(pl.multiple_of((2 * x + which) * width, width), width)
            out_ref[x] = times_t(hidden_ref[...], down_ref[rows]).astype(out_ref.dtype)


def feed_forward(x, first, late):
    rows = x.shape[0]
    count, depth, columns = first.shape
    columns //= 2
    width = depth // 2
    out = (count, rows, width)
    vmem = pl.BlockSpec(memory_space=pltpu.VMEM)
    hidden = columns + LATE
    weights = pltpu.VMEM((D, hidden), jnp.bfloat16)
    return pl.pallas_call(
        feed_forward_kernel,
        in_specs=[vmem, ANY, *(ANY for _ in late)],
        out_specs=(vmem, vmem),
        out_shape=(
            jax.ShapeDtypeStruct(out, jnp.bfloat16),
            jax.ShapeDtypeStruct(out, jnp.bfloat16),
        ),
        scratch_shapes=[
            weights,
            weights,
            pltpu.VMEM((rows, hidden), jnp.bfloat16),
            pltpu.SemaphoreType.DMA((columns // width + 3, count)),
        ],
        compiler_params=pltpu.CompilerParams(vmem_limit_bytes=52 * MIB),
        cost_estimate=pl.CostEstimate(
            flops=4 * rows * D * hidden, bytes_accessed=4 * D * hidden, transcendentals=0
        ),
        name="feed_forward",
    )(x, first, *late)


def body(
    states, mix_gain, w_value, w_gate, conv_kernel, chan_gain, w_mix_out, mlp_gain, w_up, w_down_t
):
    width = states.shape[1]
    gates, first, late = packed(w_value, w_gate, w_mix_out, w_up, w_down_t)
    slab = lax.all_to_all(late, "y", 0, 0, tiled=True).reshape(-1, late.shape[2])
    gates = lax.all_gather(gates, "zl", axis=0)
    first = lax.all_gather(first, "zl", axis=0)
    slabs = over_z(slab)
    own = lax.all_gather(states, "x", axis=0)
    taps = lax.dynamic_slice_in_dim(conv_kernel, lax.axis_index(TP) * width, width, 1)
    own, taps = lax.optimization_barrier((own, taps))
    gates, first = over_y(gates), over_y(first)
    normed = normed_channels(own, mix_gain)
    filtered, sums = gated_filter(normed, taps, gates, width)
    sums = lax.all_to_all(sums, TP, 0, 0, tiled=True)
    theirs, mine = mixer(filtered, sums, chan_gain, slabs)
    mixed = over_group(mine, theirs)
    middle = (states.astype(jnp.float32) + mixed).astype(jnp.bfloat16)
    normed_mid = normed_channels(lax.all_gather(middle, "x", axis=0), mlp_gain)
    theirs, mine = feed_forward(normed_mid, first, slabs)
    fed = over_group(mine, theirs)
    return (middle.astype(jnp.float32) + fed).astype(jnp.bfloat16)


def solution(mesh):
    split = Mesh(mesh.devices.reshape(2, 4, 8, 4, 2), ("rep", "zl", "y", "x", "c"))
    fs = ("zl", "y")
    return jax.shard_map(
        body,
        mesh=split,
        in_specs=(
            P(("rep", *fs), TP),
            P(),
            P(fs, TP),
            P(fs, TP),
            P(),
            P(),
            P(fs, TP),
            P(),
            P(fs, TP),
            P(fs, TP),
        ),
        out_specs=P(("rep", *fs), TP),
        check_vma=False,
    )
```

```python
import jax
import jax.numpy as jnp
from jax import lax
from jax.experimental import pallas as pl
from jax.experimental.pallas import tpu as pltpu
from jax.sharding import Mesh
from jax.sharding import PartitionSpec as P

D = 2048
KWIDTH = 31
LENGTH = 128
EPS = 1e-06
TP = ("x", "c")
SWAP = [(0, 1), (1, 0)]


MIB = 1 << 20
LANES = 128
ANY = pl.BlockSpec(memory_space=pl.ANY)
LATE = 256


def times_t(left, right):
    return lax.dot_general(
        left, right, (((1,), (1,)), ((), ())), preferred_element_type=jnp.float32
    )


def pack_kernel(value_ref, gate_ref, out_ref, up_ref, down_ref, gates_ref, first_ref, late_ref):
    width, first = value_ref.shape[1], up_ref.shape[1] - LATE
    gates_ref[:, :width] = value_ref[...]
    gates_ref[:, width:] = gate_ref[...]
    first_ref[:, :first] = up_ref[:, :first]
    first_ref[:, first:] = down_ref[:, :first]
    for copy in range(late_ref.shape[0]):
        late_ref[copy, :, :width] = out_ref[...]
        late_ref[copy, :, width : width + LATE] = up_ref[:, first:]
        late_ref[copy, :, width + LATE :] = down_ref[:, first:]


def packed(w_value, w_gate, w_mix_out, w_up, w_down_t):
    rows, width = w_value.shape
    first = w_up.shape[1] - LATE
    return pl.pallas_call(
        pack_kernel,
        out_shape=(
            jax.ShapeDtypeStruct((rows, 2 * width), jnp.bfloat16),
            jax.ShapeDtypeStruct((rows, 2 * first), jnp.bfloat16),
            jax.ShapeDtypeStruct((lax.axis_size("y"), rows, width + 2 * LATE), jnp.bfloat16),
        ),
        compiler_params=pltpu.CompilerParams(vmem_limit_bytes=60 * MIB),
        cost_estimate=pl.CostEstimate(flops=0, bytes_accessed=MIB, transcendentals=0),
        name="pack",
    )(w_value, w_gate, w_mix_out, w_up, w_down_t)


def over_y(run):
    return lax.all_gather(run, "y", axis=1, tiled=True)


def over_z(slab):
    def from_z(step):
        pairs = [((i + step(i)) % 8, i) for i in range(8)]
        return lax.ppermute(slab, ("rep", "zl"), pairs)

    two = from_z(lambda i: 2 if i % 2 == 0 else -2)
    return [slab, from_z(lambda i: 1), two, from_z(lambda i: -1)]


def gate_kernel(x_ref, taps_ref, weight_ref, filtered_ref, sums_ref, padded_ref, held_ref, sems):
    count, depth, width = held_ref.shape[0], held_ref.shape[1], held_ref.shape[2] // 2
    copies = [
        pltpu.make_async_copy(weight_ref.at[z, :, : 2 * width], held_ref.at[z], sems.at[z])
        for z in range(count)
    ]
    for copy in copies:
        copy.start()
    value, gate = 0.0, 0.0
    for z, copy in enumerate(copies):
        copy.wait()
        x = x_ref[:, z * depth : (z + 1) * depth]
        value += jnp.dot(x, held_ref[z, :, :width], preferred_element_type=jnp.float32)
        gate += jnp.dot(x, held_ref[z, :, width:], preferred_element_type=jnp.float32)
    gated = value * jax.nn.sigmoid(gate)
    pad = padded_ref.shape[1] - LENGTH
    sequences = padded_ref.shape[0]
    for s in range(sequences):
        padded_ref[s, :pad] = jnp.zeros((pad, width), jnp.float32)
        padded_ref[s, pad:] = gated[s * LENGTH : (s + 1) * LENGTH]
    for lane in range(0, width, LANES):
        taps = taps_ref[:, lane : lane + LANES]
        for s in range(sequences):
            total = jnp.zeros((LENGTH, LANES), jnp.float32)
            for shift in range(8):
                offsets = [o for o in range(pad - KWIDTH + 1, pad + 1) if o % 8 == shift]
                span = offsets[-1] - shift + LENGTH
                rows = padded_ref[s, shift : shift + span, lane : lane + LANES]
                for o in offsets:
                    tap = o - (pad - KWIDTH + 1)
                    total += taps[tap : tap + 1] * rows[o - shift : o - shift + LENGTH]
            filtered_ref[s * LENGTH : (s + 1) * LENGTH, lane : lane + LANES] = total
    filtered = filtered_ref[...]
    ones = jnp.ones((8, width), jnp.float32)
    rows = x_ref.shape[0]
    for i, terms in enumerate((filtered, filtered * filtered)):
        sums = lax.dot_general(
            ones,
            terms,
            (((1,), (1,)), ((), ())),
            precision=lax.Precision.HIGHEST,
            preferred_element_type=jnp.float32,
        )
        for copy in range(sums_ref.shape[0]):
            sums_ref[copy, :, i * rows : (i + 1) * rows] = sums[:1]


def gated_filter(x, taps, weights, width):
    rows = x.shape[0]
    count, depth, _ = weights.shape
    vmem = pl.BlockSpec(memory_space=pltpu.VMEM)
    return pl.pallas_call(
        gate_kernel,
        in_specs=[vmem, vmem, ANY],
        out_specs=(vmem, vmem),
        out_shape=(
            jax.ShapeDtypeStruct((rows, width), jnp.float32),
            jax.ShapeDtypeStruct((lax.axis_size(TP), 1, 2 * rows), jnp.float32),
        ),
        scratch_shapes=[
            pltpu.VMEM((rows // LENGTH, LENGTH + 32, width), jnp.float32),
            pltpu.VMEM((count, depth, 2 * width), jnp.bfloat16),
            pltpu.SemaphoreType.DMA((count,)),
        ],
        compiler_params=pltpu.CompilerParams(vmem_limit_bytes=52 * MIB),
        cost_estimate=pl.CostEstimate(
            flops=4 * rows * D * width, bytes_accessed=4 * D * width, transcendentals=rows * width
        ),
        name="gated_filter",
    )(x, taps, weights)


def fetched(slab_refs, held_ref, columns, sems):
    here, count = lax.axis_index("zl"), lax.axis_size("zl")
    copies = []
    for turn, ref in enumerate(slab_refs):
        to = held_ref.at[lax.rem(here + turn, count)]
        copies.append(pltpu.make_async_copy(ref.at[:, columns], to, sems.at[turn]))
        copies[turn].start()
    return copies


def mixer_kernel(filtered_ref, sums_ref, gain_ref, *refs):
    *slab_refs, theirs_ref, mine_ref, held_ref, sems = refs
    core = lax.axis_index("c")
    rows, width = filtered_ref.shape
    copies = fetched(slab_refs, held_ref, slice(0, width), sems)
    sums = sum(sums_ref[d] for d in range(sums_ref.shape[0])) / D
    mean = sums[:, :rows]
    scale = lax.rsqrt(sums[:, rows:] - mean * mean + EPS)

    def down_rows(row):
        column = jnp.broadcast_to(row, (LANES, rows)).T
        return jnp.concatenate([column] * (width // LANES), axis=1)

    gain = gain_ref[:, pl.ds(pl.multiple_of(lax.axis_index(TP) * width, width), width)]
    values = (filtered_ref[...] - down_rows(mean)) * down_rows(scale) * gain
    activated = (values / (1.0 + jnp.exp(-values))).astype(jnp.bfloat16)
    for copy in copies:
        copy.wait()
    for out_ref, which in ((theirs_ref, 1 - core), (mine_ref, core)):
        at = pl.ds(pl.multiple_of(which * width, width), width)
        for z in range(held_ref.shape[0]):
            out_ref[z] = times_t(activated, held_ref[z, at]).astype(out_ref.dtype)


def mixer(filtered, sums, gain, slabs):
    rows, width = filtered.shape
    vmem = pl.BlockSpec(memory_space=pltpu.VMEM)
    out = (lax.axis_size("zl"), rows, width)
    return pl.pallas_call(
        mixer_kernel,
        in_specs=[vmem, vmem, vmem, *(ANY for _ in slabs)],
        out_specs=(vmem, vmem),
        out_shape=(
            jax.ShapeDtypeStruct(out, jnp.bfloat16),
            jax.ShapeDtypeStruct(out, jnp.bfloat16),
        ),
        scratch_shapes=[
            pltpu.VMEM((out[0], 2 * width, width), jnp.bfloat16),
            pltpu.SemaphoreType.DMA((len(slabs),)),
        ],
        compiler_params=pltpu.CompilerParams(vmem_limit_bytes=52 * MIB),
        cost_estimate=pl.CostEstimate(
            flops=2 * rows * D * width, bytes_accessed=2 * D * width, transcendentals=rows * width
        ),
        name="mixer",
    )(filtered, sums, gain[None], *slabs)


def norm_kernel(own_ref, other_ref, gain_ref, out_ref):
    core = lax.axis_index("c")
    count, _, width = own_ref.shape
    pieces = [(r[i].astype(jnp.float32), i, s) for s, r in enumerate((own_ref, other_ref)) for i in range(count)]
    total = sum(jnp.sum(v * v, axis=-1, keepdims=True) for v, _, _ in pieces)
    scale = lax.rsqrt(total / D + EPS)
    for values, i, side in pieces:
        which = core if side == 0 else 1 - core
        at = pl.ds(pl.multiple_of((2 * i + which) * width, width), width)
        out_ref[:, at] = (values * scale * gain_ref[:, at]).astype(jnp.bfloat16)


def normed_channels(own, gain):
    other = lax.ppermute(own, "c", SWAP)
    count, rows, width = own.shape
    part = pl.BlockSpec((count, LENGTH, width), lambda i: (0, i, 0))
    return pl.pallas_call(
        norm_kernel,
        grid=(rows // LENGTH,),
        in_specs=[part, part, pl.BlockSpec((1, D), lambda i: (0, 0))],
        out_specs=pl.BlockSpec((LENGTH, D), lambda i: (i, 0)),
        out_shape=jax.ShapeDtypeStruct((rows, D), jnp.bfloat16),
        cost_estimate=pl.CostEstimate(
            flops=6 * rows * D, bytes_accessed=4 * rows * D, transcendentals=rows
        ),
        compiler_params=pltpu.CompilerParams(vmem_limit_bytes=12 * MIB),
        name="norm",
    )(own, other, gain[None])


def over_group(mine, theirs):
    got = lax.ppermute(theirs, "c", SWAP)
    pair = (mine.astype(jnp.float32) + got.astype(jnp.float32)).astype(jnp.bfloat16)
    return jnp.sum(lax.all_to_all(pair, "x", 0, 0, tiled=True).astype(jnp.float32), axis=0)


def feed_forward_kernel(rows_ref, first_ref, *refs):
    *slab_refs, theirs_ref, mine_ref, x_ref, up_ref, down_ref, late_ref, hidden_ref, sems = refs
    core = lax.axis_index("c")
    count, depth, columns = up_ref.shape
    width = depth // 2
    steps = [slice(low, low + width) for low in range(0, columns, width)]
    copies = [
        pltpu.make_async_copy(first_ref.at[:, :, at], up_ref.at[:, :, at], sems.at[i])
        for i, at in enumerate(steps)
    ]
    past = len(steps) + 2
    whole_x = pltpu.make_async_copy(rows_ref, x_ref, sems.at[past - 1])
    down = pltpu.make_async_copy(first_ref.at[:, :, columns:], down_ref, sems.at[len(steps)])
    whole_x.start()
    for copy in copies:
        copy.start()

    def hidden_of(weight_ref, at):
        upward = 0.0
        for z in range(count):
            x = x_ref[:, z * depth : (z + 1) * depth]
            upward += jnp.dot(x, weight_ref[z, :, at], preferred_element_type=jnp.float32)
        return jnp.square(jnp.maximum(upward, 0.0)).astype(jnp.bfloat16)

    whole_x.wait()
    copies[0].wait()
    late_copies = fetched(slab_refs, late_ref, slice(width, width + 2 * LATE), sems.at[past:])
    down.start()
    hidden_ref[:, steps[0]] = hidden_of(up_ref, steps[0])
    for copy, at in zip(copies[1:], steps[1:]):
        copy.wait()
        hidden_ref[:, at] = hidden_of(up_ref, at)
    for copy in late_copies:
        copy.wait()
    hidden_ref[:, columns:] = hidden_of(late_ref, slice(0, LATE))
    down.wait()
    for out_ref, which in ((theirs_ref, 1 - core), (mine_ref, core)):
        rows = pl.ds(pl.multiple_of(which * width, width), width)
        for z in range(count):
            part = times_t(hidden_ref[:, :columns], down_ref[z, rows])
            part += times_t(hidden_ref[:, columns:], late_ref[z, rows, LATE:])
            out_ref[z] = part.astype(out_ref.dtype)


def feed_forward(x, first, late):
    rows = x.shape[0]
    count, depth, columns = first.shape
    columns //= 2
    width = depth // 2
    out = (count, rows, width)
    vmem = pl.BlockSpec(memory_space=pltpu.VMEM)
    weights = pltpu.VMEM((count, depth, columns), jnp.bfloat16)
    hidden = columns + LATE
    return pl.pallas_call(
        feed_forward_kernel,
        in_specs=[ANY, ANY, *(ANY for _ in late)],
        out_specs=(vmem, vmem),
        out_shape=(
            jax.ShapeDtypeStruct(out, jnp.bfloat16),
            jax.ShapeDtypeStruct(out, jnp.bfloat16),
        ),
        scratch_shapes=[
            pltpu.VMEM(x.shape, jnp.bfloat16),
            weights,
            weights,
            pltpu.VMEM((count, depth, 2 * LATE), jnp.bfloat16),
            pltpu.VMEM((rows, hidden), jnp.bfloat16),
            pltpu.SemaphoreType.DMA((columns // width + 2 + len(late),)),
        ],
        compiler_params=pltpu.CompilerParams(vmem_limit_bytes=52 * MIB),
        cost_estimate=pl.CostEstimate(
            flops=4 * rows * D * hidden, bytes_accessed=4 * D * hidden, transcendentals=0
        ),
        name="feed_forward",
    )(x, first, *late)


def body(
    states, mix_gain, w_value, w_gate, conv_kernel, chan_gain, w_mix_out, mlp_gain, w_up, w_down_t
):
    width = states.shape[1]
    gates, first, late = packed(w_value, w_gate, w_mix_out, w_up, w_down_t)
    slab = lax.all_to_all(late, "y", 0, 0, tiled=True).reshape(-1, late.shape[2])
    gates = lax.all_gather(gates, "zl", axis=0)
    first = lax.all_gather(first, "zl", axis=0)
    slabs = over_z(slab)
    own = lax.all_gather(states, "x", axis=0)
    taps = lax.dynamic_slice_in_dim(conv_kernel, lax.axis_index(TP) * width, width, 1)
    own, taps = lax.optimization_barrier((own, taps))
    gates, first = over_y(gates), over_y(first)
    normed = normed_channels(own, mix_gain)
    filtered, sums = gated_filter(normed, taps, gates, width)
    sums = lax.all_to_all(sums, TP, 0, 0, tiled=True)
    theirs, mine = mixer(filtered, sums, chan_gain, slabs)
    mixed = over_group(mine, theirs)
    middle = (states.astype(jnp.float32) + mixed).astype(jnp.bfloat16)
    normed_mid = normed_channels(lax.all_gather(middle, "x", axis=0), mlp_gain)
    theirs, mine = feed_forward(normed_mid, first, slabs)
    fed = over_group(mine, theirs)
    return (middle.astype(jnp.float32) + fed).astype(jnp.bfloat16)


def solution(mesh):
    split = Mesh(mesh.devices.reshape(2, 4, 8, 4, 2), ("rep", "zl", "y", "x", "c"))
    fs = ("zl", "y")
    return jax.shard_map(
        body,
        mesh=split,
        in_specs=(
            P(("rep", *fs), TP),
            P(),
            P(fs, TP),
            P(fs, TP),
            P(),
            P(),
            P(fs, TP),
            P(),
            P(fs, TP),
            P(fs, TP),
        ),
        out_specs=P(("rep", *fs), TP),
        check_vma=False,
    )
```

```python
import jax
import jax.numpy as jnp
from jax import lax
from jax.experimental import pallas as pl
from jax.experimental.pallas import tpu as pltpu
from jax.sharding import Mesh
from jax.sharding import PartitionSpec as P

D = 2048
KWIDTH = 31
LENGTH = 128
EPS = 1e-06
TP = ("x", "c")
SWAP = [(0, 1), (1, 0)]


MIB = 1 << 20
LANES = 128
ANY = pl.BlockSpec(memory_space=pl.ANY)
LATE = 256


def times_t(left, right):
    return lax.dot_general(
        left, right, (((1,), (1,)), ((), ())), preferred_element_type=jnp.float32
    )


def pack_kernel(value_ref, gate_ref, out_ref, up_ref, down_ref, gates_ref, first_ref, late_ref):
    width, first = value_ref.shape[1], up_ref.shape[1] - LATE
    gates_ref[:, :width] = value_ref[...]
    gates_ref[:, width:] = gate_ref[...]
    first_ref[:, :first] = up_ref[:, :first]
    first_ref[:, first:] = down_ref[:, :first]
    for copy in range(late_ref.shape[0]):
        late_ref[copy, :, :width] = out_ref[...]
        late_ref[copy, :, width : width + LATE] = up_ref[:, first:]
        late_ref[copy, :, width + LATE :] = down_ref[:, first:]


def packed(w_value, w_gate, w_mix_out, w_up, w_down_t):
    rows, width = w_value.shape
    first = w_up.shape[1] - LATE
    return pl.pallas_call(
        pack_kernel,
        out_shape=(
            jax.ShapeDtypeStruct((rows, 2 * width), jnp.bfloat16),
            jax.ShapeDtypeStruct((rows, 2 * first), jnp.bfloat16),
            jax.ShapeDtypeStruct((lax.axis_size("y"), rows, width + 2 * LATE), jnp.bfloat16),
        ),
        compiler_params=pltpu.CompilerParams(vmem_limit_bytes=60 * MIB),
        cost_estimate=pl.CostEstimate(flops=0, bytes_accessed=MIB, transcendentals=0),
        name="pack",
    )(w_value, w_gate, w_mix_out, w_up, w_down_t)


def over_y(run):
    return lax.all_gather(run, "y", axis=1, tiled=True)


def over_z(slab):
    def from_z(step):
        pairs = [((i + step(i)) % 8, i) for i in range(8)]
        return lax.ppermute(slab, ("rep", "zl"), pairs)

    two = from_z(lambda i: 2 if i % 2 == 0 else -2)
    return [slab, from_z(lambda i: 1), two, from_z(lambda i: -1)]


def gate_kernel(x_ref, taps_ref, weight_ref, filtered_ref, sums_ref, padded_ref, held_ref, sems):
    count, depth, width = held_ref.shape[0], held_ref.shape[1], held_ref.shape[2] // 2
    copies = [
        pltpu.make_async_copy(weight_ref.at[z, :, : 2 * width], held_ref.at[z], sems.at[z])
        for z in range(count)
    ]
    for copy in copies:
        copy.start()
    value, gate = 0.0, 0.0
    for z, copy in enumerate(copies):
        copy.wait()
        x = x_ref[:, z * depth : (z + 1) * depth]
        value += jnp.dot(x, held_ref[z, :, :width], preferred_element_type=jnp.float32)
        gate += jnp.dot(x, held_ref[z, :, width:], preferred_element_type=jnp.float32)
    gated = value * jax.nn.sigmoid(gate)
    pad = padded_ref.shape[1] - LENGTH
    sequences = padded_ref.shape[0]
    for s in range(sequences):
        padded_ref[s, :pad] = jnp.zeros((pad, width), jnp.float32)
        padded_ref[s, pad:] = gated[s * LENGTH : (s + 1) * LENGTH]
    for lane in range(0, width, LANES):
        taps = taps_ref[:, lane : lane + LANES]
        for s in range(sequences):
            total = jnp.zeros((LENGTH, LANES), jnp.float32)
            for shift in range(8):
                offsets = [o for o in range(pad - KWIDTH + 1, pad + 1) if o % 8 == shift]
                span = offsets[-1] - shift + LENGTH
                rows = padded_ref[s, shift : shift + span, lane : lane + LANES]
                for o in offsets:
                    tap = o - (pad - KWIDTH + 1)
                    total += taps[tap : tap + 1] * rows[o - shift : o - shift + LENGTH]
            filtered_ref[s * LENGTH : (s + 1) * LENGTH, lane : lane + LANES] = total
    filtered = filtered_ref[...]
    ones = jnp.ones((8, width), jnp.float32)
    rows = x_ref.shape[0]
    for i, terms in enumerate((filtered, filtered * filtered)):
        sums = lax.dot_general(
            ones,
            terms,
            (((1,), (1,)), ((), ())),
            precision=lax.Precision.HIGHEST,
            preferred_element_type=jnp.float32,
        )
        for copy in range(sums_ref.shape[0]):
            sums_ref[copy, :, i * rows : (i + 1) * rows] = sums[:1]


def gated_filter(x, taps, weights, width):
    rows = x.shape[0]
    count, depth, _ = weights.shape
    vmem = pl.BlockSpec(memory_space=pltpu.VMEM)
    return pl.pallas_call(
        gate_kernel,
        in_specs=[vmem, vmem, ANY],
        out_specs=(vmem, vmem),
        out_shape=(
            jax.ShapeDtypeStruct((rows, width), jnp.float32),
            jax.ShapeDtypeStruct((lax.axis_size(TP), 1, 2 * rows), jnp.float32),
        ),
        scratch_shapes=[
            pltpu.VMEM((rows // LENGTH, LENGTH + 32, width), jnp.float32),
            pltpu.VMEM((count, depth, 2 * width), jnp.bfloat16),
            pltpu.SemaphoreType.DMA((count,)),
        ],
        compiler_params=pltpu.CompilerParams(vmem_limit_bytes=52 * MIB),
        cost_estimate=pl.CostEstimate(
            flops=4 * rows * D * width, bytes_accessed=4 * D * width, transcendentals=rows * width
        ),
        name="gated_filter",
    )(x, taps, weights)


def fetched(slab_refs, held_ref, columns, sems):
    here, count = lax.axis_index("zl"), lax.axis_size("zl")
    copies = []
    for turn, ref in enumerate(slab_refs):
        to = held_ref.at[lax.rem(here + turn, count)]
        copies.append(pltpu.make_async_copy(ref.at[:, columns], to, sems.at[turn]))
        copies[turn].start()
    return copies


def mixer_kernel(filtered_ref, sums_ref, gain_ref, *refs):
    *slab_refs, theirs_ref, mine_ref, held_ref, sems = refs
    core = lax.axis_index("c")
    rows, width = filtered_ref.shape
    copies = fetched(slab_refs, held_ref, slice(0, width), sems)
    sums = sum(sums_ref[d] for d in range(sums_ref.shape[0])) / D
    mean = sums[:, :rows]
    scale = lax.rsqrt(sums[:, rows:] - mean * mean + EPS)

    def down_rows(row):
        column = jnp.broadcast_to(row, (LANES, rows)).T
        return jnp.concatenate([column] * (width // LANES), axis=1)

    gain = gain_ref[:, pl.ds(pl.multiple_of(lax.axis_index(TP) * width, width), width)]
    values = (filtered_ref[...] - down_rows(mean)) * down_rows(scale) * gain
    activated = (values / (1.0 + jnp.exp(-values))).astype(jnp.bfloat16)
    here, count = lax.axis_index("zl"), lax.axis_size("zl")
    for turn, copy in enumerate(copies):
        z = lax.rem(here + turn, count)
        copy.wait()
        for out_ref, which in ((theirs_ref, 1 - core), (mine_ref, core)):
            at = pl.ds(pl.multiple_of(which * width, width), width)
            out_ref[z] = times_t(activated, held_ref[z, at]).astype(out_ref.dtype)


def mixer(filtered, sums, gain, slabs):
    rows, width = filtered.shape
    vmem = pl.BlockSpec(memory_space=pltpu.VMEM)
    out = (lax.axis_size("zl"), rows, width)
    return pl.pallas_call(
        mixer_kernel,
        in_specs=[vmem, vmem, vmem, *(ANY for _ in slabs)],
        out_specs=(vmem, vmem),
        out_shape=(
            jax.ShapeDtypeStruct(out, jnp.bfloat16),
            jax.ShapeDtypeStruct(out, jnp.bfloat16),
        ),
        scratch_shapes=[
            pltpu.VMEM((out[0], 2 * width, width), jnp.bfloat16),
            pltpu.SemaphoreType.DMA((len(slabs),)),
        ],
        compiler_params=pltpu.CompilerParams(vmem_limit_bytes=52 * MIB),
        cost_estimate=pl.CostEstimate(
            flops=2 * rows * D * width, bytes_accessed=2 * D * width, transcendentals=rows * width
        ),
        name="mixer",
    )(filtered, sums, gain[None], *slabs)


def norm_kernel(own_ref, other_ref, gain_ref, out_ref):
    core = lax.axis_index("c")
    count, _, width = own_ref.shape
    pieces = [(r[i].astype(jnp.float32), i, s) for s, r in enumerate((own_ref, other_ref)) for i in range(count)]
    total = sum(jnp.sum(v * v, axis=-1, keepdims=True) for v, _, _ in pieces)
    scale = lax.rsqrt(total / D + EPS)
    for values, i, side in pieces:
        which = core if side == 0 else 1 - core
        at = pl.ds(pl.multiple_of((2 * i + which) * width, width), width)
        out_ref[:, at] = (values * scale * gain_ref[:, at]).astype(jnp.bfloat16)


def normed_channels(own, gain, vmem_mib):
    other = lax.ppermute(own, "c", SWAP)
    count, rows, width = own.shape
    part = pl.BlockSpec((count, LENGTH, width), lambda i: (0, i, 0))
    return pl.pallas_call(
        norm_kernel,
        grid=(rows // LENGTH,),
        in_specs=[part, part, pl.BlockSpec((1, D), lambda i: (0, 0))],
        out_specs=pl.BlockSpec((LENGTH, D), lambda i: (i, 0)),
        out_shape=jax.ShapeDtypeStruct((rows, D), jnp.bfloat16),
        cost_estimate=pl.CostEstimate(
            flops=6 * rows * D, bytes_accessed=4 * rows * D, transcendentals=rows
        ),
        compiler_params=pltpu.CompilerParams(vmem_limit_bytes=vmem_mib * MIB),
        name="norm",
    )(own, other, gain[None])


def over_group(mine, theirs):
    got = lax.ppermute(theirs, "c", SWAP)
    pair = (mine.astype(jnp.float32) + got.astype(jnp.float32)).astype(jnp.bfloat16)
    return jnp.sum(lax.all_to_all(pair, "x", 0, 0, tiled=True).astype(jnp.float32), axis=0)


def feed_forward_kernel(rows_ref, first_ref, *refs):
    *slab_refs, theirs_ref, mine_ref, x_ref, up_ref, down_ref, late_ref, hidden_ref, sems = refs
    core = lax.axis_index("c")
    count, depth, columns = up_ref.shape
    width = depth // 2
    steps = [slice(low, low + width) for low in range(0, columns, width)]
    copies = [
        pltpu.make_async_copy(first_ref.at[:, :, at], up_ref.at[:, :, at], sems.at[i])
        for i, at in enumerate(steps)
    ]
    past = len(steps) + 2
    whole_x = pltpu.make_async_copy(rows_ref, x_ref, sems.at[past - 1])
    down = pltpu.make_async_copy(first_ref.at[:, :, columns:], down_ref, sems.at[len(steps)])
    whole_x.start()
    for copy in copies:
        copy.start()

    def hidden_of(weight_ref, at):
        upward = 0.0
        for z in range(count):
            x = x_ref[:, z * depth : (z + 1) * depth]
            upward += jnp.dot(x, weight_ref[z, :, at], preferred_element_type=jnp.float32)
        return jnp.square(jnp.maximum(upward, 0.0)).astype(jnp.bfloat16)

    whole_x.wait()
    copies[0].wait()
    late_copies = fetched(slab_refs, late_ref, slice(width, width + 2 * LATE), sems.at[past:])
    down.start()
    hidden_ref[:, steps[0]] = hidden_of(up_ref, steps[0])
    for copy, at in zip(copies[1:], steps[1:]):
        copy.wait()
        hidden_ref[:, at] = hidden_of(up_ref, at)
    for copy in late_copies:
        copy.wait()
    hidden_ref[:, columns:] = hidden_of(late_ref, slice(0, LATE))
    down.wait()
    for out_ref, which in ((theirs_ref, 1 - core), (mine_ref, core)):
        rows = pl.ds(pl.multiple_of(which * width, width), width)
        for z in range(count):
            part = times_t(hidden_ref[:, :columns], down_ref[z, rows])
            part += times_t(hidden_ref[:, columns:], late_ref[z, rows, LATE:])
            out_ref[z] = part.astype(out_ref.dtype)


def feed_forward(x, first, late):
    rows = x.shape[0]
    count, depth, columns = first.shape
    columns //= 2
    width = depth // 2
    out = (count, rows, width)
    vmem = pl.BlockSpec(memory_space=pltpu.VMEM)
    weights = pltpu.VMEM((count, depth, columns), jnp.bfloat16)
    hidden = columns + LATE
    return pl.pallas_call(
        feed_forward_kernel,
        in_specs=[ANY, ANY, *(ANY for _ in late)],
        out_specs=(vmem, vmem),
        out_shape=(
            jax.ShapeDtypeStruct(out, jnp.bfloat16),
            jax.ShapeDtypeStruct(out, jnp.bfloat16),
        ),
        scratch_shapes=[
            pltpu.VMEM(x.shape, jnp.bfloat16),
            weights,
            weights,
            pltpu.VMEM((count, depth, 2 * LATE), jnp.bfloat16),
            pltpu.VMEM((rows, hidden), jnp.bfloat16),
            pltpu.SemaphoreType.DMA((columns // width + 2 + len(late),)),
        ],
        compiler_params=pltpu.CompilerParams(vmem_limit_bytes=52 * MIB),
        cost_estimate=pl.CostEstimate(
            flops=4 * rows * D * hidden, bytes_accessed=4 * D * hidden, transcendentals=0
        ),
        name="feed_forward",
    )(x, first, *late)


def body(
    states, mix_gain, w_value, w_gate, conv_kernel, chan_gain, w_mix_out, mlp_gain, w_up, w_down_t
):
    width = states.shape[1]
    gates, first, late = packed(w_value, w_gate, w_mix_out, w_up, w_down_t)
    slab = lax.all_to_all(late, "y", 0, 0, tiled=True).reshape(-1, late.shape[2])
    gates = lax.all_gather(gates, "zl", axis=0)
    first = lax.all_gather(first, "zl", axis=0)
    slabs = over_z(slab)
    own = lax.all_gather(states, "x", axis=0)
    taps = lax.dynamic_slice_in_dim(conv_kernel, lax.axis_index(TP) * width, width, 1)
    own, taps = lax.optimization_barrier((own, taps))
    gates, first = over_y(gates), over_y(first)
    normed = normed_channels(own, mix_gain, 12)
    filtered, sums = gated_filter(normed, taps, gates, width)
    sums = lax.all_to_all(sums, TP, 0, 0, tiled=True)
    theirs, mine = mixer(filtered, sums, chan_gain, slabs)
    mixed = over_group(mine, theirs)
    middle = (states.astype(jnp.float32) + mixed).astype(jnp.bfloat16)
    normed_mid = normed_channels(lax.all_gather(middle, "x", axis=0), mlp_gain, 56)
    theirs, mine = feed_forward(normed_mid, first, slabs)
    fed = over_group(mine, theirs)
    return (middle.astype(jnp.float32) + fed).astype(jnp.bfloat16)


def solution(mesh):
    split = Mesh(mesh.devices.reshape(2, 4, 8, 4, 2), ("rep", "zl", "y", "x", "c"))
    fs = ("zl", "y")
    return jax.shard_map(
        body,
        mesh=split,
        in_specs=(
            P(("rep", *fs), TP),
            P(),
            P(fs, TP),
            P(fs, TP),
            P(),
            P(),
            P(fs, TP),
            P(),
            P(fs, TP),
            P(fs, TP),
        ),
        out_specs=P(("rep", *fs), TP),
        check_vma=False,
    )
```

```python
import jax
import jax.numpy as jnp
from jax import lax
from jax.experimental import pallas as pl
from jax.experimental.pallas import tpu as pltpu
from jax.sharding import Mesh
from jax.sharding import PartitionSpec as P

D = 2048
KWIDTH = 31
LENGTH = 128
EPS = 1e-06
TP = ("x", "c")
SWAP = [(0, 1), (1, 0)]


MIB = 1 << 20
LANES = 128
ANY = pl.BlockSpec(memory_space=pl.ANY)
LATE = 256


def times_t(left, right):
    return lax.dot_general(
        left, right, (((1,), (1,)), ((), ())), preferred_element_type=jnp.float32
    )


def pack_kernel(value_ref, gate_ref, out_ref, up_ref, down_ref, gates_ref, first_ref, late_ref):
    width, first = value_ref.shape[1], up_ref.shape[1] - LATE
    gates_ref[:, :width] = value_ref[...]
    gates_ref[:, width:] = gate_ref[...]
    first_ref[:, :first] = up_ref[:, :first]
    first_ref[:, first:] = down_ref[:, :first]
    for copy in range(late_ref.shape[0]):
        late_ref[copy, :, :width] = out_ref[...]
        late_ref[copy, :, width : width + LATE] = up_ref[:, first:]
        late_ref[copy, :, width + LATE :] = down_ref[:, first:]


def packed(w_value, w_gate, w_mix_out, w_up, w_down_t):
    rows, width = w_value.shape
    first = w_up.shape[1] - LATE
    return pl.pallas_call(
        pack_kernel,
        out_shape=(
            jax.ShapeDtypeStruct((rows, 2 * width), jnp.bfloat16),
            jax.ShapeDtypeStruct((rows, 2 * first), jnp.bfloat16),
            jax.ShapeDtypeStruct((lax.axis_size("y"), rows, width + 2 * LATE), jnp.bfloat16),
        ),
        compiler_params=pltpu.CompilerParams(vmem_limit_bytes=60 * MIB),
        cost_estimate=pl.CostEstimate(flops=0, bytes_accessed=MIB, transcendentals=0),
        name="pack",
    )(w_value, w_gate, w_mix_out, w_up, w_down_t)


def over_y(run):
    return lax.all_gather(run, "y", axis=1, tiled=True)


def over_z(slab):
    def from_z(step):
        pairs = [((i + step(i)) % 8, i) for i in range(8)]
        return lax.ppermute(slab, ("rep", "zl"), pairs)

    two = from_z(lambda i: 2 if i % 2 == 0 else -2)
    return [slab, from_z(lambda i: 1), two, from_z(lambda i: -1)]


def gate_kernel(x_ref, taps_ref, weight_ref, filtered_ref, sums_ref, padded_ref, held_ref, sems):
    count, depth, width = held_ref.shape[0], held_ref.shape[1], held_ref.shape[2] // 2
    copies = [
        pltpu.make_async_copy(weight_ref.at[z, :, : 2 * width], held_ref.at[z], sems.at[z])
        for z in range(count)
    ]
    for copy in copies:
        copy.start()
    value, gate = 0.0, 0.0
    for z, copy in enumerate(copies):
        copy.wait()
        x = x_ref[:, z * depth : (z + 1) * depth]
        value += jnp.dot(x, held_ref[z, :, :width], preferred_element_type=jnp.float32)
        gate += jnp.dot(x, held_ref[z, :, width:], preferred_element_type=jnp.float32)
    gated = value * jax.nn.sigmoid(gate)
    pad = padded_ref.shape[1] - LENGTH
    sequences = padded_ref.shape[0]
    for s in range(sequences):
        padded_ref[s, :pad] = jnp.zeros((pad, width), jnp.float32)
        padded_ref[s, pad:] = gated[s * LENGTH : (s + 1) * LENGTH]
    for lane in range(0, width, LANES):
        taps = taps_ref[:, lane : lane + LANES]
        for s in range(sequences):
            total = jnp.zeros((LENGTH, LANES), jnp.float32)
            for shift in range(8):
                offsets = [o for o in range(pad - KWIDTH + 1, pad + 1) if o % 8 == shift]
                span = offsets[-1] - shift + LENGTH
                rows = padded_ref[s, shift : shift + span, lane : lane + LANES]
                for o in offsets:
                    tap = o - (pad - KWIDTH + 1)
                    total += taps[tap : tap + 1] * rows[o - shift : o - shift + LENGTH]
            filtered_ref[s * LENGTH : (s + 1) * LENGTH, lane : lane + LANES] = total
    filtered = filtered_ref[...]
    ones = jnp.ones((8, width), jnp.float32)
    rows = x_ref.shape[0]
    for i, terms in enumerate((filtered, filtered * filtered)):
        sums = lax.dot_general(
            ones,
            terms,
            (((1,), (1,)), ((), ())),
            precision=lax.Precision.HIGHEST,
            preferred_element_type=jnp.float32,
        )
        for copy in range(sums_ref.shape[0]):
            sums_ref[copy, :, i * rows : (i + 1) * rows] = sums[:1]


def gated_filter(x, taps, weights, width):
    rows = x.shape[0]
    count, depth, _ = weights.shape
    vmem = pl.BlockSpec(memory_space=pltpu.VMEM)
    return pl.pallas_call(
        gate_kernel,
        in_specs=[vmem, vmem, ANY],
        out_specs=(vmem, vmem),
        out_shape=(
            jax.ShapeDtypeStruct((rows, width), jnp.float32),
            jax.ShapeDtypeStruct((lax.axis_size(TP), 1, 2 * rows), jnp.float32),
        ),
        scratch_shapes=[
            pltpu.VMEM((rows // LENGTH, LENGTH + 32, width), jnp.float32),
            pltpu.VMEM((count, depth, 2 * width), jnp.bfloat16),
            pltpu.SemaphoreType.DMA((count,)),
        ],
        compiler_params=pltpu.CompilerParams(vmem_limit_bytes=52 * MIB),
        cost_estimate=pl.CostEstimate(
            flops=4 * rows * D * width, bytes_accessed=4 * D * width, transcendentals=rows * width
        ),
        name="gated_filter",
    )(x, taps, weights)


def fetched(slab_refs, held_ref, columns, sems):
    here, count = lax.axis_index("zl"), lax.axis_size("zl")
    copies = []
    for turn, ref in enumerate(slab_refs):
        to = held_ref.at[lax.rem(here + turn, count)]
        copies.append(pltpu.make_async_copy(ref.at[:, columns], to, sems.at[turn]))
        copies[turn].start()
    return copies


def mixer_kernel(filtered_ref, sums_ref, gain_ref, *refs):
    *slab_refs, theirs_ref, mine_ref, held_ref, sems = refs
    core = lax.axis_index("c")
    rows, width = filtered_ref.shape
    copies = fetched(slab_refs, held_ref, slice(0, width), sems)
    sums = sum(sums_ref[d] for d in range(sums_ref.shape[0])) / D
    mean = sums[:, :rows]
    scale = lax.rsqrt(sums[:, rows:] - mean * mean + EPS)

    def down_rows(row):
        column = jnp.broadcast_to(row, (LANES, rows)).T
        return jnp.concatenate([column] * (width // LANES), axis=1)

    gain = gain_ref[:, pl.ds(pl.multiple_of(lax.axis_index(TP) * width, width), width)]
    values = (filtered_ref[...] - down_rows(mean)) * down_rows(scale) * gain
    activated = (values / (1.0 + jnp.exp(-values))).astype(jnp.bfloat16)
    here, count = lax.axis_index("zl"), lax.axis_size("zl")
    for turn, copy in enumerate(copies):
        z = lax.rem(here + turn, count)
        copy.wait()
        for out_ref, which in ((theirs_ref, 1 - core), (mine_ref, core)):
            at = pl.ds(pl.multiple_of(which * width, width), width)
            out_ref[z] = times_t(activated, held_ref[z, at]).astype(out_ref.dtype)


def mixer(filtered, sums, gain, slabs):
    rows, width = filtered.shape
    vmem = pl.BlockSpec(memory_space=pltpu.VMEM)
    out = (lax.axis_size("zl"), rows, width)
    return pl.pallas_call(
        mixer_kernel,
        in_specs=[vmem, vmem, vmem, *(ANY for _ in slabs)],
        out_specs=(vmem, vmem),
        out_shape=(
            jax.ShapeDtypeStruct(out, jnp.bfloat16),
            jax.ShapeDtypeStruct(out, jnp.bfloat16),
        ),
        scratch_shapes=[
            pltpu.VMEM((out[0], 2 * width, width), jnp.bfloat16),
            pltpu.SemaphoreType.DMA((len(slabs),)),
        ],
        compiler_params=pltpu.CompilerParams(vmem_limit_bytes=52 * MIB),
        cost_estimate=pl.CostEstimate(
            flops=2 * rows * D * width, bytes_accessed=2 * D * width, transcendentals=rows * width
        ),
        name="mixer",
    )(filtered, sums, gain[None], *slabs)


def norm_kernel(own_ref, other_ref, gain_ref, out_ref):
    core = lax.axis_index("c")
    count, _, width = own_ref.shape
    pieces = [(r[i].astype(jnp.float32), i, s) for s, r in enumerate((own_ref, other_ref)) for i in range(count)]
    total = sum(jnp.sum(v * v, axis=-1, keepdims=True) for v, _, _ in pieces)
    scale = lax.rsqrt(total / D + EPS)
    for values, i, side in pieces:
        which = core if side == 0 else 1 - core
        at = pl.ds(pl.multiple_of((2 * i + which) * width, width), width)
        out_ref[:, at] = (values * scale * gain_ref[:, at]).astype(jnp.bfloat16)


def normed_channels(own, gain):
    other = lax.ppermute(own, "c", SWAP)
    count, rows, width = own.shape
    part = pl.BlockSpec((count, LENGTH, width), lambda i: (0, i, 0))
    return pl.pallas_call(
        norm_kernel,
        grid=(rows // LENGTH,),
        in_specs=[part, part, pl.BlockSpec((1, D), lambda i: (0, 0))],
        out_specs=pl.BlockSpec((LENGTH, D), lambda i: (i, 0)),
        out_shape=jax.ShapeDtypeStruct((rows, D), jnp.bfloat16),
        cost_estimate=pl.CostEstimate(
            flops=6 * rows * D, bytes_accessed=4 * rows * D, transcendentals=rows
        ),
        compiler_params=pltpu.CompilerParams(vmem_limit_bytes=12 * MIB),
        name="norm",
    )(own, other, gain[None])


def over_group(mine, theirs):
    got = lax.ppermute(theirs, "c", SWAP)
    pair = (mine.astype(jnp.float32) + got.astype(jnp.float32)).astype(jnp.bfloat16)
    return jnp.sum(lax.all_to_all(pair, "x", 0, 0, tiled=True).astype(jnp.float32), axis=0)


def feed_forward_kernel(rows_ref, first_ref, *refs):
    *slab_refs, theirs_ref, mine_ref, x_ref, up_ref, down_ref, late_ref, hidden_ref, sems = refs
    core = lax.axis_index("c")
    count, depth, columns = up_ref.shape
    width = depth // 2
    steps = [slice(low, low + width) for low in range(0, columns, width)]
    copies = [
        pltpu.make_async_copy(first_ref.at[:, :, at], up_ref.at[:, :, at], sems.at[i])
        for i, at in enumerate(steps)
    ]
    past = len(steps) + 2
    whole_x = pltpu.make_async_copy(rows_ref, x_ref, sems.at[past - 1])
    down = pltpu.make_async_copy(first_ref.at[:, :, columns:], down_ref, sems.at[len(steps)])
    whole_x.start()
    for copy in copies:
        copy.start()

    def hidden_of(weight_ref, at):
        upward = 0.0
        for z in range(count):
            x = x_ref[:, z * depth : (z + 1) * depth]
            upward += jnp.dot(x, weight_ref[z, :, at], preferred_element_type=jnp.float32)
        return jnp.square(jnp.maximum(upward, 0.0)).astype(jnp.bfloat16)

    whole_x.wait()
    copies[0].wait()
    late_copies = fetched(slab_refs, late_ref, slice(width, width + 2 * LATE), sems.at[past:])
    down.start()
    hidden_ref[:, steps[0]] = hidden_of(up_ref, steps[0])
    for copy, at in zip(copies[1:], steps[1:]):
        copy.wait()
        hidden_ref[:, at] = hidden_of(up_ref, at)
    for copy in late_copies:
        copy.wait()
    hidden_ref[:, columns:] = hidden_of(late_ref, slice(0, LATE))
    down.wait()
    for out_ref, which in ((theirs_ref, 1 - core), (mine_ref, core)):
        rows = pl.ds(pl.multiple_of(which * width, width), width)
        for z in range(count):
            part = times_t(hidden_ref[:, :columns], down_ref[z, rows])
            part += times_t(hidden_ref[:, columns:], late_ref[z, rows, LATE:])
            out_ref[z] = part.astype(out_ref.dtype)


def feed_forward(x, first, late):
    rows = x.shape[0]
    count, depth, columns = first.shape
    columns //= 2
    width = depth // 2
    out = (count, rows, width)
    vmem = pl.BlockSpec(memory_space=pltpu.VMEM)
    weights = pltpu.VMEM((count, depth, columns), jnp.bfloat16)
    hidden = columns + LATE
    return pl.pallas_call(
        feed_forward_kernel,
        in_specs=[ANY, ANY, *(ANY for _ in late)],
        out_specs=(vmem, vmem),
        out_shape=(
            jax.ShapeDtypeStruct(out, jnp.bfloat16),
            jax.ShapeDtypeStruct(out, jnp.bfloat16),
        ),
        scratch_shapes=[
            pltpu.VMEM(x.shape, jnp.bfloat16),
            weights,
            weights,
            pltpu.VMEM((count, depth, 2 * LATE), jnp.bfloat16),
            pltpu.VMEM((rows, hidden), jnp.bfloat16),
            pltpu.SemaphoreType.DMA((columns // width + 2 + len(late),)),
        ],
        compiler_params=pltpu.CompilerParams(vmem_limit_bytes=52 * MIB),
        cost_estimate=pl.CostEstimate(
            flops=4 * rows * D * hidden, bytes_accessed=4 * D * hidden, transcendentals=0
        ),
        name="feed_forward",
    )(x, first, *late)


def body(
    states, mix_gain, w_value, w_gate, conv_kernel, chan_gain, w_mix_out, mlp_gain, w_up, w_down_t
):
    width = states.shape[1]
    gates, first, late = packed(w_value, w_gate, w_mix_out, w_up, w_down_t)
    slab = lax.all_to_all(late, "y", 0, 0, tiled=True).reshape(-1, late.shape[2])
    gates = lax.all_gather(gates, "zl", axis=0)
    first = lax.all_gather(first, "zl", axis=0)
    slabs = over_z(slab)
    own = lax.all_gather(states, "x", axis=0)
    taps = lax.dynamic_slice_in_dim(conv_kernel, lax.axis_index(TP) * width, width, 1)
    own, taps = lax.optimization_barrier((own, taps))
    gates, first = over_y(gates), over_y(first)
    normed = normed_channels(own, mix_gain)
    filtered, sums = gated_filter(normed, taps, gates, width)
    sums = lax.all_to_all(sums, TP, 0, 0, tiled=True)
    theirs, mine = mixer(filtered, sums, chan_gain, slabs)
    mixed = over_group(mine, theirs)
    middle = (states.astype(jnp.float32) + mixed).astype(jnp.bfloat16)
    normed_mid = normed_channels(lax.all_gather(middle, "x", axis=0), mlp_gain)
    theirs, mine = feed_forward(normed_mid, first, slabs)
    fed = over_group(mine, theirs)
    return (middle.astype(jnp.float32) + fed).astype(jnp.bfloat16)


def solution(mesh):
    split = Mesh(mesh.devices.reshape(2, 4, 8, 4, 2), ("rep", "zl", "y", "x", "c"))
    fs = ("zl", "y")
    return jax.shard_map(
        body,
        mesh=split,
        in_specs=(
            P(("rep", *fs), TP),
            P(),
            P(fs, TP),
            P(fs, TP),
            P(),
            P(),
            P(fs, TP),
            P(),
            P(fs, TP),
            P(fs, TP),
        ),
        out_specs=P(("rep", *fs), TP),
        check_vma=False,
    )
```
